256 devices in a mesh: sp: 32 (over z, x), fs: 4 (over y), tp: 2 (over core).
Axes of the slice: x: 4, y: 4, z: 8, core: 2. Of those that a mesh axis runs over, the one named last changes fastest.
Arguments:
- inputs: bfloat16 [4, 4096, 2048], P('fs', 'sp', 'tp'), may hold values from -1000 to 1000
- input_norm_gain: float32 [2048], replicated, may hold values from 0.1 to 1.9
- receptance_weight: bfloat16 [2048, 1024], P(('sp', 'fs'), 'tp'), may hold values from -0.125 to 0.125
- linear_key_weight: bfloat16 [2048, 1024], P(('sp', 'fs'), 'tp'), may hold values from -0.125 to 0.125
- linear_value_weight: bfloat16 [2048, 1024], P(('sp', 'fs'), 'tp'), may hold values from -0.125 to 0.125
- window_query_weight: bfloat16 [2048, 1024], P(('sp', 'fs'), 'tp'), may hold values from -1 to 1
- window_key_weight: bfloat16 [2048, 256], P(('sp', 'fs'), 'tp'), may hold values from -1 to 1
- window_value_weight: bfloat16 [2048, 256], P(('sp', 'fs'), 'tp'), may hold values from -0.125 to 0.125
- decay_down_weight: bfloat16 [2048, 96], replicated, may hold values from -0.125 to 0.125
- decay_up_weight: bfloat16 [2, 96, 1024], replicated, may hold values from -1 to 1
- decay_offset: float32 [2, 1024], replicated, may hold values from -13 to -3
- decay_log_extra: float32 [4, 16, 4096], P('fs', 'tp', 'sp'), may hold values from -1.4 to 0
- erasure_down_weight: bfloat16 [2048, 96], replicated, may hold values from -0.125 to 0.125
- erasure_up_weight: bfloat16 [2, 96, 1024], replicated, may hold values from -0.625 to 0.625
- erasure_offset: float32 [2, 1024], replicated, may hold values from -9.5 to 1
- initial_state: float32 [2, 16, 64, 64], replicated, may hold values from -384 to 384
- head_norm_gain: float32 [1024], replicated, may hold values from 0.1 to 1.9
- query_sink_logit: float32 [16], replicated, may hold values from 2 to 7
- linear_output_weight: bfloat16 [1024, 2048], P('tp', ('sp', 'fs')), may hold values from -0.1875 to 0.1875
- window_output_weight: bfloat16 [1024, 2048], P('tp', ('sp', 'fs')), may hold values from -1.5 to 1.5
Outputs:
- layer_out: bfloat16 [4, 4096, 2048], P('fs', ('sp', 'tp'))
The draws below stay inside these ranges and needn't reach their ends.
All inputs are finite; a program needn't handle non-finite values.
Results may differ from the reference program's by a relative error of at most 0.006.
The reference program's roundings to bfloat16 on the way count: a program that leaves them out, or rounds other values in their place, can miss the bound.
Values may be sent and summed in bfloat16 or wider, within the bound.
A program may use at most 128 MiB of HBM per device.

```python
import math
import jax
import jax.numpy as jnp
from jax import lax

MODEL_DIM = 2048
RH = 16
HD = 64
AH = 16
AKV = 4
LOW_RANK_WIDTH = 96
WINDOW = 128
GRID_W = 64
ATT_BLOCK = 128
SPAN = 8
TOK_DEV = 128
SEQS = 4
LENGTH = 4096
LINEAR_WIDTH = 1024
AW = 1024
KVW = 256


def slow_flags(key):
    share = 0.5
    flags = jax.random.bernoulli(jax.random.fold_in(key, 103), share, (RH,))
    return jnp.repeat(flags, HD)


def draw_inputs(key, part):
    shape = (SEQS, LENGTH, MODEL_DIM)
    noise_key = jax.random.fold_in(key, 1)
    return jax.random.normal(noise_key, shape, jnp.float32).astype(jnp.bfloat16)


def drawn_weight(key, salt, head_count):
    shape = (MODEL_DIM, head_count * HD)
    scale = MODEL_DIM ** (-0.5)
    noise_key = jax.random.fold_in(key, salt)
    return jax.random.normal(noise_key, shape, jnp.float32) * scale


def draw_window_query_weight(key, part):
    return drawn_weight(key, 5, AH).astype(jnp.bfloat16)


def draw_window_key_weight(key, part):
    return drawn_weight(key, 6, AKV).astype(jnp.bfloat16)


def draw_decay_offset(key, part):
    slow = slow_flags(key)[None, :]
    spread = jax.random.uniform(jax.random.fold_in(key, 7), (2, LINEAR_WIDTH), jnp.float32, 0.0, 1.0)
    slow_value = -math.log(LENGTH) - 2.0 + spread
    fast_value = -4.2 + spread
    return jnp.where(slow, slow_value, fast_value)


def draw_erasure_offset(key, part):
    slow = slow_flags(key)[None, :]
    spread = jax.random.uniform(jax.random.fold_in(key, 8), (2, LINEAR_WIDTH), jnp.float32, 0.0, 1.0)
    return jnp.where(slow, -9.5 + spread, -1.0 + 2.0 * spread)


def draw_decay_log_extra(key, part):
    span_len = TOK_DEV // 2
    span_count = LENGTH // span_len
    factor = jax.random.uniform(jax.random.fold_in(key, 9), (SEQS, RH, span_count, 1), jnp.float32, 0.0, 0.8)
    steady = -jnp.broadcast_to(factor, (SEQS, RH, span_count, span_len)).reshape(SEQS, RH, LENGTH) / LENGTH
    places = jax.random.randint(jax.random.fold_in(key, 10), (SEQS, RH, 2, 1), 0, LENGTH)
    depths = jax.random.uniform(jax.random.fold_in(key, 11), (SEQS, RH, 2, 1), jnp.float32, 0.22, 0.69)
    hits = jnp.sum(depths * (jnp.arange(LENGTH)[None, None, None, :] == places).astype(jnp.float32), axis=2)
    return steady - hits


def steps_of(rng, extent, cuts, smallest, high):
    gain, own = 1.0, jax.random.fold_in(rng, 6)
    for dim, blocks in cuts:
        draws = jnp.exp(jax.random.uniform(jax.random.fold_in(own, dim), (blocks,), jnp.float32, smallest / len(cuts), high / len(cuts)))
        gain = gain * jnp.repeat(draws, extent[dim] // blocks).reshape([-1 if axis == dim else 1 for axis in range(len(extent))])
    return gain


def scatter_about(own_key, shape, scale, limit, cuts=(), kind=jnp.bfloat16):
    factor_of = steps_of(own_key, shape, cuts, -0.22, 0.18) if cuts else 1.0
    drawn = jax.random.normal(own_key, shape, jnp.float32) * scale * factor_of
    return jnp.minimum(jnp.maximum(drawn, -limit), limit).astype(kind)


def setup_inputs(seed: int = 0) -> dict:
    key_of = jax.random.split(jax.random.key(seed), 21)
    return {
        "inputs": draw_inputs(jax.random.fold_in(key_of[20], 71), 0),
        "input_norm_gain": jnp.clip(1.0 + 0.18 * jax.random.normal(key_of[1], (MODEL_DIM,), jnp.float32), 0.1, 1.9),
        "receptance_weight": scatter_about(key_of[2], (MODEL_DIM, LINEAR_WIDTH), MODEL_DIM ** -0.5, 0.125, ((0, 128), (1, 2))),
        "linear_key_weight": scatter_about(key_of[3], (MODEL_DIM, LINEAR_WIDTH), MODEL_DIM ** -0.5, 0.125, ((0, 128), (1, 2))),
        "linear_value_weight": scatter_about(key_of[4], (MODEL_DIM, LINEAR_WIDTH), MODEL_DIM ** -0.5, 0.125, ((0, 128), (1, 2))),
        "window_query_weight": draw_window_query_weight(jax.random.fold_in(key_of[20], 71), 0),
        "window_key_weight": draw_window_key_weight(jax.random.fold_in(key_of[20], 71), 0),
        "window_value_weight": scatter_about(key_of[7], (MODEL_DIM, KVW), MODEL_DIM ** -0.5, 0.125, ((0, 128), (1, 2))),
        "decay_down_weight": scatter_about(key_of[8], (MODEL_DIM, LOW_RANK_WIDTH), MODEL_DIM ** -0.5, 0.125),
        "decay_up_weight": scatter_about(key_of[9], (2, LOW_RANK_WIDTH, LINEAR_WIDTH), 36 ** -0.5, 1.0),
        "decay_offset": draw_decay_offset(jax.random.fold_in(key_of[20], 71), 0),
        "decay_log_extra": draw_decay_log_extra(jax.random.fold_in(key_of[20], 71), 0),
        "erasure_down_weight": scatter_about(key_of[12], (MODEL_DIM, LOW_RANK_WIDTH), MODEL_DIM ** -0.5, 0.125),
        "erasure_up_weight": scatter_about(key_of[13], (2, LOW_RANK_WIDTH, LINEAR_WIDTH), LOW_RANK_WIDTH ** -0.5, 0.625),
        "erasure_offset": draw_erasure_offset(jax.random.fold_in(key_of[20], 71), 0),
        "initial_state": scatter_about(key_of[15], (2, RH, HD, HD), (LENGTH ** 0.5), 384.0, (), jnp.float32),
        "head_norm_gain": jnp.clip(1.0 + 0.18 * jax.random.normal(key_of[16], (LINEAR_WIDTH,), jnp.float32), 0.1, 1.9),
        "query_sink_logit": jnp.clip(jax.random.uniform(key_of[17], (AH,), jnp.float32, 2.0, 7.0), 2.0, 7.0),
        "linear_output_weight": scatter_about(key_of[18], (LINEAR_WIDTH, MODEL_DIM), LINEAR_WIDTH ** -0.5, 0.1875, ((0, 2), (1, 128))),
        "window_output_weight": scatter_about(key_of[19], (AW, MODEL_DIM), (AW // 64) ** -0.5, 1.5, ((0, 2), (1, 128))),
    }


NORM_EPS = 1e-06
GROUP_EPS = 0.00064
ROPE_BASE = 10000.0
HIGHEST = lax.Precision.HIGHEST

def to_bf16(array):
    return lax.optimization_barrier(array.astype(jnp.bfloat16))

def rope_axial(values, positions):
    quarter = values.shape[-1] // 4
    inverse = ROPE_BASE ** (-jnp.arange(quarter, dtype=jnp.float32) / quarter)
    grid_rows = (positions // GRID_W).astype(jnp.float32)
    grid_cols = (positions % GRID_W).astype(jnp.float32)
    pieces = []
    for which_half, coordinate in ((0, grid_rows), (1, grid_cols)):
        angles = coordinate[:, None] * inverse[None, :]
        cosine = jnp.cos(angles)[:, None, :]
        sine_part = jnp.sin(angles)[:, None, :]
        front_part = values[..., 2 * which_half * quarter:(2 * which_half + 1) * quarter]
        back_part = values[..., (2 * which_half + 1) * quarter:(2 * which_half + 2) * quarter]
        pieces.append(front_part * cosine - back_part * sine_part)
        pieces.append(front_part * sine_part + back_part * cosine)
    return jnp.concatenate(pieces, axis=-1)

def run_chain(initial, recept, decay_factor, keys, values, unit, erase, backward):
    seq_count, length = (recept.shape[0], recept.shape[1])
    segments = length // SPAN

    def blocked(array):
        return jnp.moveaxis(array.reshape(seq_count, segments, SPAN, RH, HD), 1, 0)
    streams = tuple((blocked(array) for array in (recept, decay_factor, keys, values, unit, erase)))
    visits = list(range(SPAN))[::-1] if backward else list(range(SPAN))

    def advance(memory, segment):
        results = [None] * SPAN
        for position in visits:
            read_now, decay_now, key_now, value_now, unit_now, erase_now = (array[:, position] for array in segment)
            erased = jnp.einsum('bhvk,bhk->bhv', memory, unit_now, precision=HIGHEST)
            memory = memory * decay_now[:, :, None, :] - erased[..., None] * erase_now[:, :, None, :] + value_now[..., None] * key_now[:, :, None, :]
            results[position] = jnp.einsum('bhvk,bhk->bhv', memory, read_now, precision=HIGHEST)
        return (memory, jnp.stack(results, axis=1))
    memory_init = jnp.broadcast_to(initial[None], (seq_count,) + initial.shape)
    _, outputs = lax.scan(advance, memory_init, streams, reverse=backward)
    return jnp.moveaxis(outputs, 0, 1).reshape(seq_count, length, RH, HD)

def window_attention(queries, keys, values, query_sink_logit):
    seq_count, length = (queries.shape[0], queries.shape[1])
    group_size = AH // AKV
    grouped = queries.reshape(seq_count, length, AKV, group_size, HD).astype(jnp.float32)
    padding = ((0, 0), (WINDOW, WINDOW), (0, 0), (0, 0))
    key_pad = jnp.pad(keys, padding).astype(jnp.float32)
    value_pad = jnp.pad(values, padding).astype(jnp.float32)
    sink_local = query_sink_logit.reshape(AKV, group_size)[None, :, :, None, None]
    reach = ATT_BLOCK + 2 * WINDOW

    def one_block(block_idx):
        query_rows = lax.dynamic_slice_in_dim(grouped, block_idx * ATT_BLOCK, ATT_BLOCK, 1)
        key_rows = lax.dynamic_slice_in_dim(key_pad, block_idx * ATT_BLOCK, reach, 1)
        value_rows = lax.dynamic_slice_in_dim(value_pad, block_idx * ATT_BLOCK, reach, 1)
        scores = jnp.einsum('sqgrd,skgd->sgrqk', query_rows, key_rows) * HD ** (-0.5)
        query_pos = block_idx * ATT_BLOCK + jnp.arange(ATT_BLOCK, dtype=jnp.int32)
        key_pos = block_idx * ATT_BLOCK - WINDOW + jnp.arange(reach, dtype=jnp.int32)
        allowed = (jnp.abs(query_pos[:, None] - key_pos[None, :]) <= WINDOW) & (key_pos[None, :] >= 0) & (key_pos[None, :] < length)
        scores = jnp.where(allowed, scores, -jnp.inf)
        top_score = jnp.maximum(lax.optimization_barrier(jnp.max(scores, axis=-1, keepdims=True)), sink_local)
        raised = jnp.exp(scores - top_score)
        denominator = jnp.exp(sink_local - top_score) + lax.optimization_barrier(jnp.sum(raised, axis=-1, keepdims=True))
        weights = to_bf16(raised / denominator).astype(jnp.float32)
        mixed = jnp.einsum('sgrqk,skgd->sqgrd', weights, value_rows)
        return mixed.astype(jnp.bfloat16)
    blocks = lax.map(one_block, jnp.arange(length // ATT_BLOCK, dtype=jnp.int32))
    return jnp.moveaxis(blocks, 0, 1).reshape(seq_count, length, AH * HD)

def reference(inputs, input_norm_gain, receptance_weight, linear_key_weight, linear_value_weight, window_query_weight, window_key_weight, window_value_weight, decay_down_weight, decay_up_weight, decay_offset, decay_log_extra, erasure_down_weight, erasure_up_weight, erasure_offset, initial_state, head_norm_gain, query_sink_logit, linear_output_weight, window_output_weight):
    seq_count, length, model_width = inputs.shape
    widened = inputs.astype(jnp.float32)
    hidden = to_bf16(widened * lax.rsqrt(lax.optimization_barrier(jnp.mean(widened * widened, axis=-1, keepdims=True)) + NORM_EPS) * input_norm_gain).reshape(seq_count * length, model_width)

    def project(weight):
        return to_bf16(jnp.dot(hidden, weight, preferred_element_type=jnp.float32))

    def lin_heads(array):
        return array.astype(jnp.float32).reshape(seq_count, length, RH, HD)
    recept = lin_heads(project(receptance_weight))
    keys = lin_heads(project(linear_key_weight))
    values = lin_heads(project(linear_value_weight))
    unit = keys * lax.rsqrt(lax.optimization_barrier(jnp.sum(keys * keys, axis=-1, keepdims=True)) + NORM_EPS)
    decay_act = to_bf16(jnp.tanh(project(decay_down_weight).astype(jnp.float32)))
    learn_low = project(erasure_down_weight)
    decay_spikes = jnp.transpose(decay_log_extra, (0, 2, 1))[..., None]
    lin_sum = jnp.zeros((seq_count, length, RH, HD), jnp.float32)
    for direction in range(2):
        pre_decay = decay_offset[direction] + jnp.dot(decay_act, decay_up_weight[direction], preferred_element_type=jnp.float32)
        erasure_rate = lin_heads(jnp.exp(-jax.nn.softplus(-pre_decay) - 0.5))
        decay_factor = jnp.exp(decay_spikes - erasure_rate)
        learn = lin_heads(jax.nn.sigmoid(erasure_offset[direction] + jnp.dot(learn_low, erasure_up_weight[direction], preferred_element_type=jnp.float32)))
        lin_sum = lin_sum + run_chain(initial_state[direction], recept, decay_factor, keys, values, unit, unit * learn, direction == 1)
    centred = lin_sum - lax.optimization_barrier(jnp.mean(lin_sum, axis=-1, keepdims=True))
    normed = centred * lax.rsqrt(lax.optimization_barrier(jnp.mean(centred * centred, axis=-1, keepdims=True)) + GROUP_EPS)
    lin_mix = (normed.reshape(seq_count * length, RH * HD) * head_norm_gain).astype(jnp.bfloat16)
    positions = jnp.arange(length, dtype=jnp.int32)
    queries = to_bf16(rope_axial(project(window_query_weight).astype(jnp.float32).reshape(seq_count, length, AH, HD), positions))
    att_keys = to_bf16(rope_axial(project(window_key_weight).astype(jnp.float32).reshape(seq_count, length, AKV, HD), positions))
    att_values = project(window_value_weight).reshape(seq_count, length, AKV, HD)
    att_mix = window_attention(queries, att_keys, att_values, query_sink_logit).reshape(seq_count * length, AH * HD)
    result = jnp.dot(lin_mix, linear_output_weight, preferred_element_type=jnp.float32) + jnp.dot(att_mix, window_output_weight, preferred_element_type=jnp.float32)
    return result.astype(jnp.bfloat16).reshape(seq_count, length, model_width)
```

```python
import functools
import jax
import jax.numpy as jnp
from jax import lax
from jax.experimental import pallas as pl
from jax.experimental.pallas import tpu as pltpu

from jax.sharding import Mesh
from jax.sharding import PartitionSpec as P

HD = 64
CH = 64
PAIR = 128
WINDOW = 128
GRID_W = 64
ATT_BLOCK = 128
SP = ("sp_0", "sp_1")
SP_FS = ("sp_0", "sp_1", "fs")
SP_TP = ("sp_0", "sp_1", "tp")
NORM_EPS = 1e-06
GROUP_EPS = 0.00064
ROPE_BASE = 10000.0
F32 = jnp.float32
BF = jnp.bfloat16
MESSAGE = jnp.float32
NN = (((1,), (0,)), ((), ()))
NT = (((1,), (1,)), ((), ()))
TN = (((0,), (0,)), ((), ()))


def dot(a, b, dims=NN):
    return lax.dot_general(a, b, dims, preferred_element_type=F32)


def split2(a):
    high = a.astype(BF)
    return high, (a - high.astype(F32)).astype(BF)


def split3(a):
    high, rest = a.astype(BF), None
    rest = a - high.astype(F32)
    mid = rest.astype(BF)
    return high, mid, (rest - mid.astype(F32)).astype(BF)


def mm3(a, b, dims=NN):
    (ka,), (kb,) = dims[0]
    a_hi, a_lo = split2(a)
    b_hi, b_lo = split2(b)
    main = dot(
        jnp.concatenate([a_hi, a_lo], axis=ka), jnp.concatenate([b_hi, b_hi], axis=kb), dims
    )
    return main + dot(a_hi, b_lo, dims)


def mm2(a, b_exact, dims=NN):
    (ka,), (kb,) = dims[0]
    a_hi, a_lo = split2(a)
    return dot(
        jnp.concatenate([a_hi, a_lo], axis=ka), jnp.concatenate([b_exact, b_exact], axis=kb), dims
    )


def iota(shape, dim):
    return lax.broadcasted_iota(jnp.int32, shape, dim)


def ones_where(cond):
    return jnp.where(cond, 1.0, 0.0).astype(BF)


def rates_kernel(
    hidden_ref, down_d_ref, down_e_ref, up_d_ref, up_e_ref, off_d_ref, off_e_ref, extra_ref,
    logd_ref, learn_ref,
):
    width = logd_ref.shape[2]
    start = pl.multiple_of(lax.axis_index("tp") * width, width)
    cols = pl.ds(start, width)
    hidden = hidden_ref[...]
    decay_low = dot(hidden, down_d_ref[...]).astype(BF)
    learn_low = dot(hidden, down_e_ref[...]).astype(BF)
    decay_act = jnp.tanh(decay_low.astype(F32)).astype(BF)
    heads = width // HD
    spread = ones_where(iota((heads, width), 1) // HD == iota((heads, width), 0)).astype(F32)
    spikes = lax.dot_general(
        extra_ref[0], spread, TN, precision=lax.Precision.HIGHEST, preferred_element_type=F32
    )
    for d in range(2):
        x = off_d_ref[d : d + 1, cols] + dot(decay_act, up_d_ref[d, :, cols])
        softplus = jnp.maximum(-x, 0.0) + jnp.log1p(jnp.exp(-jnp.abs(x)))
        logd_ref[d] = spikes - jnp.exp(-softplus - 0.5)
        y = off_e_ref[d : d + 1, cols] + dot(learn_low, up_e_ref[d, :, cols])
        learn_ref[d] = jax.nn.sigmoid(y)


def stacked(x):
    low = iota(x.shape, 1) < HD
    return jnp.concatenate([jnp.where(low, x, 0.0), jnp.where(low, 0.0, x)], axis=0)


def unstacked(x):
    return x[:CH] + x[CH:]


def local_kernel(proj_ref, logd_ref, learn_ref, q_ref, o_ref, msg_ref):
    width = o_ref.shape[1]
    row = iota((2 * CH, 2 * CH), 0)
    col = iota((2 * CH, 2 * CH), 1)
    t, s = row % CH, col % CH
    eye = row == col
    same_head = ones_where(row // HD == col // HD)
    tri = [ones_where((iota((CH, CH), 0) >= iota((CH, CH), 1))), ones_where((iota((CH, CH), 0) <= iota((CH, CH), 1)))]
    strict = [t > s, t < s]
    within = [t >= s, t <= s]

    def one_pair(p, carry):
        lanes = pl.ds(pl.multiple_of(p * PAIR, PAIR), PAIR)
        recept = proj_ref[:, pl.ds(pl.multiple_of(p * PAIR, PAIR), PAIR)].astype(F32)
        keys = proj_ref[:, pl.ds(pl.multiple_of(width + p * PAIR, PAIR), PAIR)].astype(F32)
        values = proj_ref[:, pl.ds(pl.multiple_of(2 * width + p * PAIR, PAIR), PAIR)].astype(F32)
        squares = mm2(keys * keys, same_head)
        unit = keys * lax.rsqrt(squares + NORM_EPS)
        jobs = [(d, c) for d in range(2) for c in range(2)]
        stage = {}
        for d, c in jobs:
            rows = slice(c * CH, (c + 1) * CH)
            logd = logd_ref[d, rows, lanes]
            parts = jnp.concatenate(split3(logd), axis=0)
            total = dot(jnp.concatenate([tri[d]] * 3, axis=1), parts)
            middle = total[CH // 2 - 1 : CH // 2] if d == 0 else total[CH // 2 : CH // 2 + 1]
            last = total[CH - 1 : CH] if d == 0 else total[0:1]
            grow = jnp.exp(total - middle)
            shrink = jnp.exp(middle - total)
            read = recept[rows] * grow
            mark = unit[rows] * jnp.exp(total - logd - middle)
            erase = unit[rows] * learn_ref[d, rows, lanes] * shrink
            key = keys[rows] * shrink
            read_s, mark_s, erase_s, key_s = map(stacked, (read, mark, erase, key))
            scores = mm3(
                jnp.concatenate([mark_s, read_s], axis=0),
                jnp.concatenate([erase_s, key_s], axis=0),
                NT,
            )
            stage[d, c] = (read, mark_s, erase_s, key_s, scores, jnp.exp(middle), jnp.exp(last - middle), jnp.exp(last))
        inverse = {}
        grams = {}
        for d, c in jobs:
            gram = jnp.where(strict[d], stage[d, c][4][: 2 * CH, : 2 * CH], 0.0)
            grams[d, c] = gram
            inverse[d, c] = jnp.where(eye, 1.0, 0.0) - jnp.where(t // 2 == s // 2, gram, 0.0)
        block = 2
        while block < CH:
            joins = (t // (2 * block) == s // (2 * block)) & (t // block != s // block)
            for job in jobs:
                x = inverse[job]
                inverse[job] = x - mm3(x, mm3(jnp.where(joins, grams[job], 0.0), x))
            block *= 2
        maps, reads, outs = {}, {}, {}
        for d, c in jobs:
            rows = slice(c * CH, (c + 1) * CH)
            read, mark_s, erase_s, key_s, scores, to_start, to_end, whole = stage[d, c]
            val_s = stacked(values[rows]).astype(BF)
            cross = jnp.where(strict[d], scores[: 2 * CH, 2 * CH :], 0.0)
            read_e = jnp.where(within[d], scores[2 * CH :, : 2 * CH], 0.0)
            read_k = jnp.where(within[d], scores[2 * CH :, 2 * CH :], 0.0)
            solved = mm3(inverse[d, c], jnp.concatenate([mark_s, mm2(cross, val_s)], axis=1))
            solved = jnp.concatenate([solved[:, :PAIR] * to_start, solved[:, PAIR:]], axis=1)
            taken = mm3(read_e, solved)
            reads[d, c] = read * to_start - unstacked(taken[:, :PAIR])
            outs[d, c] = unstacked(mm2(read_k, val_s) - taken[:, PAIR:])
            ended = mm3(solved, erase_s * to_end, TN)
            k_hi, k_lo = split2(key_s * to_end)
            added = dot(jnp.concatenate([val_s, val_s], axis=0), jnp.concatenate([k_hi, k_lo], axis=0), TN)
            prod = jnp.where(eye, whole - 1.0, 0.0) - ended[:PAIR]
            maps[d, c] = (prod, added - ended[PAIR:])
        out_rows = [outs[0, 0] + outs[1, 0], outs[0, 1] + outs[1, 1]]
        for d in range(2):
            first, second = (0, 1) if d == 0 else (1, 0)
            (prod1, add1), (prod2, add2) = maps[d, first], maps[d, second]
            both = jnp.concatenate([prod1, add1], axis=0)
            through = mm3(reads[d, second], both, NT)
            q_ref[d, first * CH : (first + 1) * CH, lanes] = reads[d, first]
            q_ref[d, second * CH : (second + 1) * CH, lanes] = reads[d, second] + through[:, :PAIR]
            out_rows[second] = out_rows[second] + through[:, PAIR:]
            joined = mm3(both, prod2)
            prod = prod1 + prod2 + joined[:PAIR]
            add = add1 + joined[PAIR:] + add2
            for hh in range(2):
                for half in range(2):
                    message = jnp.concatenate(
                        [
                            folded(prod, hh, hh * HD, HD // 2),
                            folded(add, hh, hh * HD + half * (HD // 2), HD // 4),
                        ],
                        axis=0,
                    )
                    msg_ref[d * 16 + p * 4 + hh * 2 + half] = message.astype(msg_ref.dtype)
        for c in range(2):
            o_ref[c * CH : (c + 1) * CH, lanes] = out_rows[c]
        return carry

    lax.fori_loop(0, width // PAIR, one_pair, 0)


def folded(x, hh, first, count):
    upper, lower = x[first : first + count], x[first + count : first + 2 * count]
    if hh == 0:
        return upper + pltpu.roll(lower, HD, 1)
    return pltpu.roll(upper, HD, 1) + lower


def chain_kernel(recv_ref, init_ref, sent_ref):
    place = lax.axis_index("sp_0") * lax.axis_size("sp_1") + lax.axis_index("sp_1")
    count = recv_ref.shape[0]
    unit_idx = place // 2
    direction, head, half = unit_idx // 8, unit_idx % 8, place % 2
    rows = HD // 2
    start = pl.multiple_of(half * rows, rows)
    state = init_ref[direction, lax.axis_index("tp") * 8 + head, pl.ds(start, rows), :]

    def unfolded(x):
        return jnp.concatenate([x[:, :HD], x[:, HD:]], axis=0)

    for step in range(count):
        idx = direction * (count - 1) + step * (1 - 2 * direction)
        quarter = rows // 2
        sent_ref[idx] = jnp.concatenate([state[:quarter], state[quarter:]], axis=1).astype(sent_ref.dtype)
        if step == count - 1:
            break
        message = recv_ref[idx].astype(F32)
        prod = unfolded(message[:rows])
        state = state + mm3(state, prod) + unfolded(message[rows:])


def finish_kernel(q_ref, o_ref, enter_ref, gain_ref, mix_ref):
    width = o_ref.shape[1]
    row = iota((PAIR, PAIR), 0)
    col = iota((PAIR, PAIR), 1)
    same_head = ones_where(row // HD == col // HD)
    low = iota((HD // 4, PAIR), 1) < HD
    start = lax.axis_index("tp") * width

    def one_pair(p, carry):
        lanes = pl.ds(pl.multiple_of(p * PAIR, PAIR), PAIR)
        out = o_ref[:, lanes]
        for d in range(2):
            pieces = []
            for hh in range(2):
                for half in range(2):
                    m = enter_ref[d * 16 + p * 4 + hh * 2 + half].astype(F32)
                    turned = pltpu.roll(m, HD, 1)
                    if hh == 0:
                        pieces += [jnp.where(low, m, 0.0), jnp.where(low, turned, 0.0)]
                    else:
                        pieces += [jnp.where(low, 0.0, turned), jnp.where(low, 0.0, m)]
            out = out + mm3(q_ref[d, :, lanes], jnp.concatenate(pieces, axis=0), NT)
        centred = out - mm2(out, same_head) * (1.0 / HD)
        spread = mm2(centred * centred, same_head) * (1.0 / HD)
        gain = gain_ref[:, pl.ds(pl.multiple_of(start + p * PAIR, PAIR), PAIR)]
        mix_ref[:, lanes] = (centred * lax.rsqrt(spread + GROUP_EPS) * gain).astype(BF)
        return carry

    lax.fori_loop(0, width // PAIR, one_pair, 0)


def laid_out(parts, dim):
    parts = jnp.moveaxis(parts, 0, dim)
    dims = parts.shape
    return parts.reshape(*dims[:dim], dims[dim] * dims[dim + 1], *dims[dim + 2 :])


def from_everyone(value, axis):
    copies = jnp.broadcast_to(value, (lax.axis_size(axis), *value.shape))
    return lax.all_to_all(copies, axis, split_axis=0, concat_axis=0, tiled=True)


def gather_directly(value, axis, dim):
    return laid_out(from_everyone(value, axis), dim)


def whole_of(value, axes, dim):
    out = value
    for number in range(len(axes) - 1, -1, -1):
        out = lax.all_gather(out, axes[number], axis=dim, tiled=True)
    return out


def padded(block, sides, width):
    for axis, dim in sides:
        count = lax.axis_size(axis)
        forward = [(i, i + 1) for i in range(count - 1)]
        backward = [(target, source) for source, target in forward]
        low = lax.ppermute(
            lax.slice_in_dim(block, block.shape[dim] - width, None, axis=dim), axis, forward
        )
        high = lax.ppermute(lax.slice_in_dim(block, 0, width, axis=dim), axis, backward)
        block = jnp.concatenate([low, block, high], axis=dim)
    return block


def turned_gather(arrays, axis, dims):
    turned = [jnp.moveaxis(a, dim, 0) for a, dim in zip(arrays, dims)]
    both = jnp.concatenate([t.reshape(len(t), -1) for t in turned], axis=1)
    out, at, gathered = (lax.all_gather(both, axis, axis=0, tiled=True), 0, [])
    for t, dim in zip(turned, dims):
        share = out[:, at : at + t[0].size].reshape(-1, *t.shape[1:])
        gathered.append(jnp.moveaxis(share, 0, dim))
        at += t[0].size
    return tuple(gathered)


def cut_along(value, dim, size):
    dims = value.shape
    parts = value.reshape(*dims[:dim], size, dims[dim] // size, *dims[dim + 1 :])
    return jnp.moveaxis(parts, dim, 0)


def sum_at_owner(value, axis, dim):
    parts = cut_along(value, dim, lax.axis_size(axis))
    arrived = lax.all_to_all(parts, axis, split_axis=0, concat_axis=0, tiled=True)
    return arrived.sum(axis=0)


def to_bf16(array):
    return lax.optimization_barrier(array.astype(jnp.bfloat16))


def rope_axial(values, positions):
    quarter = values.shape[-1] // 4
    inverse = ROPE_BASE ** (-jnp.arange(quarter, dtype=jnp.float32) / quarter)
    grid_rows = (positions // GRID_W).astype(jnp.float32)
    grid_cols = (positions % GRID_W).astype(jnp.float32)
    pieces = []
    for which_half, coordinate in ((0, grid_rows), (1, grid_cols)):
        angles = coordinate[:, None] * inverse[None, :]
        cosine = jnp.cos(angles)[:, None, :]
        sine_part = jnp.sin(angles)[:, None, :]
        front_part = values[..., 2 * which_half * quarter : (2 * which_half + 1) * quarter]
        back_part = values[..., (2 * which_half + 1) * quarter : (2 * which_half + 2) * quarter]
        pieces.append(front_part * cosine - back_part * sine_part)
        pieces.append(front_part * sine_part + back_part * cosine)
    return jnp.concatenate(pieces, axis=-1)


def local(
    inputs,
    input_norm_gain,
    receptance_weight,
    linear_key_weight,
    linear_value_weight,
    window_query_weight,
    window_key_weight,
    window_value_weight,
    decay_down_weight,
    decay_up_weight,
    decay_offset,
    decay_log_extra,
    erasure_down_weight,
    erasure_up_weight,
    erasure_offset,
    initial_state,
    head_norm_gain,
    query_sink_logit,
    linear_output_weight,
    window_output_weight,
):
    tokens = inputs.shape[1]
    tp_index = lax.axis_index("tp")
    length = tokens * lax.axis_size(SP)
    offset = lax.axis_index(SP) * tokens
    gathered = gather_directly(inputs, "tp", 2)[0]
    widened = gathered.astype(jnp.float32)
    hidden = to_bf16(
        widened
        * lax.rsqrt(jnp.mean(widened * widened, axis=-1, keepdims=True) + NORM_EPS)
        * input_norm_gain
    )
    weights = (
        receptance_weight,
        linear_key_weight,
        linear_value_weight,
        window_query_weight,
        window_key_weight,
        window_value_weight,
    )
    widths = [weight.shape[1] for weight in weights]
    joined = jnp.concatenate(weights, axis=1)
    regrouped = lax.all_to_all(joined, "fs", split_axis=1, concat_axis=0, tiled=True)
    every_seq = gather_directly(hidden, "fs", 0)
    whole_cols = whole_of(regrouped, SP, 0)
    partial_cols = jnp.dot(every_seq, whole_cols, preferred_element_type=jnp.float32)
    returned = lax.all_to_all(to_bf16(partial_cols), "fs", split_axis=0, concat_axis=1, tiled=True)
    bounds = [0]
    for col_width in widths:
        bounds.append(bounds[-1] + col_width)
    projected = [returned[:, bounds[role_idx] : bounds[role_idx + 1]] for role_idx in range(6)]
    recept, lin_keys, lin_values, queries, att_keys, att_values = projected
    head_width = recept.shape[1]
    logd, learn = pl.pallas_call(
        rates_kernel,
        out_shape=[jax.ShapeDtypeStruct((2, tokens, head_width), F32)] * 2,
        name="rates",
        cost_estimate=pl.CostEstimate(flops=2 * tokens * 2048 * 96 * 4, bytes_accessed=2**21, transcendentals=0),
    )(
        hidden, decay_down_weight, erasure_down_weight, decay_up_weight, erasure_up_weight,
        decay_offset, erasure_offset, decay_log_extra,
    )
    reads, local_out, messages = pl.pallas_call(
        local_kernel,
        out_shape=[
            jax.ShapeDtypeStruct((2, tokens, head_width), F32),
            jax.ShapeDtypeStruct((tokens, head_width), F32),
            jax.ShapeDtypeStruct((32, 48, PAIR), MESSAGE),
        ],
        name="local_maps",
        cost_estimate=pl.CostEstimate(flops=10**9, bytes_accessed=2**21, transcendentals=0),
    )(returned, logd, learn)
    arrived = lax.all_to_all(messages, SP, split_axis=0, concat_axis=0, tiled=True)
    entries = pl.pallas_call(
        chain_kernel,
        out_shape=jax.ShapeDtypeStruct((32, 16, PAIR), MESSAGE),
        name="chain",
    )(arrived, initial_state)
    entered = lax.all_to_all(entries, SP, split_axis=0, concat_axis=0, tiled=True)
    lin_mix = pl.pallas_call(
        finish_kernel,
        out_shape=jax.ShapeDtypeStruct((tokens, head_width), BF),
        name="finish",
    )(reads, local_out, entered, head_norm_gain[None])
    positions = offset + jnp.arange(tokens, dtype=jnp.int32)
    query_count = queries.shape[1] // HD
    group_count = att_keys.shape[1] // HD
    group_size = query_count // group_count
    roped_q = rope_axial(
        queries.astype(jnp.float32).reshape(tokens, query_count, HD), positions
    ).astype(jnp.bfloat16)
    roped_k = rope_axial(
        att_keys.astype(jnp.float32).reshape(tokens, group_count, HD), positions
    ).astype(jnp.bfloat16)
    kv_width = group_count * HD
    packed = jnp.concatenate([roped_k.reshape(tokens, kv_width), att_values], axis=1)
    bordered = padded(packed, ((SP, 0),), WINDOW)
    sink_local = lax.dynamic_slice_in_dim(
        query_sink_logit, tp_index * query_count, query_count, 0
    ).reshape(group_count, group_size)[:, :, None, None]
    reach = ATT_BLOCK + 2 * WINDOW
    query_rows = roped_q.reshape(ATT_BLOCK, group_count, group_size, HD)
    key_rows = bordered[:, :kv_width].reshape(reach, group_count, HD)
    value_rows = bordered[:, kv_width:].reshape(reach, group_count, HD)
    scores = jnp.einsum(
        "qgrd,kgd->grqk", query_rows, key_rows, preferred_element_type=jnp.float32
    ) * HD ** (-0.5)
    query_pos = offset + 0 + jnp.arange(ATT_BLOCK, dtype=jnp.int32)
    key_pos = offset + 0 - WINDOW + jnp.arange(reach, dtype=jnp.int32)
    allowed = (
        (jnp.abs(query_pos[:, None] - key_pos[None, :]) <= WINDOW)
        & (key_pos[None, :] >= 0)
        & (key_pos[None, :] < length)
    )
    scores = jnp.where(allowed, scores, -jnp.inf)
    top_score = jnp.maximum(jnp.max(scores, axis=-1, keepdims=True), sink_local)
    raised = jnp.exp(scores - top_score)
    denominator = jnp.exp(sink_local - top_score) + jnp.sum(raised, axis=-1, keepdims=True)
    weights_bf = (raised / denominator).astype(jnp.bfloat16)
    mixed = jnp.einsum("grqk,kgd->qgrd", weights_bf, value_rows, preferred_element_type=jnp.float32)
    outputs = mixed.astype(jnp.bfloat16).reshape(ATT_BLOCK, query_count * HD)
    lin_weight, att_weight = turned_gather(
        (linear_output_weight, window_output_weight), SP_FS, (1, 1)
    )
    layer_out = sum_at_owner(
        jnp.dot(lin_mix, lin_weight, preferred_element_type=jnp.float32)
        + jnp.dot(outputs, att_weight, preferred_element_type=jnp.float32),
        "tp",
        0,
    )
    return layer_out.astype(jnp.bfloat16)[None]


def solution(mesh):
    finer = Mesh(
        mesh.devices.reshape(8, 4, mesh.shape["fs"], mesh.shape["tp"]), ("sp_0", "sp_1", "fs", "tp")
    )
    placed = (
        P("fs", SP, "tp"),
        P(),
        P(SP_FS, "tp"),
        P(SP_FS, "tp"),
        P(SP_FS, "tp"),
        P(SP_FS, "tp"),
        P(SP_FS, "tp"),
        P(SP_FS, "tp"),
        P(),
        P(),
        P(),
        P("fs", "tp", SP),
        P(),
        P(),
        P(),
        P(),
        P(),
        P(),
        P("tp", SP_FS),
        P("tp", SP_FS),
    )
    return jax.shard_map(
        local, mesh=finer, in_specs=placed, out_specs=P("fs", SP_TP, None), check_vma=False
    )
```

```python
import functools
import jax
import jax.numpy as jnp
from jax import lax
from jax.experimental import pallas as pl
from jax.experimental.pallas import tpu as pltpu

from jax.sharding import Mesh
from jax.sharding import PartitionSpec as P

HD = 64
CH = 64
PAIR = 128
WINDOW = 128
GRID_W = 64
ATT_BLOCK = 128
SP = ("sp_0", "sp_1")
SP_FS = ("sp_0", "sp_1", "fs")
SP_TP = ("sp_0", "sp_1", "tp")
NORM_EPS = 1e-06
GROUP_EPS = 0.00064
ROPE_BASE = 10000.0
F32 = jnp.float32
BF = jnp.bfloat16
MESSAGE = jnp.bfloat16
MESH = pl.DeviceIdType.MESH
NN = (((1,), (0,)), ((), ()))
NT = (((1,), (1,)), ((), ()))
TN = (((0,), (0,)), ((), ()))


def dot(a, b, dims=NN):
    return lax.dot_general(a, b, dims, preferred_element_type=F32)


def split2(a):
    high = a.astype(BF)
    return high, (a - high.astype(F32)).astype(BF)


def split3(a):
    high, rest = a.astype(BF), None
    rest = a - high.astype(F32)
    mid = rest.astype(BF)
    return high, mid, (rest - mid.astype(F32)).astype(BF)


def mm3(a, b, dims=NN):
    (ka,), (kb,) = dims[0]
    a_hi, a_lo = split2(a)
    b_hi, b_lo = split2(b)
    main = dot(
        jnp.concatenate([a_hi, a_lo], axis=ka), jnp.concatenate([b_hi, b_hi], axis=kb), dims
    )
    return main + dot(a_hi, b_lo, dims)


def mm2(a, b_exact, dims=NN):
    (ka,), (kb,) = dims[0]
    a_hi, a_lo = split2(a)
    return dot(
        jnp.concatenate([a_hi, a_lo], axis=ka), jnp.concatenate([b_exact, b_exact], axis=kb), dims
    )


def iota(shape, dim):
    return lax.broadcasted_iota(jnp.int32, shape, dim)


def ones_where(cond):
    return jnp.where(cond, 1.0, 0.0).astype(BF)


def rates_kernel(
    hidden_ref, down_d_ref, down_e_ref, up_d_ref, up_e_ref, off_d_ref, off_e_ref, extra_ref,
    logd_ref, learn_ref,
):
    width = logd_ref.shape[2]
    start = pl.multiple_of(lax.axis_index("tp") * width, width)
    cols = pl.ds(start, width)
    hidden = hidden_ref[...]
    decay_low = dot(hidden, down_d_ref[...]).astype(BF)
    learn_low = dot(hidden, down_e_ref[...]).astype(BF)
    decay_act = jnp.tanh(decay_low.astype(F32)).astype(BF)
    heads = width // HD
    spread = ones_where(iota((heads, width), 1) // HD == iota((heads, width), 0)).astype(F32)
    spikes = lax.dot_general(
        extra_ref[0], spread, TN, precision=lax.Precision.HIGHEST, preferred_element_type=F32
    )
    for d in range(2):
        x = off_d_ref[d : d + 1, cols] + dot(decay_act, up_d_ref[d, :, cols])
        softplus = jnp.maximum(-x, 0.0) + jnp.log1p(jnp.exp(-jnp.abs(x)))
        logd_ref[d] = spikes - jnp.exp(-softplus - 0.5)
        y = off_e_ref[d : d + 1, cols] + dot(learn_low, up_e_ref[d, :, cols])
        learn_ref[d] = jax.nn.sigmoid(y)


def stacked(x):
    low = iota(x.shape, 1) < HD
    return jnp.concatenate([jnp.where(low, x, 0.0), jnp.where(low, 0.0, x)], axis=0)


def unstacked(x):
    return x[:CH] + x[CH:]


def local_kernel(proj_ref, logd_ref, learn_ref, q_ref, o_ref, msg_ref):
    width = o_ref.shape[1]
    row = iota((2 * CH, 2 * CH), 0)
    col = iota((2 * CH, 2 * CH), 1)
    t, s = row % CH, col % CH
    eye = row == col
    same_head = ones_where(row // HD == col // HD)
    tri = [ones_where((iota((CH, CH), 0) >= iota((CH, CH), 1))), ones_where((iota((CH, CH), 0) <= iota((CH, CH), 1)))]
    strict = [t > s, t < s]
    within = [t >= s, t <= s]

    def one_pair(p, carry):
        lanes = pl.ds(pl.multiple_of(p * PAIR, PAIR), PAIR)
        recept = proj_ref[:, pl.ds(pl.multiple_of(p * PAIR, PAIR), PAIR)].astype(F32)
        keys = proj_ref[:, pl.ds(pl.multiple_of(width + p * PAIR, PAIR), PAIR)].astype(F32)
        values = proj_ref[:, pl.ds(pl.multiple_of(2 * width + p * PAIR, PAIR), PAIR)].astype(F32)
        squares = mm2(keys * keys, same_head)
        unit = keys * lax.rsqrt(squares + NORM_EPS)
        jobs = [(d, c) for d in range(2) for c in range(2)]
        stage = {}
        for d, c in jobs:
            rows = slice(c * CH, (c + 1) * CH)
            logd = logd_ref[d, rows, lanes]
            parts = jnp.concatenate(split3(logd), axis=0)
            total = dot(jnp.concatenate([tri[d]] * 3, axis=1), parts)
            middle = total[CH // 2 - 1 : CH // 2] if d == 0 else total[CH // 2 : CH // 2 + 1]
            last = total[CH - 1 : CH] if d == 0 else total[0:1]
            grow = jnp.exp(total - middle)
            shrink = jnp.exp(middle - total)
            read = recept[rows] * grow
            mark = unit[rows] * jnp.exp(total - logd - middle)
            erase = unit[rows] * learn_ref[d, rows, lanes] * shrink
            key = keys[rows] * shrink
            read_s, mark_s, erase_s, key_s = map(stacked, (read, mark, erase, key))
            scores = mm3(
                jnp.concatenate([mark_s, read_s], axis=0),
                jnp.concatenate([erase_s, key_s], axis=0),
                NT,
            )
            stage[d, c] = (read, mark_s, erase_s, key_s, scores, jnp.exp(middle), jnp.exp(last - middle), jnp.exp(last))
        inverse = {}
        grams = {}
        for d, c in jobs:
            gram = jnp.where(strict[d], stage[d, c][4][: 2 * CH, : 2 * CH], 0.0)
            grams[d, c] = gram
            inverse[d, c] = jnp.where(eye, 1.0, 0.0) - jnp.where(t // 2 == s // 2, gram, 0.0)
        block = 2
        while block < CH:
            joins = (t // (2 * block) == s // (2 * block)) & (t // block != s // block)
            for job in jobs:
                x = inverse[job]
                inverse[job] = x - mm3(x, mm3(jnp.where(joins, grams[job], 0.0), x))
            block *= 2
        maps, reads, outs = {}, {}, {}
        for d, c in jobs:
            rows = slice(c * CH, (c + 1) * CH)
            read, mark_s, erase_s, key_s, scores, to_start, to_end, whole = stage[d, c]
            val_s = stacked(values[rows]).astype(BF)
            cross = jnp.where(strict[d], scores[: 2 * CH, 2 * CH :], 0.0)
            read_e = jnp.where(within[d], scores[2 * CH :, : 2 * CH], 0.0)
            read_k = jnp.where(within[d], scores[2 * CH :, 2 * CH :], 0.0)
            solved = mm3(inverse[d, c], jnp.concatenate([mark_s, mm2(cross, val_s)], axis=1))
            solved = jnp.concatenate([solved[:, :PAIR] * to_start, solved[:, PAIR:]], axis=1)
            taken = mm3(read_e, solved)
            reads[d, c] = read * to_start - unstacked(taken[:, :PAIR])
            outs[d, c] = unstacked(mm2(read_k, val_s) - taken[:, PAIR:])
            ended = mm3(solved, erase_s * to_end, TN)
            k_hi, k_lo = split2(key_s * to_end)
            added = dot(jnp.concatenate([val_s, val_s], axis=0), jnp.concatenate([k_hi, k_lo], axis=0), TN)
            prod = jnp.where(eye, whole - 1.0, 0.0) - ended[:PAIR]
            maps[d, c] = (prod, added - ended[PAIR:])
        out_rows = [outs[0, 0] + outs[1, 0], outs[0, 1] + outs[1, 1]]
        for d in range(2):
            first, second = (0, 1) if d == 0 else (1, 0)
            (prod1, add1), (prod2, add2) = maps[d, first], maps[d, second]
            both = jnp.concatenate([prod1, add1], axis=0)
            through = mm3(reads[d, second], both, NT)
            q_ref[d, first * CH : (first + 1) * CH, lanes] = reads[d, first]
            q_ref[d, second * CH : (second + 1) * CH, lanes] = reads[d, second] + through[:, :PAIR]
            out_rows[second] = out_rows[second] + through[:, PAIR:]
            joined = mm3(both, prod2)
            prod = prod1 + prod2 + joined[:PAIR]
            add = add1 + joined[PAIR:] + add2
            for hh in range(2):
                for half in range(2):
                    message = jnp.concatenate(
                        [
                            folded(prod, hh, hh * HD, HD // 2),
                            folded(add, hh, hh * HD + half * (HD // 2), HD // 4),
                        ],
                        axis=0,
                    )
                    msg_ref[d * 16 + p * 4 + hh * 2 + half] = message.astype(msg_ref.dtype)
        for c in range(2):
            o_ref[c * CH : (c + 1) * CH, lanes] = out_rows[c]
        return carry

    lax.fori_loop(0, width // PAIR, one_pair, 0)


def folded(x, hh, first, count):
    upper, lower = x[first : first + count], x[first + count : first + 2 * count]
    if hh == 0:
        return upper + pltpu.roll(lower, HD, 1)
    return pltpu.roll(upper, HD, 1) + lower


def peer_id(index):
    inner = lax.axis_size("sp_1")
    return {"sp_0": index // inner, "sp_1": index % inner}


def exchange_kernel(
    msg_ref, init_ref, reads_ref, local_ref, gain_ref, proj_ref, cos_ref, sin_ref, sink_ref,
    mix_ref, att_ref,
    recv_ref, sent_ref, enter_ref, halo_ref,
    out_sem, in_sem, back_out_sem, back_in_sem, halo_out_sem, halo_in_sem,
):
    count = recv_ref.shape[0]
    place = lax.axis_index("sp_0") * lax.axis_size("sp_1") + lax.axis_index("sp_1")
    width = local_ref.shape[1]
    kv_first = 4 * width
    barrier = pltpu.get_barrier_semaphore()

    def greet(k, carry):
        pl.semaphore_signal(barrier, inc=1, device_id=peer_id((place + k) % count), device_id_type=MESH)
        return carry

    lax.fori_loop(1, count, greet, 0)
    pl.semaphore_wait(barrier, count - 1)

    def halo_copy(side):
        target = (place + count - 1 + 2 * side) % count
        return pltpu.make_async_remote_copy(
            src_ref=proj_ref.at[:, kv_first : kv_first + 2 * PAIR],
            dst_ref=halo_ref.at[1 - side],
            send_sem=halo_out_sem.at[side],
            recv_sem=halo_in_sem.at[1 - side],
            device_id=peer_id(target),
            device_id_type=MESH,
        )

    def map_copy(target):
        return pltpu.make_async_remote_copy(
            src_ref=msg_ref.at[target],
            dst_ref=recv_ref.at[place],
            send_sem=out_sem.at[target],
            recv_sem=in_sem.at[place],
            device_id=peer_id(target),
            device_id_type=MESH,
        )

    def map_arrival(source):
        return pltpu.make_async_remote_copy(
            src_ref=msg_ref.at[source],
            dst_ref=recv_ref.at[source],
            send_sem=out_sem.at[source],
            recv_sem=in_sem.at[source],
            device_id=peer_id(source),
            device_id_type=MESH,
        )

    def entry_copy(target):
        return pltpu.make_async_remote_copy(
            src_ref=sent_ref.at[target],
            dst_ref=enter_ref.at[place],
            send_sem=back_out_sem.at[target],
            recv_sem=back_in_sem.at[place],
            device_id=peer_id(target),
            device_id_type=MESH,
        )

    def entry_arrival(source):
        return pltpu.make_async_remote_copy(
            src_ref=sent_ref.at[source],
            dst_ref=enter_ref.at[source],
            send_sem=back_out_sem.at[source],
            recv_sem=back_in_sem.at[source],
            device_id=peer_id(source),
            device_id_type=MESH,
        )

    halo_copy(0).start()
    halo_copy(1).start()

    def send_map(k, carry):
        map_copy((place + k) % count).start()
        return carry

    lax.fori_loop(1, count, send_map, 0)
    recv_ref[place] = msg_ref[place]

    tokens = local_ref.shape[0]
    for side in range(2):
        halo_copy(side).wait()
    kv = jnp.concatenate(
        [halo_ref[0], proj_ref[:, kv_first : kv_first + 2 * PAIR], halo_ref[1]], axis=0
    )
    lane = iota((1, PAIR), 1)
    low = lane < HD
    front = lane % 32 < 16

    def turned(x, rows):
        other = jnp.where(front, -pltpu.roll(x, PAIR - 16, 1), pltpu.roll(x, 16, 1))
        return x * cos_ref[rows, :] + other * sin_ref[rows, :]

    reach = 3 * tokens
    roped_k = turned(kv[:, :PAIR].astype(F32), slice(0, reach))
    values = kv[:, PAIR:].astype(F32)
    q_pos = place * tokens + iota((2 * tokens, reach), 0) % tokens
    k_pos = (place - 1) * tokens + iota((2 * tokens, reach), 1)
    allowed = (jnp.abs(q_pos - k_pos) <= WINDOW) & (k_pos >= 0) & (k_pos < count * tokens)
    upper = iota((2 * tokens, 1), 0) < tokens
    head_first = lax.axis_index("tp") * (width // HD)
    for group in range(2):
        doubled = []
        for x in (roped_k, values):
            other = pltpu.roll(x, HD, 1)
            doubled.append((jnp.where(low, x, other) if group == 0 else jnp.where(low, other, x)).astype(BF))
        for p in (2 * group, 2 * group + 1):
            lanes = slice(p * PAIR, (p + 1) * PAIR)
            query = turned(proj_ref[:, 3 * width + p * PAIR : 3 * width + (p + 1) * PAIR].astype(F32), slice(tokens, 2 * tokens))
            query = jnp.concatenate([jnp.where(low, query, 0.0), jnp.where(low, 0.0, query)], axis=0)
            scores = dot(query.astype(BF), doubled[0], NT) * HD**-0.5
            scores = jnp.where(allowed, scores, -jnp.inf)
            head = head_first + 2 * p
            sink = jnp.where(upper, sink_ref[head], sink_ref[head + 1])
            top = jnp.maximum(jnp.max(scores, axis=-1, keepdims=True), sink)
            raised = jnp.exp(scores - top)
            total = jnp.exp(sink - top) + jnp.sum(raised, axis=-1, keepdims=True)
            mixed = dot((raised / total).astype(BF), doubled[1])
            att_ref[:, lanes] = jnp.where(low, mixed[:tokens], mixed[tokens:]).astype(BF)

    def await_map(k, carry):
        map_arrival((place + k) % count).wait()
        return carry

    lax.fori_loop(1, count, await_map, 0)

    unit_idx = place // 2
    direction, head, half = unit_idx // 8, unit_idx % 8, place % 2
    rows = HD // 2
    quarter = rows // 2
    start = pl.multiple_of(half * rows, rows)

    def unfolded(x):
        return jnp.concatenate([x[:, :HD], x[:, HD:]], axis=0)

    def nth(step):
        return direction * (count - 1) + step * (1 - 2 * direction)

    def advance(step, state):
        idx = nth(step)
        sent_ref[idx] = jnp.concatenate([state[:quarter], state[quarter:]], axis=1).astype(BF)
        before = nth(step - 1)

        @pl.when((step > 0) & (before != place))
        def _():
            entry_copy(before).start()

        message = recv_ref[idx].astype(F32)
        return state + mm3(state, unfolded(message[:rows])) + unfolded(message[rows:])

    state = init_ref[direction, lax.axis_index("tp") * 8 + head, pl.ds(start, rows), :]
    lax.fori_loop(0, count, advance, state)
    final = nth(count - 1)
    enter_ref[place] = sent_ref[place]

    @pl.when(final != place)
    def _():
        entry_copy(final).start()

    def await_entry(k, carry):
        entry_arrival((place + k) % count).wait()
        return carry

    lax.fori_loop(1, count, await_entry, 0)
    finish(reads_ref, local_ref, enter_ref, gain_ref, mix_ref)


def finish(q_ref, o_ref, enter_ref, gain_ref, mix_ref):
    width = o_ref.shape[1]
    row = iota((PAIR, PAIR), 0)
    col = iota((PAIR, PAIR), 1)
    same_head = ones_where(row // HD == col // HD)
    low = iota((HD // 4, PAIR), 1) < HD
    start = lax.axis_index("tp") * width
    for p in range(width // PAIR):
        lanes = slice(p * PAIR, (p + 1) * PAIR)
        out = o_ref[:, lanes]
        for d in range(2):
            pieces = []
            for hh in range(2):
                for half in range(2):
                    m = enter_ref[d * 16 + p * 4 + hh * 2 + half].astype(F32)
                    turned = pltpu.roll(m, HD, 1)
                    if hh == 0:
                        pieces += [jnp.where(low, m, 0.0), jnp.where(low, turned, 0.0)]
                    else:
                        pieces += [jnp.where(low, 0.0, turned), jnp.where(low, 0.0, m)]
            out = out + mm2(q_ref[d, :, lanes], jnp.concatenate(pieces, axis=0).astype(BF), NT)
        centred = out - mm2(out, same_head) * (1.0 / HD)
        spread = mm2(centred * centred, same_head) * (1.0 / HD)
        gain = gain_ref[:, pl.ds(pl.multiple_of(start + p * PAIR, PAIR), PAIR)]
        mix_ref[:, lanes] = (centred * lax.rsqrt(spread + GROUP_EPS) * gain).astype(BF)


def laid_out(parts, dim):
    parts = jnp.moveaxis(parts, 0, dim)
    dims = parts.shape
    return parts.reshape(*dims[:dim], dims[dim] * dims[dim + 1], *dims[dim + 2 :])


def from_everyone(value, axis):
    copies = jnp.broadcast_to(value, (lax.axis_size(axis), *value.shape))
    return lax.all_to_all(copies, axis, split_axis=0, concat_axis=0, tiled=True)


def gather_directly(value, axis, dim):
    return laid_out(from_everyone(value, axis), dim)


def whole_of(value, axes, dim):
    out = value
    for number in range(len(axes) - 1, -1, -1):
        out = lax.all_gather(out, axes[number], axis=dim, tiled=True)
    return out


def turned_gather(arrays, axis, dims):
    turned = [jnp.moveaxis(a, dim, 0) for a, dim in zip(arrays, dims)]
    both = jnp.concatenate([t.reshape(len(t), -1) for t in turned], axis=1)
    out, at, gathered = (lax.all_gather(both, axis, axis=0, tiled=True), 0, [])
    for t, dim in zip(turned, dims):
        share = out[:, at : at + t[0].size].reshape(-1, *t.shape[1:])
        gathered.append(jnp.moveaxis(share, 0, dim))
        at += t[0].size
    return tuple(gathered)


def cut_along(value, dim, size):
    dims = value.shape
    parts = value.reshape(*dims[:dim], size, dims[dim] // size, *dims[dim + 1 :])
    return jnp.moveaxis(parts, dim, 0)


def sum_at_owner(value, axis, dim):
    parts = cut_along(value, dim, lax.axis_size(axis))
    arrived = lax.all_to_all(parts, axis, split_axis=0, concat_axis=0, tiled=True)
    return arrived.sum(axis=0)


def to_bf16(array):
    return lax.optimization_barrier(array.astype(jnp.bfloat16))


def rope_axial(values, positions):
    quarter = values.shape[-1] // 4
    inverse = ROPE_BASE ** (-jnp.arange(quarter, dtype=jnp.float32) / quarter)
    grid_rows = (positions // GRID_W).astype(jnp.float32)
    grid_cols = (positions % GRID_W).astype(jnp.float32)
    pieces = []
    for which_half, coordinate in ((0, grid_rows), (1, grid_cols)):
        angles = coordinate[:, None] * inverse[None, :]
        cosine = jnp.cos(angles)[:, None, :]
        sine_part = jnp.sin(angles)[:, None, :]
        front_part = values[..., 2 * which_half * quarter : (2 * which_half + 1) * quarter]
        back_part = values[..., (2 * which_half + 1) * quarter : (2 * which_half + 2) * quarter]
        pieces.append(front_part * cosine - back_part * sine_part)
        pieces.append(front_part * sine_part + back_part * cosine)
    return jnp.concatenate(pieces, axis=-1)


def local(
    inputs,
    input_norm_gain,
    receptance_weight,
    linear_key_weight,
    linear_value_weight,
    window_query_weight,
    window_key_weight,
    window_value_weight,
    decay_down_weight,
    decay_up_weight,
    decay_offset,
    decay_log_extra,
    erasure_down_weight,
    erasure_up_weight,
    erasure_offset,
    initial_state,
    head_norm_gain,
    query_sink_logit,
    linear_output_weight,
    window_output_weight,
):
    tokens = inputs.shape[1]
    tp_index = lax.axis_index("tp")
    length = tokens * lax.axis_size(SP)
    offset = lax.axis_index(SP) * tokens
    gathered = gather_directly(inputs, "tp", 2)[0]
    widened = gathered.astype(jnp.float32)
    hidden = to_bf16(
        widened
        * lax.rsqrt(jnp.mean(widened * widened, axis=-1, keepdims=True) + NORM_EPS)
        * input_norm_gain
    )
    weights = (
        receptance_weight,
        linear_key_weight,
        linear_value_weight,
        window_query_weight,
        window_key_weight,
        window_value_weight,
    )
    widths = [weight.shape[1] for weight in weights]
    joined = jnp.concatenate(weights, axis=1)
    regrouped = lax.all_to_all(joined, "fs", split_axis=1, concat_axis=0, tiled=True)
    every_seq = gather_directly(hidden, "fs", 0)
    whole_cols = whole_of(regrouped, SP, 0)
    partial_cols = jnp.dot(every_seq, whole_cols, preferred_element_type=jnp.float32)
    returned = lax.all_to_all(to_bf16(partial_cols), "fs", split_axis=0, concat_axis=1, tiled=True)
    bounds = [0]
    for col_width in widths:
        bounds.append(bounds[-1] + col_width)
    projected = [returned[:, bounds[role_idx] : bounds[role_idx + 1]] for role_idx in range(6)]
    recept, lin_keys, lin_values, queries, att_keys, att_values = projected
    head_width = recept.shape[1]
    logd, learn = pl.pallas_call(
        rates_kernel,
        out_shape=[jax.ShapeDtypeStruct((2, tokens, head_width), F32)] * 2,
        name="rates",
        cost_estimate=pl.CostEstimate(flops=2 * tokens * 2048 * 96 * 4, bytes_accessed=2**21, transcendentals=0),
    )(
        hidden, decay_down_weight, erasure_down_weight, decay_up_weight, erasure_up_weight,
        decay_offset, erasure_offset, decay_log_extra,
    )
    reads, local_out, messages = pl.pallas_call(
        local_kernel,
        out_shape=[
            jax.ShapeDtypeStruct((2, tokens, head_width), F32),
            jax.ShapeDtypeStruct((tokens, head_width), F32),
            jax.ShapeDtypeStruct((32, 48, PAIR), MESSAGE),
        ],
        name="local_maps",
        cost_estimate=pl.CostEstimate(flops=10**9, bytes_accessed=2**21, transcendentals=0),
    )(returned, logd, learn)
    angle_pos = offset - WINDOW + jnp.arange(tokens + 2 * WINDOW, dtype=jnp.int32)
    inverse = ROPE_BASE ** (-jnp.arange(HD // 4, dtype=jnp.float32) / (HD // 4))
    row_angles = (angle_pos // GRID_W).astype(F32)[:, None] * inverse[None, :]
    col_angles = (angle_pos % GRID_W).astype(F32)[:, None] * inverse[None, :]
    angles = jnp.concatenate([row_angles, row_angles, col_angles, col_angles] * 2, axis=1)
    whole = [pl.BlockSpec(memory_space=pltpu.VMEM)] * 8 + [pl.BlockSpec(memory_space=pltpu.SMEM)]
    places = lax.axis_size(SP)
    lin_mix, outputs = pl.pallas_call(
        exchange_kernel,
        out_shape=[jax.ShapeDtypeStruct((tokens, head_width), BF)] * 2,
        in_specs=whole,
        out_specs=[pl.BlockSpec(memory_space=pltpu.VMEM)] * 2,
        scratch_shapes=[
            pltpu.VMEM((places, 48, PAIR), BF),
            pltpu.VMEM((places, 16, PAIR), BF),
            pltpu.VMEM((places, 16, PAIR), BF),
            pltpu.VMEM((2, tokens, 2 * PAIR), BF),
            pltpu.SemaphoreType.DMA((places,)),
            pltpu.SemaphoreType.DMA((places,)),
            pltpu.SemaphoreType.DMA((places,)),
            pltpu.SemaphoreType.DMA((places,)),
            pltpu.SemaphoreType.DMA((2,)),
            pltpu.SemaphoreType.DMA((2,)),
        ],
        compiler_params=pltpu.CompilerParams(collective_id=0, has_side_effects=True),
        name="exchange",
        cost_estimate=pl.CostEstimate(flops=10**9, bytes_accessed=2**21, transcendentals=0),
    )(
        messages, initial_state, reads, local_out, head_norm_gain[None], returned,
        jnp.cos(angles), jnp.sin(angles), query_sink_logit,
    )
    lin_weight, att_weight = turned_gather(
        (linear_output_weight, window_output_weight), SP_FS, (1, 1)
    )
    layer_out = sum_at_owner(
        jnp.dot(lin_mix, lin_weight, preferred_element_type=jnp.float32)
        + jnp.dot(outputs, att_weight, preferred_element_type=jnp.float32),
        "tp",
        0,
    )
    return layer_out.astype(jnp.bfloat16)[None]


def solution(mesh):
    finer = Mesh(
        mesh.devices.reshape(8, 4, mesh.shape["fs"], mesh.shape["tp"]), ("sp_0", "sp_1", "fs", "tp")
    )
    placed = (
        P("fs", SP, "tp"),
        P(),
        P(SP_FS, "tp"),
        P(SP_FS, "tp"),
        P(SP_FS, "tp"),
        P(SP_FS, "tp"),
        P(SP_FS, "tp"),
        P(SP_FS, "tp"),
        P(),
        P(),
        P(),
        P("fs", "tp", SP),
        P(),
        P(),
        P(),
        P(),
        P(),
        P(),
        P("tp", SP_FS),
        P("tp", SP_FS),
    )
    return jax.shard_map(
        local, mesh=finer, in_specs=placed, out_specs=P("fs", SP_TP, None), check_vma=False
    )
```

```python
import functools
import jax
import jax.numpy as jnp
from jax import lax
from jax.experimental import pallas as pl
from jax.experimental.pallas import tpu as pltpu

from jax.sharding import Mesh
from jax.sharding import PartitionSpec as P

HD = 64
CH = 64
PAIR = 128
WINDOW = 128
GRID_W = 64
ATT_BLOCK = 128
SP = ("sp_0", "sp_1")
FOUR = 4
SP_FS = ("sp_0", "sp_1", "fs")
SP_TP = ("sp_0", "sp_1", "tp")
NORM_EPS = 1e-06
GROUP_EPS = 0.00064
ROPE_BASE = 10000.0
F32 = jnp.float32
BF = jnp.bfloat16
MESSAGE = jnp.bfloat16
MESH = pl.DeviceIdType.MESH
NN = (((1,), (0,)), ((), ()))
NT = (((1,), (1,)), ((), ()))
TN = (((0,), (0,)), ((), ()))


def dot(a, b, dims=NN):
    return lax.dot_general(a, b, dims, preferred_element_type=F32)


def split2(a):
    high = a.astype(BF)
    return high, (a - high.astype(F32)).astype(BF)


def split3(a):
    high, rest = a.astype(BF), None
    rest = a - high.astype(F32)
    mid = rest.astype(BF)
    return high, mid, (rest - mid.astype(F32)).astype(BF)


def mm3(a, b, dims=NN):
    (ka,), (kb,) = dims[0]
    a_hi, a_lo = split2(a)
    b_hi, b_lo = split2(b)
    main = dot(
        jnp.concatenate([a_hi, a_lo], axis=ka), jnp.concatenate([b_hi, b_hi], axis=kb), dims
    )
    return main + dot(a_hi, b_lo, dims)


def mm2(a, b_exact, dims=NN):
    (ka,), (kb,) = dims[0]
    a_hi, a_lo = split2(a)
    return dot(
        jnp.concatenate([a_hi, a_lo], axis=ka), jnp.concatenate([b_exact, b_exact], axis=kb), dims
    )


def iota(shape, dim):
    return lax.broadcasted_iota(jnp.int32, shape, dim)


def ones_where(cond):
    return jnp.where(cond, 1.0, 0.0).astype(BF)


def ring_of_four(buf, out_sem, in_sem):
    me = lax.axis_index("fs")
    right, left, far = (me + 1) % FOUR, (me + 3) % FOUR, (me + 2) % FOUR
    half = buf.shape[1] // 2

    def piece(block, part, target, number):
        where = buf.at[block, part * half : (part + 1) * half]
        return pltpu.make_async_remote_copy(
            src_ref=where, dst_ref=where, send_sem=out_sem.at[number], recv_sem=in_sem.at[number],
            device_id={"fs": target}, device_id_type=MESH,
        )

    def start():
        piece(me, 0, right, 0).start()
        piece(me, 1, left, 1).start()
        piece(me, 1, right, 2).start()
        piece(me, 0, left, 3).start()

    def relay():
        piece(left, 0, right, 0).wait_recv()
        piece(left, 0, right, 4).start()
        piece(right, 1, left, 1).wait_recv()
        piece(right, 1, left, 5).start()

    def arrive_near():
        piece(left, 1, right, 2).wait_recv()
        piece(right, 0, left, 3).wait_recv()

    def arrive_far():
        piece(far, 0, right, 4).wait_recv()
        piece(far, 1, left, 5).wait_recv()

    def finish_sends():
        piece(me, 0, right, 0).wait_send()
        piece(me, 1, left, 1).wait_send()
        piece(me, 1, right, 2).wait_send()
        piece(me, 0, left, 3).wait_send()
        piece(left, 0, right, 4).wait_send()
        piece(right, 1, left, 5).wait_send()

    return start, relay, arrive_near, arrive_far, finish_sends


def front_kernel(
    x_ref, gain_ref, wr_ref, wk_ref, wv_ref, wq_ref, wak_ref, wav_ref,
    down_d_ref, down_e_ref, up_d_ref, up_e_ref, off_d_ref, off_e_ref, extra_ref,
    proj_ref, logd_ref, learn_ref,
    both_ref, hid_ref, stage_ref, cols_ref, ext_ref,
    x_out, x_in, hid_out, hid_in, stage_out, stage_in, ext_out, ext_in,
    z_out, z_in, near_out, near_in, far_out, far_in,
):
    z, x, f, c = (lax.axis_index(a) for a in ("sp_0", "sp_1", "fs", "tp"))
    nz, nx = lax.axis_size("sp_0"), lax.axis_size("sp_1")
    mine = z * nx + x
    rows = wr_ref.shape[0]
    barrier = pltpu.get_barrier_semaphore()
    peers = [{"fs": (f + k) % FOUR} for k in range(1, FOUR)] + [{"tp": 1 - c}]
    peers += [{"sp_0": (z + k) % nz} for k in (1, nz - 1)] + [{"sp_1": (x + k) % nx} for k in (1, nx - 1)]
    for peer in peers:
        pl.semaphore_signal(barrier, inc=1, device_id=peer, device_id_type=MESH)
    low = iota((rows, PAIR), 1) < HD
    keys, values = wak_ref[...].astype(F32), wav_ref[...].astype(F32)
    shared = [
        jnp.where(low, keys, pltpu.roll(values, HD, 1)).astype(BF),
        jnp.where(low, pltpu.roll(keys, HD, 1), values).astype(BF),
    ]
    for g in range(FOUR):
        lanes = slice(g * PAIR, (g + 1) * PAIR)
        for k, ref in enumerate((wr_ref, wk_ref, wv_ref, wq_ref)):
            stage_ref[g, :, k * PAIR : (k + 1) * PAIR] = ref[:, lanes]
        stage_ref[g, :, 4 * PAIR :] = shared[g // 2]
    both_ref[c] = x_ref[...]
    ext_ref[f] = extra_ref[0]
    my_rows = pl.ds(pl.multiple_of(f * rows, rows), rows)
    cols_ref[mine, my_rows, :] = stage_ref[f]
    pl.semaphore_wait(barrier, len(peers))

    half_copy = pltpu.make_async_remote_copy(
        src_ref=x_ref, dst_ref=both_ref.at[c], send_sem=x_out, recv_sem=x_in,
        device_id={"tp": 1 - c}, device_id_type=MESH,
    )
    half_copy.start()

    def stage_copy(k):
        g = (f + k) % FOUR
        return pltpu.make_async_remote_copy(
            src_ref=stage_ref.at[g], dst_ref=cols_ref.at[mine, my_rows, :],
            send_sem=stage_out.at[k], recv_sem=stage_in.at[k], device_id={"fs": g}, device_id_type=MESH,
        )

    def stage_arrival(k):
        g = (f + FOUR - k) % FOUR
        return pltpu.make_async_remote_copy(
            src_ref=stage_ref.at[g], dst_ref=cols_ref.at[mine, pl.ds(pl.multiple_of(g * rows, rows), rows), :],
            send_sem=stage_out.at[k], recv_sem=stage_in.at[k], device_id={"fs": g}, device_id_type=MESH,
        )

    def ext_copy(k, source):
        return pltpu.make_async_remote_copy(
            src_ref=extra_ref.at[0], dst_ref=ext_ref.at[source],
            send_sem=ext_out.at[k], recv_sem=ext_in.at[k], device_id={"fs": (f + k) % FOUR}, device_id_type=MESH,
        )

    for k in range(1, FOUR):
        stage_copy(k).start()

    def z_block(k):
        if k == 0:
            return z
        step = (k - 1) // 2
        return (z + nz - 1 - step) % nz if k % 2 else (z + 1 + step) % nz

    def z_copy(k_from, side, step):
        where = cols_ref.at[z_block(k_from) * nx + x]
        return pltpu.make_async_remote_copy(
            src_ref=where, dst_ref=where, send_sem=z_out.at[side, step], recv_sem=z_in.at[side, step],
            device_id={"sp_0": (z + (1 if side == 0 else nz - 1)) % nz}, device_id_type=MESH,
        )

    def near_copy(k, side, column):
        where = cols_ref.at[z_block(k) * nx + column]
        return pltpu.make_async_remote_copy(
            src_ref=where, dst_ref=where, send_sem=near_out.at[k, side], recv_sem=near_in.at[k, side],
            device_id={"sp_1": (x + (1 if side == 0 else nx - 1)) % nx}, device_id_type=MESH,
        )

    def far_copy(k, column):
        where = cols_ref.at[z_block(k) * nx + column]
        return pltpu.make_async_remote_copy(
            src_ref=where, dst_ref=where, send_sem=far_out.at[k], recv_sem=far_in.at[k],
            device_id={"sp_1": (x + (1 if k % 2 == 0 else nx - 1)) % nx}, device_id_type=MESH,
        )

    left, right, across = (x + nx - 1) % nx, (x + 1) % nx, (x + 2) % nx

    def spread(k):
        near_copy(k, 0, x).start()
        near_copy(k, 1, x).start()

    def pass_on(k):
        near_copy(k, 0, left).wait_recv()
        near_copy(k, 1, right).wait_recv()
        far_copy(k, left if k % 2 == 0 else right).start()

    for k in range(1, FOUR):
        stage_arrival(k).wait_recv()
    z_copy(0, 0, 0).start()
    z_copy(0, 1, 0).start()
    spread(0)

    half_copy.wait_recv()
    full = jnp.concatenate([both_ref[0], both_ref[1]], axis=1).astype(F32)
    scale = lax.rsqrt(jnp.mean(full * full, axis=-1, keepdims=True) + NORM_EPS)
    hid_ref[f] = (full * scale * gain_ref[...]).astype(BF)
    start, relay, arrive_near, arrive_far, finish_sends = ring_of_four(hid_ref, hid_out, hid_in)
    for k in range(1, FOUR):
        ext_copy(k, f).start()
    start()

    steps = nz // 2
    for step in range(steps):
        k = 2 * step + 1
        z_copy(k, 0, step).wait_recv()
        if step < steps - 1:
            z_copy(k, 0, step + 1).start()
        spread(k)
        if step < steps - 1:
            z_copy(k + 1, 1, step).wait_recv()
            if step < steps - 2:
                z_copy(k + 1, 1, step + 1).start()
            spread(k + 1)
        if step == 0:
            pass_on(0)
        else:
            pass_on(k - 2)
            pass_on(k - 1)
        if step == 1:
            relay()
    pass_on(nz - 1)
    arrive_near()
    arrive_far()
    for k in range(1, FOUR):
        ext_copy(k, (f + FOUR - k) % FOUR).wait_recv()

    tokens = hid_ref.shape[1]
    hidden = hid_ref[...].reshape(FOUR * tokens, hid_ref.shape[2])
    decay_low = dot(hidden, down_d_ref[...]).astype(BF)
    learn_low = dot(hidden, down_e_ref[...]).astype(BF)
    decay_act = jnp.tanh(decay_low.astype(F32)).astype(BF)
    heads = extra_ref.shape[1]
    first = c * heads * HD + f * PAIR
    chosen = pl.ds(pl.multiple_of(first, PAIR), PAIR)
    select = ones_where(iota((heads, PAIR), 0) == 2 * f + iota((heads, PAIR), 1) // HD).astype(F32)
    spikes = [
        lax.dot_general(
            ext_ref[p], select, TN, precision=lax.Precision.HIGHEST, preferred_element_type=F32
        )
        for p in range(FOUR)
    ]
    for d in range(2):
        pre = off_d_ref[d : d + 1, chosen] + dot(decay_act, up_d_ref[d, :, chosen])
        softplus = jnp.maximum(-pre, 0.0) + jnp.log1p(jnp.exp(-jnp.abs(pre)))
        rate = jnp.exp(-softplus - 0.5)
        learn = jax.nn.sigmoid(off_e_ref[d : d + 1, chosen] + dot(learn_low, up_e_ref[d, :, chosen]))
        for p in range(FOUR):
            part = slice(p * tokens, (p + 1) * tokens)
            logd_ref[d, p] = spikes[p] - rate[part]
            learn_ref[d, p] = learn[part]

    for k in range(nz):
        far_copy(k, across).wait_recv()
    depth = cols_ref.shape[0] * cols_ref.shape[1]
    for first_col, last_col in ((0, 256), (256, 512), (512, 640)):
        weight = cols_ref[:, :, first_col:last_col].reshape(depth, last_col - first_col)
        result = dot(hidden, weight).astype(BF)
        for p in range(FOUR):
            proj_ref[p, :, first_col:last_col] = result[p * tokens : (p + 1) * tokens]

    half_copy.wait_send()
    finish_sends()
    for k in range(1, FOUR):
        stage_copy(k).wait_send()
        ext_copy(k, f).wait_send()
    for step in range(steps):
        z_copy(0, 0, step).wait_send()
        if step < steps - 1:
            z_copy(0, 1, step).wait_send()
    for k in range(nz):
        near_copy(k, 0, x).wait_send()
        near_copy(k, 1, x).wait_send()
        far_copy(k, left).wait_send()


def stacked(x):
    low = iota(x.shape, 1) < HD
    return jnp.concatenate([jnp.where(low, x, 0.0), jnp.where(low, 0.0, x)], axis=0)


def unstacked(x):
    return x[:CH] + x[CH:]


def local_kernel(
    proj_ref, logd_ref, learn_ref, wout_ref, q_ref, o_ref, msg_ref, rows_ref,
    z_out, z_in, x_out, x_in,
):
    z, x = lax.axis_index("sp_0"), lax.axis_index("sp_1")
    nz, nx = lax.axis_size("sp_0"), lax.axis_size("sp_1")
    barrier = pltpu.get_barrier_semaphore()
    peers = [{"sp_0": (z + k) % nz} for k in range(1, nz)] + [{"sp_1": (x + k) % nx} for k in range(1, nx)]
    for peer in peers:
        pl.semaphore_signal(barrier, inc=1, device_id=peer, device_id_type=MESH)
    rows_ref[z, x] = wout_ref[...]
    pl.semaphore_wait(barrier, len(peers))

    def z_copy(k, source):
        return pltpu.make_async_remote_copy(
            src_ref=wout_ref, dst_ref=rows_ref.at[source, x], send_sem=z_out.at[k], recv_sem=z_in.at[k],
            device_id={"sp_0": (z + k) % nz}, device_id_type=MESH,
        )

    def x_copy(k, column):
        where = rows_ref.at[:, column]
        return pltpu.make_async_remote_copy(
            src_ref=where, dst_ref=where, send_sem=x_out.at[k], recv_sem=x_in.at[k],
            device_id={"sp_1": (x + k) % nx}, device_id_type=MESH,
        )

    for k in range(1, nz):
        z_copy(k, z).start()
    row = iota((2 * CH, 2 * CH), 0)
    col = iota((2 * CH, 2 * CH), 1)
    t, s = row % CH, col % CH
    eye = row == col
    same_head = ones_where(row // HD == col // HD)
    tri = [ones_where((iota((CH, CH), 0) >= iota((CH, CH), 1))), ones_where((iota((CH, CH), 0) <= iota((CH, CH), 1)))]
    strict = [t > s, t < s]
    within = [t >= s, t <= s]

    def one_pair(p, carry):
        @pl.when(p == FOUR // 2)
        def _():
            for k in range(1, nz):
                z_copy(k, (z + nz - k) % nz).wait_recv()
            for k in range(1, nx):
                x_copy(k, x).start()

        recept = proj_ref[p, :, :PAIR].astype(F32)
        keys = proj_ref[p, :, PAIR : 2 * PAIR].astype(F32)
        values = proj_ref[p, :, 2 * PAIR : 3 * PAIR].astype(F32)
        squares = mm2(keys * keys, same_head)
        unit = keys * lax.rsqrt(squares + NORM_EPS)
        jobs = [(d, c) for d in range(2) for c in range(2)]
        stage = {}
        for d, c in jobs:
            rows = slice(c * CH, (c + 1) * CH)
            logd = logd_ref[d, p, rows, :]
            parts = jnp.concatenate(split3(logd), axis=0)
            total = dot(jnp.concatenate([tri[d]] * 3, axis=1), parts)
            middle = total[CH // 2 - 1 : CH // 2] if d == 0 else total[CH // 2 : CH // 2 + 1]
            last = total[CH - 1 : CH] if d == 0 else total[0:1]
            grow = jnp.exp(total - middle)
            shrink = jnp.exp(middle - total)
            read = recept[rows] * grow
            mark = unit[rows] * jnp.exp(total - logd - middle)
            erase = unit[rows] * learn_ref[d, p, rows, :] * shrink
            key = keys[rows] * shrink
            read_s, mark_s, erase_s, key_s = map(stacked, (read, mark, erase, key))
            scores = mm3(
                jnp.concatenate([mark_s, read_s], axis=0),
                jnp.concatenate([erase_s, key_s], axis=0),
                NT,
            )
            stage[d, c] = (read, mark_s, erase_s, key_s, scores, jnp.exp(middle), jnp.exp(last - middle), jnp.exp(last))
        inverse = {}
        grams = {}
        for d, c in jobs:
            gram = jnp.where(strict[d], stage[d, c][4][: 2 * CH, : 2 * CH], 0.0)
            grams[d, c] = gram
            inverse[d, c] = jnp.where(eye, 1.0, 0.0) - jnp.where(t // 2 == s // 2, gram, 0.0)
        block = 2
        while block < CH:
            joins = (t // (2 * block) == s // (2 * block)) & (t // block != s // block)
            for job in jobs:
                found = inverse[job]
                inverse[job] = found - mm3(found, mm3(jnp.where(joins, grams[job], 0.0), found))
            block *= 2
        maps, reads, outs = {}, {}, {}
        for d, c in jobs:
            rows = slice(c * CH, (c + 1) * CH)
            read, mark_s, erase_s, key_s, scores, to_start, to_end, whole = stage[d, c]
            val_s = stacked(values[rows]).astype(BF)
            cross = jnp.where(strict[d], scores[: 2 * CH, 2 * CH :], 0.0)
            read_e = jnp.where(within[d], scores[2 * CH :, : 2 * CH], 0.0)
            read_k = jnp.where(within[d], scores[2 * CH :, 2 * CH :], 0.0)
            solved = mm3(inverse[d, c], jnp.concatenate([mark_s, mm2(cross, val_s)], axis=1))
            solved = jnp.concatenate([solved[:, :PAIR] * to_start, solved[:, PAIR:]], axis=1)
            taken = mm3(read_e, solved)
            reads[d, c] = read * to_start - unstacked(taken[:, :PAIR])
            outs[d, c] = unstacked(mm2(read_k, val_s) - taken[:, PAIR:])
            ended = mm3(solved, erase_s * to_end, TN)
            k_hi, k_lo = split2(key_s * to_end)
            added = dot(jnp.concatenate([val_s, val_s], axis=0), jnp.concatenate([k_hi, k_lo], axis=0), TN)
            prod = jnp.where(eye, whole - 1.0, 0.0) - ended[:PAIR]
            maps[d, c] = (prod, added - ended[PAIR:])
        out_rows = [outs[0, 0] + outs[1, 0], outs[0, 1] + outs[1, 1]]
        for d in range(2):
            first, second = (0, 1) if d == 0 else (1, 0)
            (prod1, add1), (prod2, add2) = maps[d, first], maps[d, second]
            both = jnp.concatenate([prod1, add1], axis=0)
            through = mm3(reads[d, second], both, NT)
            q_ref[d, p, first * CH : (first + 1) * CH, :] = reads[d, first]
            q_ref[d, p, second * CH : (second + 1) * CH, :] = reads[d, second] + through[:, :PAIR]
            out_rows[second] = out_rows[second] + through[:, PAIR:]
            joined = mm3(both, prod2)
            prod = prod1 + prod2 + joined[:PAIR]
            add = add1 + joined[PAIR:] + add2
            for hh in range(2):
                for half in range(2):
                    message = jnp.concatenate(
                        [
                            folded(prod, hh, hh * HD, HD // 2),
                            folded(add, hh, hh * HD + half * (HD // 2), HD // 4),
                        ],
                        axis=0,
                    )
                    msg_ref[d * 16 + p * 4 + hh * 2 + half] = message.astype(msg_ref.dtype)
        for c in range(2):
            o_ref[p, c * CH : (c + 1) * CH, :] = out_rows[c]
        return carry

    lax.fori_loop(0, FOUR, one_pair, 0)
    for k in range(1, nx):
        x_copy(k, (x + nx - k) % nx).wait_recv()
    for k in range(1, nz):
        z_copy(k, z).wait_send()
    for k in range(1, nx):
        x_copy(k, x).wait_send()


def folded(x, hh, first, count):
    upper, lower = x[first : first + count], x[first + count : first + 2 * count]
    if hh == 0:
        return upper + pltpu.roll(lower, HD, 1)
    return pltpu.roll(upper, HD, 1) + lower


def peer_id(index):
    inner = lax.axis_size("sp_1")
    return {"sp_0": index // inner, "sp_1": index % inner}


def exchange_kernel(
    msg_ref, init_ref, reads_ref, local_ref, gain_ref, proj_ref, cos_ref, sin_ref, sink_ref,
    mix_ref,
    recv_ref, sent_ref, enter_ref, halo_ref,
    out_sem, in_sem, back_out_sem, back_in_sem, halo_out_sem, halo_in_sem,
):
    count = recv_ref.shape[0]
    place = lax.axis_index("sp_0") * lax.axis_size("sp_1") + lax.axis_index("sp_1")
    kv_first = 4 * PAIR
    barrier = pltpu.get_barrier_semaphore()

    def greet(k, carry):
        pl.semaphore_signal(barrier, inc=1, device_id=peer_id((place + k) % count), device_id_type=MESH)
        return carry

    lax.fori_loop(1, count, greet, 0)
    pl.semaphore_wait(barrier, count - 1)

    def halo_copy(side):
        target = (place + count - 1 + 2 * side) % count
        return pltpu.make_async_remote_copy(
            src_ref=proj_ref.at[:, :, kv_first : kv_first + PAIR],
            dst_ref=halo_ref.at[1 - side],
            send_sem=halo_out_sem.at[side],
            recv_sem=halo_in_sem.at[1 - side],
            device_id=peer_id(target),
            device_id_type=MESH,
        )

    def map_copy(target):
        return pltpu.make_async_remote_copy(
            src_ref=msg_ref.at[target],
            dst_ref=recv_ref.at[place],
            send_sem=out_sem.at[target],
            recv_sem=in_sem.at[place],
            device_id=peer_id(target),
            device_id_type=MESH,
        )

    def map_arrival(source):
        return pltpu.make_async_remote_copy(
            src_ref=msg_ref.at[source],
            dst_ref=recv_ref.at[source],
            send_sem=out_sem.at[source],
            recv_sem=in_sem.at[source],
            device_id=peer_id(source),
            device_id_type=MESH,
        )

    def entry_copy(target):
        return pltpu.make_async_remote_copy(
            src_ref=sent_ref.at[target],
            dst_ref=enter_ref.at[place],
            send_sem=back_out_sem.at[target],
            recv_sem=back_in_sem.at[place],
            device_id=peer_id(target),
            device_id_type=MESH,
        )

    def entry_arrival(source):
        return pltpu.make_async_remote_copy(
            src_ref=sent_ref.at[source],
            dst_ref=enter_ref.at[source],
            send_sem=back_out_sem.at[source],
            recv_sem=back_in_sem.at[source],
            device_id=peer_id(source),
            device_id_type=MESH,
        )

    halo_copy(0).start()
    halo_copy(1).start()

    def send_map(k, carry):
        map_copy((place + k) % count).start()
        return carry

    lax.fori_loop(1, count, send_map, 0)
    recv_ref[place] = msg_ref[place]

    tokens = local_ref.shape[1]
    for side in range(2):
        halo_copy(side).wait()
    lane = iota((1, PAIR), 1)
    low = lane < HD
    front = lane % 32 < 16

    def turned(v, first, last):
        other = jnp.where(front, -pltpu.roll(v, PAIR - 16, 1), pltpu.roll(v, 16, 1))
        return v * cos_ref[first:last, :] + other * sin_ref[first:last, :]

    reach = 3 * tokens
    q_pos = place * tokens + iota((2 * tokens, reach), 0) % tokens
    k_pos = (place - 1) * tokens + iota((2 * tokens, reach), 1)
    allowed = (jnp.abs(q_pos - k_pos) <= WINDOW) & (k_pos >= 0) & (k_pos < count * tokens)
    upper = iota((2 * tokens, 1), 0) < tokens
    pair = lax.axis_index("fs")
    first_head = lax.axis_index("tp") * (2 * FOUR) + 2 * pair
    sink = jnp.where(upper, sink_ref[first_head], sink_ref[first_head + 1])

    def attend(p, carry):
        kv = jnp.concatenate(
            [halo_ref[0, p], proj_ref[p, :, kv_first : kv_first + PAIR], halo_ref[1, p]], axis=0
        ).astype(F32)
        roped = turned(kv, 0, reach)
        swapped = pltpu.roll(kv, HD, 1)
        key = jnp.where(low, roped, pltpu.roll(roped, HD, 1)).astype(BF)
        value = jnp.where(low, swapped, kv).astype(BF)
        query = turned(proj_ref[p, :, kv_first - PAIR : kv_first].astype(F32), tokens, 2 * tokens)
        query = jnp.concatenate([jnp.where(low, query, 0.0), jnp.where(low, 0.0, query)], axis=0)
        scores = dot(query.astype(BF), key, NT) * HD**-0.5
        scores = jnp.where(allowed, scores, -jnp.inf)
        top = jnp.maximum(jnp.max(scores, axis=-1, keepdims=True), sink)
        raised = jnp.exp(scores - top)
        total = jnp.exp(sink - top) + jnp.sum(raised, axis=-1, keepdims=True)
        mixed = dot((raised / total).astype(BF), value)
        mix_ref[p, :, PAIR:] = jnp.where(low, mixed[:tokens], mixed[tokens:]).astype(BF)
        return carry

    lax.fori_loop(0, FOUR, attend, 0)

    def await_map(k, carry):
        map_arrival((place + k) % count).wait()
        return carry

    lax.fori_loop(1, count, await_map, 0)

    unit_idx = place // 2
    direction, half = unit_idx // 8, place % 2
    rows = HD // 2
    quarter = rows // 2
    start = pl.multiple_of(half * rows, rows)

    def unfolded(x):
        return jnp.concatenate([x[:, :HD], x[:, HD:]], axis=0)

    def nth(step):
        return direction * (count - 1) + step * (1 - 2 * direction)

    def advance(step, state):
        idx = nth(step)
        sent_ref[idx] = jnp.concatenate([state[:quarter], state[quarter:]], axis=1).astype(BF)
        before = nth(step - 1)

        @pl.when((step > 0) & (before != place))
        def _():
            entry_copy(before).start()

        message = recv_ref[idx].astype(F32)
        return state + mm3(state, unfolded(message[:rows])) + unfolded(message[rows:])

    state = init_ref[direction, first_head + unit_idx % 2, pl.ds(start, rows), :]
    lax.fori_loop(0, count, advance, state)
    final = nth(count - 1)
    enter_ref[place] = sent_ref[place]

    @pl.when(final != place)
    def _():
        entry_copy(final).start()

    def await_entry(k, carry):
        entry_arrival((place + k) % count).wait()
        return carry

    lax.fori_loop(1, count, await_entry, 0)
    finish(reads_ref, local_ref, enter_ref, gain_ref, mix_ref)


def finish(q_ref, o_ref, enter_ref, gain_ref, mix_ref):
    row = iota((PAIR, PAIR), 0)
    col = iota((PAIR, PAIR), 1)
    same_head = ones_where(row // HD == col // HD)
    low = iota((HD // 4, PAIR), 1) < HD
    start = (lax.axis_index("tp") * FOUR + lax.axis_index("fs")) * PAIR
    gain = gain_ref[:, pl.ds(pl.multiple_of(start, PAIR), PAIR)]
    for p in range(FOUR):
        out = o_ref[p]
        for d in range(2):
            pieces = []
            for hh in range(2):
                for half in range(2):
                    m = enter_ref[d * 16 + p * 4 + hh * 2 + half].astype(F32)
                    turned = pltpu.roll(m, HD, 1)
                    if hh == 0:
                        pieces += [jnp.where(low, m, 0.0), jnp.where(low, turned, 0.0)]
                    else:
                        pieces += [jnp.where(low, 0.0, turned), jnp.where(low, 0.0, m)]
            out = out + mm2(q_ref[d, p], jnp.concatenate(pieces, axis=0).astype(BF), NT)
        centred = out - mm2(out, same_head) * (1.0 / HD)
        spread = mm2(centred * centred, same_head) * (1.0 / HD)
        mix_ref[p, :, :PAIR] = (centred * lax.rsqrt(spread + GROUP_EPS) * gain).astype(BF)


def out_kernel(
    mix_ref, rows_ref, out_ref, all_ref, total_ref, other_ref, ready_ref, got_ref,
    mix_out, mix_in, half_out, half_in, back_out, back_in,
):
    f, c = lax.axis_index("fs"), lax.axis_index("tp")
    tokens = mix_ref.shape[1]
    barrier = pltpu.get_barrier_semaphore()
    peers = [{"fs": (f + k) % FOUR} for k in range(1, FOUR)] + [{"tp": 1 - c}]
    for peer in peers:
        pl.semaphore_signal(barrier, inc=1, device_id=peer, device_id_type=MESH)
    all_ref[f] = mix_ref[...]
    pl.semaphore_wait(barrier, len(peers))
    start, relay, arrive_near, arrive_far, finish_sends = ring_of_four(all_ref, mix_out, mix_in)
    start()
    columns = total_ref.shape[2]
    weight_rows = rows_ref.shape[0] * rows_ref.shape[1] * rows_ref.shape[2]

    def product(g):
        weight = rows_ref[:, :, :, pl.ds(pl.multiple_of(g * 2 * PAIR, 2 * PAIR), 2 * PAIR)]
        left = all_ref[g].reshape(FOUR * tokens, 2 * PAIR)
        return dot(left, weight.reshape(weight_rows, 2 * PAIR), NT).reshape(FOUR, tokens, columns)

    total_ref[...] = product(f)
    relay()
    arrive_near()
    total_ref[...] += product((f + 1) % FOUR) + product((f + 3) % FOUR)
    arrive_far()
    total_ref[...] += product((f + 2) % FOUR)
    half = tokens // 2
    theirs = pl.ds(pl.multiple_of((1 - c) * half, half), half)
    ours = pl.ds(pl.multiple_of(c * half, half), half)
    half_copy = pltpu.make_async_remote_copy(
        src_ref=total_ref.at[:, theirs, :], dst_ref=other_ref, send_sem=half_out, recv_sem=half_in,
        device_id={"tp": 1 - c}, device_id_type=MESH,
    )
    half_copy.start()
    half_copy.wait_recv()
    ready_ref[...] = (total_ref[:, ours, :] + other_ref[...]).astype(BF)

    def back_copy(k, source):
        g = (f + k) % FOUR
        return pltpu.make_async_remote_copy(
            src_ref=ready_ref.at[g], dst_ref=got_ref.at[source], send_sem=back_out.at[k], recv_sem=back_in.at[k],
            device_id={"fs": g}, device_id_type=MESH,
        )

    for k in range(1, FOUR):
        back_copy(k, f).start()
    got_ref[f] = ready_ref[f]
    finish_sends()
    half_copy.wait_send()
    wide = FOUR * PAIR
    source, target = iota((wide, wide), 0), iota((wide, wide), 1)
    place = source % PAIR // 16 * (FOUR * 16) + source // PAIR * 16 + source % 16
    shuffle = ones_where(place == target)
    for k in range(1, FOUR):
        back_copy(k, (f + FOUR - k) % FOUR).wait_recv()
    for b in range(columns // PAIR):
        lanes = slice(b * PAIR, (b + 1) * PAIR)
        joined = jnp.concatenate([got_ref[g, :, lanes] for g in range(FOUR)], axis=1)
        out_ref[:, b * wide : (b + 1) * wide] = dot(joined, shuffle).astype(BF)
    for k in range(1, FOUR):
        back_copy(k, f).wait_send()


def local(
    inputs, input_norm_gain, receptance_weight, linear_key_weight, linear_value_weight,
    window_query_weight, window_key_weight, window_value_weight, decay_down_weight, decay_up_weight,
    decay_offset, decay_log_extra, erasure_down_weight, erasure_up_weight, erasure_offset,
    initial_state, head_norm_gain, query_sink_logit, linear_output_weight, window_output_weight,
):
    tokens, model = inputs.shape[1], 2 * inputs.shape[2]
    places = lax.axis_size(SP)
    nz, nx = lax.axis_size("sp_0"), lax.axis_size("sp_1")
    offset = lax.axis_index(SP) * tokens
    rows = receptance_weight.shape[0]
    out_rows = linear_output_weight.shape[1]
    vmem = pl.BlockSpec(memory_space=pltpu.VMEM)
    dma = pltpu.SemaphoreType.DMA

    def params(number):
        return pltpu.CompilerParams(
            collective_id=number, has_side_effects=True, vmem_limit_bytes=48 * 2**20
        )

    proj, logd, learn = pl.pallas_call(
        front_kernel,
        out_shape=[
            jax.ShapeDtypeStruct((FOUR, tokens, 5 * PAIR), BF),
            jax.ShapeDtypeStruct((2, FOUR, tokens, PAIR), F32),
            jax.ShapeDtypeStruct((2, FOUR, tokens, PAIR), F32),
        ],
        in_specs=[vmem] * 15,
        out_specs=[vmem] * 3,
        scratch_shapes=[
            pltpu.VMEM((2, tokens, model // 2), BF),
            pltpu.VMEM((FOUR, tokens, model), BF),
            pltpu.VMEM((FOUR, rows, 5 * PAIR), BF),
            pltpu.VMEM((places, FOUR * rows, 5 * PAIR), BF),
            pltpu.VMEM((FOUR, *decay_log_extra.shape[1:]), F32),
            dma, dma, dma((6,)), dma((6,)), dma((FOUR,)), dma((FOUR,)), dma((FOUR,)), dma((FOUR,)),
            dma((2, nz // 2)), dma((2, nz // 2)), dma((nz, 2)), dma((nz, 2)), dma((nz,)), dma((nz,)),
        ],
        compiler_params=params(1),
        name="front",
        cost_estimate=pl.CostEstimate(flops=10**9, bytes_accessed=2**21, transcendentals=0),
    )(
        inputs[0], input_norm_gain[None], receptance_weight, linear_key_weight, linear_value_weight,
        window_query_weight, window_key_weight, window_value_weight, decay_down_weight,
        erasure_down_weight, decay_up_weight, erasure_up_weight, decay_offset, erasure_offset,
        decay_log_extra,
    )
    both = jnp.stack([linear_output_weight, window_output_weight])
    both = both.reshape(2, FOUR, PAIR, out_rows)
    out_weight = jnp.transpose(both, (3, 1, 0, 2)).reshape(out_rows, 2 * FOUR * PAIR)
    reads, local_out, messages, weight_rows = pl.pallas_call(
        local_kernel,
        out_shape=[
            jax.ShapeDtypeStruct((2, FOUR, tokens, PAIR), F32),
            jax.ShapeDtypeStruct((FOUR, tokens, PAIR), F32),
            jax.ShapeDtypeStruct((places, 48, PAIR), BF),
            jax.ShapeDtypeStruct((nz, nx, *out_weight.shape), BF),
        ],
        in_specs=[vmem] * 4,
        out_specs=[vmem] * 4,
        scratch_shapes=[dma((nz,)), dma((nz,)), dma((nx,)), dma((nx,))],
        compiler_params=params(2),
        name="local_maps",
        cost_estimate=pl.CostEstimate(flops=10**9, bytes_accessed=2**21, transcendentals=0),
    )(proj, logd, learn, out_weight)
    angle_pos = offset - WINDOW + jnp.arange(tokens + 2 * WINDOW, dtype=jnp.int32)
    inverse = ROPE_BASE ** (-jnp.arange(HD // 4, dtype=jnp.float32) / (HD // 4))
    row_angles = (angle_pos // GRID_W).astype(F32)[:, None] * inverse[None, :]
    col_angles = (angle_pos % GRID_W).astype(F32)[:, None] * inverse[None, :]
    angles = jnp.concatenate([row_angles, row_angles, col_angles, col_angles] * 2, axis=1)
    mix = pl.pallas_call(
        exchange_kernel,
        out_shape=jax.ShapeDtypeStruct((FOUR, tokens, 2 * PAIR), BF),
        in_specs=[vmem] * 8 + [pl.BlockSpec(memory_space=pltpu.SMEM)],
        out_specs=vmem,
        scratch_shapes=[
            pltpu.VMEM((places, 48, PAIR), BF),
            pltpu.VMEM((places, 16, PAIR), BF),
            pltpu.VMEM((places, 16, PAIR), BF),
            pltpu.VMEM((2, FOUR, tokens, PAIR), BF),
            dma((places,)), dma((places,)), dma((places,)), dma((places,)), dma((2,)), dma((2,)),
        ],
        compiler_params=params(3),
        name="exchange",
        cost_estimate=pl.CostEstimate(flops=10**9, bytes_accessed=2**21, transcendentals=0),
    )(
        messages, initial_state, reads, local_out, head_norm_gain[None], proj,
        jnp.cos(angles), jnp.sin(angles), query_sink_logit,
    )
    columns = places * out_rows
    out = pl.pallas_call(
        out_kernel,
        out_shape=jax.ShapeDtypeStruct((tokens // 2, FOUR * columns), BF),
        in_specs=[vmem] * 2,
        out_specs=vmem,
        scratch_shapes=[
            pltpu.VMEM((FOUR, FOUR, tokens, 2 * PAIR), BF),
            pltpu.VMEM((FOUR, tokens, columns), F32),
            pltpu.VMEM((FOUR, tokens // 2, columns), F32),
            pltpu.VMEM((FOUR, tokens // 2, columns), BF),
            pltpu.VMEM((FOUR, tokens // 2, columns), BF),
            dma((6,)), dma((6,)), dma, dma, dma((FOUR,)), dma((FOUR,)),
        ],
        compiler_params=params(4),
        name="project_out",
        cost_estimate=pl.CostEstimate(flops=10**9, bytes_accessed=2**21, transcendentals=0),
    )(mix, weight_rows)
    return out[None]


def solution(mesh):
    finer = Mesh(
        mesh.devices.reshape(8, 4, mesh.shape["fs"], mesh.shape["tp"]), ("sp_0", "sp_1", "fs", "tp")
    )
    placed = (
        P("fs", SP, "tp"),
        P(),
        P(SP_FS, "tp"),
        P(SP_FS, "tp"),
        P(SP_FS, "tp"),
        P(SP_FS, "tp"),
        P(SP_FS, "tp"),
        P(SP_FS, "tp"),
        P(),
        P(),
        P(),
        P("fs", "tp", SP),
        P(),
        P(),
        P(),
        P(),
        P(),
        P(),
        P("tp", SP_FS),
        P("tp", SP_FS),
    )
    return jax.shard_map(
        local, mesh=finer, in_specs=placed, out_specs=P("fs", SP_TP, None), check_vma=False
    )
```

```python
import math
import functools
import jax
import jax.numpy as jnp
from jax import lax
from jax.experimental import pallas as pl
from jax.experimental.pallas import tpu as pltpu

from jax.sharding import Mesh
from jax.sharding import PartitionSpec as P

HD = 64
CH = 64
PAIR = 128
WINDOW = 128
GRID_W = 64
ATT_BLOCK = 128
SP = ("sp_0", "sp_1")
FOUR = 4
SP_FS = ("sp_0", "sp_1", "fs")
SP_TP = ("sp_0", "sp_1", "tp")
NORM_EPS = 1e-06
GROUP_EPS = 0.00064
ROPE_BASE = 10000.0
F32 = jnp.float32
BF = jnp.bfloat16
MESSAGE = jnp.bfloat16
MESH = pl.DeviceIdType.MESH
NN = (((1,), (0,)), ((), ()))
NT = (((1,), (1,)), ((), ()))
TN = (((0,), (0,)), ((), ()))


def dot(a, b, dims=NN):
    return lax.dot_general(a, b, dims, preferred_element_type=F32)


def split2(a):
    high = a.astype(BF)
    return high, (a - high.astype(F32)).astype(BF)


def split3(a):
    high, rest = a.astype(BF), None
    rest = a - high.astype(F32)
    mid = rest.astype(BF)
    return high, mid, (rest - mid.astype(F32)).astype(BF)


def mm3(a, b, dims=NN):
    (ka,), (kb,) = dims[0]
    a_hi, a_lo = split2(a)
    b_hi, b_lo = split2(b)
    free = 1 - kb
    if b.shape[free] == PAIR:
        upper = jnp.concatenate([b_hi, b_lo], axis=free)
        lower = jnp.concatenate([b_hi, jnp.zeros_like(b_lo)], axis=free)
        wide = dot(
            jnp.concatenate([a_hi, a_lo], axis=ka), jnp.concatenate([upper, lower], axis=kb), dims
        )
        return wide[:, :PAIR] + wide[:, PAIR:]
    main = dot(
        jnp.concatenate([a_hi, a_lo], axis=ka), jnp.concatenate([b_hi, b_hi], axis=kb), dims
    )
    return main + dot(a_hi, b_lo, dims)


def mm2(a, b_exact, dims=NN):
    (ka,), (kb,) = dims[0]
    a_hi, a_lo = split2(a)
    return dot(
        jnp.concatenate([a_hi, a_lo], axis=ka), jnp.concatenate([b_exact, b_exact], axis=kb), dims
    )


def iota(shape, dim):
    return lax.broadcasted_iota(jnp.int32, shape, dim)


def ones_where(cond):
    return jnp.where(cond, 1.0, 0.0).astype(BF)


def ring_of_four(buf, out_sem, in_sem):
    me = lax.axis_index("fs")
    right, left, far = (me + 1) % FOUR, (me + 3) % FOUR, (me + 2) % FOUR
    half = buf.shape[1] // 2

    def piece(block, part, target, number):
        where = buf.at[block, part * half : (part + 1) * half]
        return pltpu.make_async_remote_copy(
            src_ref=where, dst_ref=where, send_sem=out_sem.at[number], recv_sem=in_sem.at[number],
            device_id={"fs": target}, device_id_type=MESH,
        )

    def start():
        piece(me, 0, right, 0).start()
        piece(me, 1, left, 1).start()
        piece(me, 1, right, 2).start()
        piece(me, 0, left, 3).start()

    def relay():
        piece(left, 0, right, 0).wait_recv()
        piece(left, 0, right, 4).start()
        piece(right, 1, left, 1).wait_recv()
        piece(right, 1, left, 5).start()

    def arrive_near():
        piece(left, 1, right, 2).wait_recv()
        piece(right, 0, left, 3).wait_recv()

    def arrive_far():
        piece(far, 0, right, 4).wait_recv()
        piece(far, 1, left, 5).wait_recv()

    def finish_sends():
        piece(me, 0, right, 0).wait_send()
        piece(me, 1, left, 1).wait_send()
        piece(me, 1, right, 2).wait_send()
        piece(me, 0, left, 3).wait_send()
        piece(left, 0, right, 4).wait_send()
        piece(right, 1, left, 5).wait_send()

    return start, relay, arrive_near, arrive_far, finish_sends


def peer_id(index):
    inner = lax.axis_size("sp_1")
    return {"sp_0": index // inner, "sp_1": index % inner}


def meet(place_of):
    z, x, f, c = place_of
    nz, nx = lax.axis_size("sp_0"), lax.axis_size("sp_1")
    count = nz * nx
    barrier = pltpu.get_barrier_semaphore()
    for k in range(1, FOUR):
        pl.semaphore_signal(barrier, inc=1, device_id={"fs": (f + k) % FOUR}, device_id_type=MESH)
    pl.semaphore_signal(barrier, inc=1, device_id={"tp": 1 - c}, device_id_type=MESH)

    def greet(k, carry):
        pl.semaphore_signal(barrier, inc=1, device_id=peer_id((z * nx + x + k) % count), device_id_type=MESH)
        return carry

    lax.fori_loop(1, count, greet, 0)
    pl.semaphore_wait(barrier, count - 1 + FOUR)


def rope_tables(place, cos_ref, sin_ref):
    reach = cos_ref.shape[0]
    block = reach // 3
    spot = iota((reach, PAIR), 0)
    lane = iota((reach, PAIR), 1)
    grid_row = ((place - 1) * (block // GRID_W) + spot // GRID_W).astype(F32)
    grid_col = (spot % GRID_W).astype(F32)
    power = (lane % 16).astype(F32) * (1.0 / 16)
    angle = jnp.where(lane % HD < HD // 2, grid_row, grid_col) * jnp.exp(power * -math.log(ROPE_BASE))
    cos_ref[...] = jnp.cos(angle)
    sin_ref[...] = jnp.sin(angle)


def front(refs, place_of):
    (
        x_ref, gain_ref, wr_ref, wk_ref, wv_ref, wq_ref, wak_ref, wav_ref, down_d_ref, down_e_ref,
        up_d_ref, up_e_ref, off_d_ref, off_e_ref, extra_ref, proj_ref, logd_ref, learn_ref,
        both_ref, hid_ref, stage_ref, cols_ref, ext_ref, load_sem,
        x_out, x_in, hid_out, hid_in, stage_out, stage_in, ext_out, ext_in,
        z_out, z_in, near_out, near_in, far_out, far_in, cos_ref, sin_ref, late,
    ) = refs
    z, x, f, c = place_of
    nz, nx = lax.axis_size("sp_0"), lax.axis_size("sp_1")
    mine = z * nx + x
    rows = wr_ref.shape[0]
    loads = []
    for g in range(FOUR):
        for k, ref in enumerate((wr_ref, wk_ref, wv_ref, wq_ref)):
            loads.append((ref.at[:, g * PAIR : (g + 1) * PAIR], stage_ref.at[g, :, k * PAIR : (k + 1) * PAIR]))
    loads.append((x_ref, both_ref.at[c]))
    loads.append((extra_ref.at[0], ext_ref.at[f]))
    loads = [
        pltpu.make_async_copy(start, end, load_sem.at[number]) for number, (start, end) in enumerate(loads)
    ]
    for load in loads:
        load.start()
    for load in late:
        load.start()
    low = iota((rows, PAIR), 1) < HD
    keys, values = wak_ref[...].astype(F32), wav_ref[...].astype(F32)
    shared = [
        jnp.where(low, keys, pltpu.roll(values, HD, 1)).astype(BF),
        jnp.where(low, pltpu.roll(keys, HD, 1), values).astype(BF),
    ]
    for g in range(FOUR):
        stage_ref[g, :, 4 * PAIR :] = shared[g // 2]
    for load in loads:
        load.wait()
    my_rows = pl.ds(pl.multiple_of(f * rows, rows), rows)
    cols_ref[mine, my_rows, :] = stage_ref[f]
    meet(place_of)

    half_copy = pltpu.make_async_remote_copy(
        src_ref=both_ref.at[c], dst_ref=both_ref.at[c], send_sem=x_out, recv_sem=x_in,
        device_id={"tp": 1 - c}, device_id_type=MESH,
    )
    half_copy.start()

    def stage_copy(k):
        g = (f + k) % FOUR
        return pltpu.make_async_remote_copy(
            src_ref=stage_ref.at[g], dst_ref=cols_ref.at[mine, my_rows, :],
            send_sem=stage_out.at[k], recv_sem=stage_in.at[k], device_id={"fs": g}, device_id_type=MESH,
        )

    def stage_arrival(k):
        g = (f + FOUR - k) % FOUR
        return pltpu.make_async_remote_copy(
            src_ref=stage_ref.at[g], dst_ref=cols_ref.at[mine, pl.ds(pl.multiple_of(g * rows, rows), rows), :],
            send_sem=stage_out.at[k], recv_sem=stage_in.at[k], device_id={"fs": g}, device_id_type=MESH,
        )

    def ext_copy(k, source):
        return pltpu.make_async_remote_copy(
            src_ref=ext_ref.at[source], dst_ref=ext_ref.at[source],
            send_sem=ext_out.at[k], recv_sem=ext_in.at[k], device_id={"fs": (f + k) % FOUR}, device_id_type=MESH,
        )

    for k in range(1, FOUR):
        stage_copy(k).start()

    def z_block(k):
        if k == 0:
            return z
        step = (k - 1) // 2
        return (z + nz - 1 - step) % nz if k % 2 else (z + 1 + step) % nz

    def z_copy(k_from, side, step):
        where = cols_ref.at[z_block(k_from) * nx + x]
        return pltpu.make_async_remote_copy(
            src_ref=where, dst_ref=where, send_sem=z_out.at[side, step], recv_sem=z_in.at[side, step],
            device_id={"sp_0": (z + (1 if side == 0 else nz - 1)) % nz}, device_id_type=MESH,
        )

    def near_copy(k, side, column):
        where = cols_ref.at[z_block(k) * nx + column]
        return pltpu.make_async_remote_copy(
            src_ref=where, dst_ref=where, send_sem=near_out.at[k, side], recv_sem=near_in.at[k, side],
            device_id={"sp_1": (x + (1 if side == 0 else nx - 1)) % nx}, device_id_type=MESH,
        )

    def far_copy(k, column):
        where = cols_ref.at[z_block(k) * nx + column]
        return pltpu.make_async_remote_copy(
            src_ref=where, dst_ref=where, send_sem=far_out.at[k], recv_sem=far_in.at[k],
            device_id={"sp_1": (x + (1 if k % 2 == 0 else nx - 1)) % nx}, device_id_type=MESH,
        )

    left, right, across = (x + nx - 1) % nx, (x + 1) % nx, (x + 2) % nx

    def spread(k):
        near_copy(k, 0, x).start()
        near_copy(k, 1, x).start()

    def pass_on(k):
        near_copy(k, 0, left).wait_recv()
        near_copy(k, 1, right).wait_recv()
        far_copy(k, left if k % 2 == 0 else right).start()

    for k in range(1, FOUR):
        stage_arrival(k).wait_recv()
    z_copy(0, 0, 0).start()
    z_copy(0, 1, 0).start()
    spread(0)

    half_copy.wait_recv()
    full = jnp.concatenate([both_ref[0], both_ref[1]], axis=1).astype(F32)
    scale = lax.rsqrt(jnp.mean(full * full, axis=-1, keepdims=True) + NORM_EPS)
    hid_ref[f] = (full * scale * gain_ref[...]).astype(BF)
    start, relay, arrive_near, arrive_far, finish_sends = ring_of_four(hid_ref, hid_out, hid_in)
    for k in range(1, FOUR):
        ext_copy(k, f).start()
    start()
    rope_tables(mine, cos_ref, sin_ref)

    steps = nz // 2
    for step in range(steps):
        k = 2 * step + 1
        z_copy(k, 0, step).wait_recv()
        if step < steps - 1:
            z_copy(k, 0, step + 1).start()
        spread(k)
        if step < steps - 1:
            z_copy(k + 1, 1, step).wait_recv()
            if step < steps - 2:
                z_copy(k + 1, 1, step + 1).start()
            spread(k + 1)
        if step == 0:
            pass_on(0)
        else:
            pass_on(k - 2)
            pass_on(k - 1)
        if step == 1:
            relay()
    pass_on(nz - 1)
    arrive_near()
    arrive_far()
    for k in range(1, FOUR):
        ext_copy(k, (f + FOUR - k) % FOUR).wait_recv()

    for load in late:
        load.wait()
    tokens = hid_ref.shape[1]
    hidden = hid_ref[...].reshape(FOUR * tokens, hid_ref.shape[2])
    decay_low = dot(hidden, down_d_ref[...], NT).astype(BF)
    learn_low = dot(hidden, down_e_ref[...], NT).astype(BF)
    decay_act = jnp.tanh(decay_low.astype(F32)).astype(BF)
    heads = ext_ref.shape[1]
    first = c * heads * HD + f * PAIR
    chosen = pl.ds(pl.multiple_of(first, PAIR), PAIR)
    select = ones_where(iota((heads, PAIR), 0) == 2 * f + iota((heads, PAIR), 1) // HD).astype(F32)
    spikes = [
        lax.dot_general(
            ext_ref[p], select, TN, precision=lax.Precision.HIGHEST, preferred_element_type=F32
        )
        for p in range(FOUR)
    ]
    for d in range(2):
        pre = off_d_ref[d : d + 1, chosen] + dot(decay_act, up_d_ref[d, :, chosen])
        softplus = jnp.maximum(-pre, 0.0) + jnp.log1p(jnp.exp(-jnp.abs(pre)))
        rate = jnp.exp(-softplus - 0.5)
        learn = jax.nn.sigmoid(off_e_ref[d : d + 1, chosen] + dot(learn_low, up_e_ref[d, :, chosen]))
        for p in range(FOUR):
            part = slice(p * tokens, (p + 1) * tokens)
            logd_ref[d, p] = spikes[p] - rate[part]
            learn_ref[d, p] = learn[part]

    for k in range(nz):
        far_copy(k, across).wait_recv()
    depth = cols_ref.shape[0] * cols_ref.shape[1]
    for first_col, last_col in ((0, 256), (256, 512), (512, 640)):
        weight = cols_ref[:, :, first_col:last_col].reshape(depth, last_col - first_col)
        result = dot(hidden, weight).astype(BF)
        for p in range(FOUR):
            proj_ref[p, :, first_col:last_col] = result[p * tokens : (p + 1) * tokens]

    half_copy.wait_send()
    finish_sends()
    for k in range(1, FOUR):
        stage_copy(k).wait_send()
        ext_copy(k, f).wait_send()
    for step in range(steps):
        z_copy(0, 0, step).wait_send()
        if step < steps - 1:
            z_copy(0, 1, step).wait_send()
    for k in range(nz):
        near_copy(k, 0, x).wait_send()
        near_copy(k, 1, x).wait_send()
        far_copy(k, left).wait_send()


def stacked(x):
    low = iota(x.shape, 1) < HD
    return jnp.concatenate([jnp.where(low, x, 0.0), jnp.where(low, 0.0, x)], axis=0)


def unstacked(x):
    return x[:CH] + x[CH:]


def local_maps(refs, place_of, send_halo, send_maps):
    proj_ref, logd_ref, learn_ref, wout_ref, q_ref, o_ref, msg_ref, rows_ref, z_out, z_in, x_out, x_in = refs
    z, x = place_of[:2]
    nz, nx = lax.axis_size("sp_0"), lax.axis_size("sp_1")
    rows_ref[z, x] = wout_ref[...]

    def z_copy(k, source):
        return pltpu.make_async_remote_copy(
            src_ref=wout_ref, dst_ref=rows_ref.at[source, x], send_sem=z_out.at[k], recv_sem=z_in.at[k],
            device_id={"sp_0": (z + k) % nz}, device_id_type=MESH,
        )

    def x_copy(k, column):
        where = rows_ref.at[:, column]
        return pltpu.make_async_remote_copy(
            src_ref=where, dst_ref=where, send_sem=x_out.at[k], recv_sem=x_in.at[k],
            device_id={"sp_1": (x + k) % nx}, device_id_type=MESH,
        )

    for k in range(1, nz):
        z_copy(k, z).start()
    row = iota((2 * CH, 2 * CH), 0)
    col = iota((2 * CH, 2 * CH), 1)
    t, s = row % CH, col % CH
    eye = row == col
    same_head = ones_where(row // HD == col // HD)
    tri = [ones_where((iota((CH, CH), 0) >= iota((CH, CH), 1))), ones_where((iota((CH, CH), 0) <= iota((CH, CH), 1)))]
    strict = [t > s, t < s]
    within = [t >= s, t <= s]

    def one_pair(p, carry):
        @pl.when(p == 1)
        def _():
            send_halo()

        @pl.when(p == FOUR // 2)
        def _():
            for k in range(1, nz):
                z_copy(k, (z + nz - k) % nz).wait_recv()
            for k in range(1, nx):
                x_copy(k, x).start()

        recept = proj_ref[p, :, :PAIR].astype(F32)
        keys = proj_ref[p, :, PAIR : 2 * PAIR].astype(F32)
        values = proj_ref[p, :, 2 * PAIR : 3 * PAIR].astype(F32)
        squares = mm2(keys * keys, same_head)
        unit = keys * lax.rsqrt(squares + NORM_EPS)
        jobs = [(d, c) for d in range(2) for c in range(2)]
        stage = {}
        for d, c in jobs:
            rows = slice(c * CH, (c + 1) * CH)
            logd = logd_ref[d, p, rows, :]
            parts = jnp.concatenate(split3(logd), axis=0)
            total = dot(jnp.concatenate([tri[d]] * 3, axis=1), parts)
            middle = total[CH // 2 - 1 : CH // 2] if d == 0 else total[CH // 2 : CH // 2 + 1]
            last = total[CH - 1 : CH] if d == 0 else total[0:1]
            grow = jnp.exp(total - middle)
            shrink = jnp.exp(middle - total)
            read = recept[rows] * grow
            mark = unit[rows] * jnp.exp(total - logd - middle)
            erase = unit[rows] * learn_ref[d, p, rows, :] * shrink
            key = keys[rows] * shrink
            read_s, mark_s, erase_s, key_s = map(stacked, (read, mark, erase, key))
            scores = mm3(
                jnp.concatenate([mark_s, read_s], axis=0),
                jnp.concatenate([erase_s, key_s], axis=0),
                NT,
            )
            stage[d, c] = (read, mark_s, erase_s, key_s, scores, jnp.exp(middle), jnp.exp(last - middle), jnp.exp(last))
        inverse = {}
        grams = {}
        for d, c in jobs:
            gram = jnp.where(strict[d], stage[d, c][4][: 2 * CH, : 2 * CH], 0.0)
            grams[d, c] = gram
            inverse[d, c] = jnp.where(eye, 1.0, 0.0) - jnp.where(t // 2 == s // 2, gram, 0.0)
        block = 2
        while block < CH:
            joins = (t // (2 * block) == s // (2 * block)) & (t // block != s // block)
            for job in jobs:
                found = inverse[job]
                inverse[job] = found - mm3(found, mm3(jnp.where(joins, grams[job], 0.0), found))
            block *= 2
        maps, reads, outs = {}, {}, {}
        for d, c in jobs:
            rows = slice(c * CH, (c + 1) * CH)
            read, mark_s, erase_s, key_s, scores, to_start, to_end, whole = stage[d, c]
            val_s = stacked(values[rows]).astype(BF)
            cross = jnp.where(strict[d], scores[: 2 * CH, 2 * CH :], 0.0)
            read_e = jnp.where(within[d], scores[2 * CH :, : 2 * CH], 0.0)
            read_k = jnp.where(within[d], scores[2 * CH :, 2 * CH :], 0.0)
            solved = mm3(inverse[d, c], jnp.concatenate([mark_s, mm2(cross, val_s)], axis=1))
            solved = jnp.concatenate([solved[:, :PAIR] * to_start, solved[:, PAIR:]], axis=1)
            taken = mm3(read_e, solved)
            reads[d, c] = read * to_start - unstacked(taken[:, :PAIR])
            outs[d, c] = unstacked(mm2(read_k, val_s) - taken[:, PAIR:])
            ended = mm3(solved, erase_s * to_end, TN)
            k_hi, k_lo = split2(key_s * to_end)
            added = dot(jnp.concatenate([val_s, val_s], axis=0), jnp.concatenate([k_hi, k_lo], axis=0), TN)
            prod = jnp.where(eye, whole - 1.0, 0.0) - ended[:PAIR]
            maps[d, c] = (prod, added - ended[PAIR:])
        out_rows = [outs[0, 0] + outs[1, 0], outs[0, 1] + outs[1, 1]]
        for d in range(2):
            first, second = (0, 1) if d == 0 else (1, 0)
            (prod1, add1), (prod2, add2) = maps[d, first], maps[d, second]
            both = jnp.concatenate([prod1, add1], axis=0)
            through = mm3(reads[d, second], both, NT)
            q_ref[d, p, first * CH : (first + 1) * CH, :] = reads[d, first]
            q_ref[d, p, second * CH : (second + 1) * CH, :] = reads[d, second] + through[:, :PAIR]
            out_rows[second] = out_rows[second] + through[:, PAIR:]
            joined = mm3(both, prod2)
            prod = prod1 + prod2 + joined[:PAIR]
            add = add1 + joined[PAIR:] + add2
            for hh in range(2):
                for half in range(2):
                    message = jnp.concatenate(
                        [
                            folded(prod, hh, hh * HD, HD // 2),
                            folded(add, hh, hh * HD + half * (HD // 2), HD // 4),
                        ],
                        axis=0,
                    )
                    msg_ref[d * 16 + p * 4 + hh * 2 + half] = message.astype(msg_ref.dtype)
        for c in range(2):
            o_ref[p, c * CH : (c + 1) * CH, :] = out_rows[c]

        @pl.when(p > 0)
        def _():
            send_maps(p - 1)

        return carry

    lax.fori_loop(0, FOUR, one_pair, 0)
    for k in range(1, nx):
        x_copy(k, (x + nx - k) % nx).wait_recv()
    send_maps(FOUR - 1)
    for k in range(1, nz):
        z_copy(k, z).wait_send()
    for k in range(1, nx):
        x_copy(k, x).wait_send()


def folded(x, hh, first, count):
    upper, lower = x[first : first + count], x[first + count : first + 2 * count]
    if hh == 0:
        return upper + pltpu.roll(lower, HD, 1)
    return pltpu.roll(upper, HD, 1) + lower


def exchange(refs, place_of):
    (
        msg_ref, init_ref, reads_ref, local_ref, gain_ref, proj_ref, cos_ref, sin_ref, sink_ref, mix_ref,
        recv_ref, sent_ref, enter_ref, halo_ref, comp_ref,
        out_sem, in_sem, back_out_sem, back_in_sem, halo_out_sem, halo_in_sem,
    ) = refs
    count = recv_ref.shape[0]
    place = place_of[0] * lax.axis_size("sp_1") + place_of[1]
    kv_first = 4 * PAIR

    def halo_copy(side):
        target = (place + count - 1 + 2 * side) % count
        return pltpu.make_async_remote_copy(
            src_ref=proj_ref.at[:, :, kv_first : kv_first + PAIR],
            dst_ref=halo_ref.at[1 - side],
            send_sem=halo_out_sem.at[side],
            recv_sem=halo_in_sem.at[1 - side],
            device_id=peer_id(target),
            device_id_type=MESH,
        )

    def map_copy(target):
        return pltpu.make_async_remote_copy(
            src_ref=msg_ref.at[target],
            dst_ref=recv_ref.at[place],
            send_sem=out_sem.at[target],
            recv_sem=in_sem.at[place],
            device_id=peer_id(target),
            device_id_type=MESH,
        )

    def map_arrival(source):
        return pltpu.make_async_remote_copy(
            src_ref=msg_ref.at[source],
            dst_ref=recv_ref.at[source],
            send_sem=out_sem.at[source],
            recv_sem=in_sem.at[source],
            device_id=peer_id(source),
            device_id_type=MESH,
        )

    def entry_copy(target):
        return pltpu.make_async_remote_copy(
            src_ref=sent_ref.at[target],
            dst_ref=enter_ref.at[place],
            send_sem=back_out_sem.at[target],
            recv_sem=back_in_sem.at[place],
            device_id=peer_id(target),
            device_id_type=MESH,
        )

    def entry_arrival(source):
        return pltpu.make_async_remote_copy(
            src_ref=sent_ref.at[source],
            dst_ref=enter_ref.at[source],
            send_sem=back_out_sem.at[source],
            recv_sem=back_in_sem.at[source],
            device_id=peer_id(source),
            device_id_type=MESH,
        )

    def send_halo():
        halo_copy(0).start()
        halo_copy(1).start()

    def send_maps(p):
        for d in range(2):
            for q in range(4):
                target = d * 16 + p * 4 + q

                @pl.when(target != place)
                def _():
                    map_copy(target).start()

    def run():
        tokens = local_ref.shape[1]
        for side in range(2):
            halo_copy(side).wait()
        lane = iota((1, PAIR), 1)
        low = lane < HD
        front = lane % 32 < 16

        def turned(v, first, last):
            other = jnp.where(front, -pltpu.roll(v, PAIR - 16, 1), pltpu.roll(v, 16, 1))
            return v * cos_ref[first:last, :] + other * sin_ref[first:last, :]

        reach = 3 * tokens
        q_pos = place * tokens + iota((2 * tokens, reach), 0) % tokens
        k_pos = (place - 1) * tokens + iota((2 * tokens, reach), 1)
        allowed = (jnp.abs(q_pos - k_pos) <= WINDOW) & (k_pos >= 0) & (k_pos < count * tokens)
        upper = iota((2 * tokens, 1), 0) < tokens
        pair = lax.axis_index("fs")
        first_head = lax.axis_index("tp") * (2 * FOUR) + 2 * pair
        sink = jnp.where(upper, sink_ref[first_head], sink_ref[first_head + 1])

        def attend(p, carry):
            kv = jnp.concatenate(
                [halo_ref[0, p], proj_ref[p, :, kv_first : kv_first + PAIR], halo_ref[1, p]], axis=0
            ).astype(F32)
            roped = turned(kv, 0, reach)
            swapped = pltpu.roll(kv, HD, 1)
            key = jnp.where(low, roped, pltpu.roll(roped, HD, 1)).astype(BF)
            value = jnp.where(low, swapped, kv).astype(BF)
            query = turned(proj_ref[p, :, kv_first - PAIR : kv_first].astype(F32), tokens, 2 * tokens)
            query = jnp.concatenate([jnp.where(low, query, 0.0), jnp.where(low, 0.0, query)], axis=0)
            scores = dot(query.astype(BF), key, NT) * HD**-0.5
            scores = jnp.where(allowed, scores, -jnp.inf)
            top = jnp.maximum(jnp.max(scores, axis=-1, keepdims=True), sink)
            raised = jnp.exp(scores - top)
            total = jnp.exp(sink - top) + jnp.sum(raised, axis=-1, keepdims=True)
            mixed = dot((raised / total).astype(BF), value)
            mix_ref[pair, p, :, PAIR:] = jnp.where(low, mixed[:tokens], mixed[tokens:]).astype(BF)
            return carry

        lax.fori_loop(0, FOUR, attend, 0)

        recv_ref[place] = msg_ref[place]

        def await_map(k, carry):
            map_arrival((place + k) % count).wait()
            return carry

        lax.fori_loop(1, count, await_map, 0)

        unit_idx = place // 2
        direction, half = unit_idx // 8, place % 2
        rows = HD // 2
        quarter = rows // 2
        start = pl.multiple_of(half * rows, rows)
        groups = 4
        length = count // groups

        def nth(step):
            return direction * (count - 1) + step * (1 - 2 * direction)

        def message(step):
            m = recv_ref[nth(step)].astype(F32)
            return jnp.concatenate([m[:rows, :HD], m[:rows, HD:], m[rows:, :HD], m[rows:, HD:]], axis=0)

        def extend(s, maps):
            longer = []
            for g in range(groups):
                step = message(g * length + s)
                comp_ref[g, s] = maps[g]
                longer.append(maps[g] + mm3(maps[g], step[:HD]) + step)
            return tuple(longer)

        nothing = jnp.zeros((3 * rows, HD), F32)
        maps = lax.fori_loop(0, length, extend, (nothing,) * groups)
        state = init_ref[direction, first_head + unit_idx % 2, pl.ds(start, rows), :]

        def dispatch(g):
            def one(s, carry):
                target = nth(g * length + s)

                @pl.when(target != place)
                def _():
                    entry_copy(target).start()

                return carry

            lax.fori_loop(0, length, one, 0)

        for g in range(groups):
            for s in range(length):
                before = comp_ref[g, s]
                entry = state + mm3(state, before[:HD]) + before[HD:] if s else state
                sent_ref[nth(g * length + s)] = jnp.concatenate(
                    [entry[:quarter], entry[quarter:]], axis=1
                ).astype(BF)
            state = state + mm3(state, maps[g][:HD]) + maps[g][HD:]
            if g:
                dispatch(g - 1)
        enter_ref[place] = sent_ref[place]
        dispatch(groups - 1)

        def await_entry(k, carry):
            entry_arrival((place + k) % count).wait()
            return carry

        lax.fori_loop(1, count, await_entry, 0)
        finish(reads_ref, local_ref, enter_ref, gain_ref, mix_ref.at[pair])

    return send_halo, send_maps, run


def finish(q_ref, o_ref, enter_ref, gain_ref, mix_ref):
    row = iota((PAIR, PAIR), 0)
    col = iota((PAIR, PAIR), 1)
    same_head = ones_where(row // HD == col // HD)
    low = iota((HD // 4, PAIR), 1) < HD
    start = (lax.axis_index("tp") * FOUR + lax.axis_index("fs")) * PAIR
    gain = gain_ref[:, pl.ds(pl.multiple_of(start, PAIR), PAIR)]
    for p in range(FOUR):
        out = o_ref[p]
        for d in range(2):
            pieces = []
            for hh in range(2):
                for half in range(2):
                    m = enter_ref[d * 16 + p * 4 + hh * 2 + half].astype(F32)
                    turned = pltpu.roll(m, HD, 1)
                    if hh == 0:
                        pieces += [jnp.where(low, m, 0.0), jnp.where(low, turned, 0.0)]
                    else:
                        pieces += [jnp.where(low, 0.0, turned), jnp.where(low, 0.0, m)]
            out = out + mm2(q_ref[d, p], jnp.concatenate(pieces, axis=0).astype(BF), NT)
        centred = out - mm2(out, same_head) * (1.0 / HD)
        spread = mm2(centred * centred, same_head) * (1.0 / HD)
        mix_ref[p, :, :PAIR] = (centred * lax.rsqrt(spread + GROUP_EPS) * gain).astype(BF)


def project_out(refs, place_of):
    (
        rows_ref, out_ref, all_ref, total_ref, other_ref, ready_ref, got_ref,
        mix_out, mix_in, half_out, half_in, back_out, back_in,
    ) = refs
    f, c = place_of[2:]
    tokens = all_ref.shape[2]
    start, relay, arrive_near, arrive_far, finish_sends = ring_of_four(all_ref, mix_out, mix_in)
    start()
    columns = total_ref.shape[2]
    weight_rows = rows_ref.shape[0] * rows_ref.shape[1] * rows_ref.shape[2]

    def product(g):
        weight = rows_ref[:, :, :, pl.ds(pl.multiple_of(g * 2 * PAIR, 2 * PAIR), 2 * PAIR)]
        left = all_ref[g].reshape(FOUR * tokens, 2 * PAIR)
        return dot(left, weight.reshape(weight_rows, 2 * PAIR), NT).reshape(FOUR, tokens, columns)

    total_ref[...] = product(f)
    relay()
    arrive_near()
    total_ref[...] += product((f + 1) % FOUR) + product((f + 3) % FOUR)
    arrive_far()
    total_ref[...] += product((f + 2) % FOUR)
    half = tokens // 2
    theirs = pl.ds(pl.multiple_of((1 - c) * half, half), half)
    ours = pl.ds(pl.multiple_of(c * half, half), half)
    half_copy = pltpu.make_async_remote_copy(
        src_ref=total_ref.at[:, theirs, :], dst_ref=other_ref, send_sem=half_out, recv_sem=half_in,
        device_id={"tp": 1 - c}, device_id_type=MESH,
    )
    half_copy.start()
    half_copy.wait_recv()
    ready_ref[...] = (total_ref[:, ours, :] + other_ref[...]).astype(BF)

    def back_copy(k, source):
        g = (f + k) % FOUR
        return pltpu.make_async_remote_copy(
            src_ref=ready_ref.at[g], dst_ref=got_ref.at[source], send_sem=back_out.at[k], recv_sem=back_in.at[k],
            device_id={"fs": g}, device_id_type=MESH,
        )

    for k in range(1, FOUR):
        back_copy(k, f).start()
    got_ref[f] = ready_ref[f]
    finish_sends()
    half_copy.wait_send()
    wide = FOUR * PAIR
    source, target = iota((wide, wide), 0), iota((wide, wide), 1)
    place = source % PAIR // 16 * (FOUR * 16) + source // PAIR * 16 + source % 16
    shuffle = ones_where(place == target)
    for k in range(1, FOUR):
        back_copy(k, (f + FOUR - k) % FOUR).wait_recv()
    for b in range(columns // PAIR):
        lanes = slice(b * PAIR, (b + 1) * PAIR)
        joined = jnp.concatenate([got_ref[g, :, lanes] for g in range(FOUR)], axis=1)
        out_ref[:, b * wide : (b + 1) * wide] = dot(joined, shuffle).astype(BF)
    for k in range(1, FOUR):
        back_copy(k, f).wait_send()


def layer_kernel(
    x_ref, gain_ref, wr_ref, wk_ref, wv_ref, wq_ref, wak_ref, wav_ref, down_d_hbm, down_e_hbm,
    up_d_hbm, up_e_hbm, off_d_ref, off_e_ref, extra_ref, init_hbm, head_gain_ref, sink_ref,
    lin_out_ref, att_out_ref,
    out_ref,
    both_ref, hid_ref, stage_ref, cols_ref, ext_ref, down_d_ref, down_e_ref, up_d_ref, up_e_ref, init_ref,
    proj_ref, logd_ref, learn_ref, cos_ref, sin_ref, wout_ref,
    reads_ref, local_ref, msg_ref, rows_ref,
    recv_ref, sent_ref, enter_ref, halo_ref, comp_ref,
    all_ref, total_ref, other_ref, ready_ref, got_ref,
    load_sem, late_sem, x_out, x_in, hid_out, hid_in, stage_out, stage_in, ext_out, ext_in,
    z_out, z_in, near_out, near_in, far_out, far_in,
    wz_out, wz_in, wx_out, wx_in,
    out_sem, in_sem, back_out_sem, back_in_sem, halo_out_sem, halo_in_sem,
    mix_out, mix_in, half_out, half_in, back_out, back_in,
):
    place_of = tuple(lax.axis_index(a) for a in ("sp_0", "sp_1", "fs", "tp"))
    pairs = (
        (down_d_hbm, down_d_ref), (down_e_hbm, down_e_ref), (up_d_hbm, up_d_ref), (up_e_hbm, up_e_ref),
        (init_hbm, init_ref),
    )
    late = [pltpu.make_async_copy(a, b, late_sem.at[k]) for k, (a, b) in enumerate(pairs)]
    for g in range(FOUR):
        for k, ref in enumerate((lin_out_ref, att_out_ref)):
            wout_ref[:, (2 * g + k) * PAIR : (2 * g + k + 1) * PAIR] = ref[:, g * PAIR : (g + 1) * PAIR]
    front(
        (
            x_ref, gain_ref, wr_ref, wk_ref, wv_ref, wq_ref, wak_ref, wav_ref, down_d_ref, down_e_ref,
            up_d_ref, up_e_ref, off_d_ref, off_e_ref, extra_ref, proj_ref, logd_ref, learn_ref,
            both_ref, hid_ref, stage_ref, cols_ref, ext_ref, load_sem,
            x_out, x_in, hid_out, hid_in, stage_out, stage_in, ext_out, ext_in,
            z_out, z_in, near_out, near_in, far_out, far_in, cos_ref, sin_ref, late,
        ),
        place_of,
    )
    send_halo, send_maps, run = exchange(
        (
            msg_ref, init_ref, reads_ref, local_ref, head_gain_ref, proj_ref, cos_ref, sin_ref, sink_ref,
            all_ref, recv_ref, sent_ref, enter_ref, halo_ref, comp_ref,
            out_sem, in_sem, back_out_sem, back_in_sem, halo_out_sem, halo_in_sem,
        ),
        place_of,
    )
    local_maps(
        (
            proj_ref, logd_ref, learn_ref, wout_ref, reads_ref, local_ref, msg_ref, rows_ref,
            wz_out, wz_in, wx_out, wx_in,
        ),
        place_of,
        send_halo,
        send_maps,
    )
    run()
    project_out(
        (
            rows_ref, out_ref, all_ref, total_ref, other_ref, ready_ref, got_ref,
            mix_out, mix_in, half_out, half_in, back_out, back_in,
        ),
        place_of,
    )


def local(
    inputs, input_norm_gain, receptance_weight, linear_key_weight, linear_value_weight,
    window_query_weight, window_key_weight, window_value_weight, decay_down_weight, decay_up_weight,
    decay_offset, decay_log_extra, erasure_down_weight, erasure_up_weight, erasure_offset,
    initial_state, head_norm_gain, query_sink_logit, linear_output_weight, window_output_weight,
):
    tokens, model = inputs.shape[1], 2 * inputs.shape[2]
    places = lax.axis_size(SP)
    nz, nx = lax.axis_size("sp_0"), lax.axis_size("sp_1")
    rows = receptance_weight.shape[0]
    out_rows = linear_output_weight.shape[1]
    columns = places * out_rows
    vmem = pl.BlockSpec(memory_space=pltpu.VMEM)
    hbm = pl.BlockSpec(memory_space=pl.ANY)
    smem = pl.BlockSpec(memory_space=pltpu.SMEM)
    dma = pltpu.SemaphoreType.DMA
    down_d, down_e = decay_down_weight.T, erasure_down_weight.T

    def space(kind, *shape):
        return pltpu.VMEM(shape, kind)

    out = pl.pallas_call(
        layer_kernel,
        out_shape=jax.ShapeDtypeStruct((tokens // 2, FOUR * columns), BF),
        in_specs=[hbm, vmem, hbm, hbm, hbm, hbm, vmem, vmem, hbm, hbm, hbm, hbm, vmem, vmem, hbm, hbm, vmem, smem, vmem, vmem],
        out_specs=vmem,
        scratch_shapes=[
            space(BF, 2, tokens, model // 2),
            space(BF, FOUR, tokens, model),
            space(BF, FOUR, rows, 5 * PAIR),
            space(BF, places, FOUR * rows, 5 * PAIR),
            space(F32, FOUR, *decay_log_extra.shape[1:]),
            space(BF, *down_d.shape),
            space(BF, *down_e.shape),
            space(BF, *decay_up_weight.shape),
            space(BF, *erasure_up_weight.shape),
            space(F32, *initial_state.shape),
            space(BF, FOUR, tokens, 5 * PAIR),
            space(F32, 2, FOUR, tokens, PAIR),
            space(F32, 2, FOUR, tokens, PAIR),
            space(F32, tokens + 2 * WINDOW, PAIR),
            space(F32, tokens + 2 * WINDOW, PAIR),
            space(BF, out_rows, 2 * FOUR * PAIR),
            space(F32, 2, FOUR, tokens, PAIR),
            space(F32, FOUR, tokens, PAIR),
            space(BF, places, 48, PAIR),
            space(BF, nz, nx, out_rows, 2 * FOUR * PAIR),
            space(BF, places, 48, PAIR),
            space(BF, places, 16, PAIR),
            space(BF, places, 16, PAIR),
            space(BF, 2, FOUR, tokens, PAIR),
            space(F32, 4, places // 4, 3 * HD // 2, HD),
            space(BF, FOUR, FOUR, tokens, 2 * PAIR),
            space(F32, FOUR, tokens, columns),
            space(F32, FOUR, tokens // 2, columns),
            space(BF, FOUR, tokens // 2, columns),
            space(BF, FOUR, tokens // 2, columns),
            dma((18,)), dma((5,)),
            dma, dma, dma((6,)), dma((6,)), dma((FOUR,)), dma((FOUR,)), dma((FOUR,)), dma((FOUR,)),
            dma((2, nz // 2)), dma((2, nz // 2)), dma((nz, 2)), dma((nz, 2)), dma((nz,)), dma((nz,)),
            dma((nz,)), dma((nz,)), dma((nx,)), dma((nx,)),
            dma((places,)), dma((places,)), dma((places,)), dma((places,)), dma((2,)), dma((2,)),
            dma((6,)), dma((6,)), dma, dma, dma((FOUR,)), dma((FOUR,)),
        ],
        compiler_params=pltpu.CompilerParams(
            collective_id=0, has_side_effects=True, vmem_limit_bytes=48 * 2**20
        ),
        name="layer",
    )(
        inputs[0], input_norm_gain[None], receptance_weight, linear_key_weight, linear_value_weight,
        window_query_weight, window_key_weight, window_value_weight, down_d, down_e,
        decay_up_weight, erasure_up_weight, decay_offset, erasure_offset, decay_log_extra,
        initial_state, head_norm_gain[None], query_sink_logit, linear_output_weight.T,
        window_output_weight.T,
    )
    return out[None]


def solution(mesh):
    finer = Mesh(
        mesh.devices.reshape(8, 4, mesh.shape["fs"], mesh.shape["tp"]), ("sp_0", "sp_1", "fs", "tp")
    )
    placed = (
        P("fs", SP, "tp"),
        P(),
        P(SP_FS, "tp"),
        P(SP_FS, "tp"),
        P(SP_FS, "tp"),
        P(SP_FS, "tp"),
        P(SP_FS, "tp"),
        P(SP_FS, "tp"),
        P(),
        P(),
        P(),
        P("fs", "tp", SP),
        P(),
        P(),
        P(),
        P(),
        P(),
        P(),
        P("tp", SP_FS),
        P("tp", SP_FS),
    )
    return jax.shard_map(
        local, mesh=finer, in_specs=placed, out_specs=P("fs", SP_TP, None), check_vma=False
    )
```

```python
import math
import functools
import jax
import jax.numpy as jnp
from jax import lax
from jax.experimental import pallas as pl
from jax.experimental.pallas import tpu as pltpu

from jax.sharding import Mesh
from jax.sharding import PartitionSpec as P

HD = 64
CH = 64
PAIR = 128
WINDOW = 128
GRID_W = 64
ATT_BLOCK = 128
SP = ("sp_0", "sp_1")
FOUR = 4
SP_FS = ("sp_0", "sp_1", "fs")
SP_TP = ("sp_0", "sp_1", "tp")
NORM_EPS = 1e-06
GROUP_EPS = 0.00064
ROPE_BASE = 10000.0
F32 = jnp.float32
BF = jnp.bfloat16
MESSAGE = jnp.bfloat16
MESH = pl.DeviceIdType.MESH
NN = (((1,), (0,)), ((), ()))
NT = (((1,), (1,)), ((), ()))
TN = (((0,), (0,)), ((), ()))


def dot(a, b, dims=NN):
    return lax.dot_general(a, b, dims, preferred_element_type=F32)


def split2(a):
    high = a.astype(BF)
    return high, (a - high.astype(F32)).astype(BF)


def split3(a):
    high, rest = a.astype(BF), None
    rest = a - high.astype(F32)
    mid = rest.astype(BF)
    return high, mid, (rest - mid.astype(F32)).astype(BF)


def mm3(a, b, dims=NN):
    (ka,), (kb,) = dims[0]
    a_hi, a_lo = split2(a)
    b_hi, b_lo = split2(b)
    free = 1 - kb
    if b.shape[free] == PAIR:
        upper = jnp.concatenate([b_hi, b_lo], axis=free)
        lower = jnp.concatenate([b_hi, jnp.zeros_like(b_lo)], axis=free)
        wide = dot(
            jnp.concatenate([a_hi, a_lo], axis=ka), jnp.concatenate([upper, lower], axis=kb), dims
        )
        return wide[:, :PAIR] + wide[:, PAIR:]
    main = dot(
        jnp.concatenate([a_hi, a_lo], axis=ka), jnp.concatenate([b_hi, b_hi], axis=kb), dims
    )
    return main + dot(a_hi, b_lo, dims)


def mm2(a, b_exact, dims=NN):
    (ka,), (kb,) = dims[0]
    a_hi, a_lo = split2(a)
    return dot(
        jnp.concatenate([a_hi, a_lo], axis=ka), jnp.concatenate([b_exact, b_exact], axis=kb), dims
    )


def iota(shape, dim):
    return lax.broadcasted_iota(jnp.int32, shape, dim)


def ones_where(cond):
    return jnp.where(cond, 1.0, 0.0).astype(BF)


def ring_of_four(buf, out_sem, in_sem):
    me = lax.axis_index("fs")
    right, left, far = (me + 1) % FOUR, (me + 3) % FOUR, (me + 2) % FOUR
    half = buf.shape[1] // 2

    def piece(block, part, target, number):
        where = buf.at[block, part * half : (part + 1) * half]
        return pltpu.make_async_remote_copy(
            src_ref=where, dst_ref=where, send_sem=out_sem.at[number], recv_sem=in_sem.at[number],
            device_id={"fs": target}, device_id_type=MESH,
        )

    def start():
        piece(me, 0, right, 0).start()
        piece(me, 1, left, 1).start()
        piece(me, 1, right, 2).start()
        piece(me, 0, left, 3).start()

    def relay():
        piece(left, 0, right, 0).wait_recv()
        piece(left, 0, right, 4).start()
        piece(right, 1, left, 1).wait_recv()
        piece(right, 1, left, 5).start()

    def arrive_near():
        piece(left, 1, right, 2).wait_recv()
        piece(right, 0, left, 3).wait_recv()

    def arrive_far():
        piece(far, 0, right, 4).wait_recv()
        piece(far, 1, left, 5).wait_recv()

    def finish_sends():
        piece(me, 0, right, 0).wait_send()
        piece(me, 1, left, 1).wait_send()
        piece(me, 1, right, 2).wait_send()
        piece(me, 0, left, 3).wait_send()
        piece(left, 0, right, 4).wait_send()
        piece(right, 1, left, 5).wait_send()

    return start, relay, arrive_near, arrive_far, finish_sends


def peer_id(index):
    inner = lax.axis_size("sp_1")
    return {"sp_0": index // inner, "sp_1": index % inner}


def neighbours(place_of):
    z, x, f, c = place_of
    nz, nx = lax.axis_size("sp_0"), lax.axis_size("sp_1")
    peers = [{"fs": (f + k) % FOUR} for k in range(1, FOUR)] + [{"tp": 1 - c}]
    peers += [{"sp_0": (z + k) % nz} for k in (1, nz - 1)]
    return peers + [{"sp_1": (x + k) % nx} for k in (1, nx - 1)]


def rope_tables(place, cos_ref, sin_ref):
    reach = cos_ref.shape[0]
    block = reach // 3
    spot = iota((reach, PAIR), 0)
    lane = iota((reach, PAIR), 1)
    grid_row = ((place - 1) * (block // GRID_W) + spot // GRID_W).astype(F32)
    grid_col = (spot % GRID_W).astype(F32)
    power = (lane % 16).astype(F32) * (1.0 / 16)
    angle = jnp.where(lane % HD < HD // 2, grid_row, grid_col) * jnp.exp(power * -math.log(ROPE_BASE))
    cos_ref[...] = jnp.cos(angle)
    sin_ref[...] = jnp.sin(angle)


def front(refs, place_of):
    (
        x_ref, gain_ref, wr_ref, wk_ref, wv_ref, wq_ref, wak_ref, wav_ref, down_d_ref, down_e_ref,
        up_d_ref, up_e_ref, off_d_ref, off_e_ref, extra_ref, proj_ref, logd_ref, learn_ref,
        both_ref, hid_ref, stage_ref, cols_ref, ext_ref, load_sem,
        x_out, x_in, hid_out, hid_in, stage_out, stage_in, ext_out, ext_in,
        z_out, z_in, near_out, near_in, far_out, far_in, cos_ref, sin_ref, late,
    ) = refs
    z, x, f, c = place_of
    nz, nx = lax.axis_size("sp_0"), lax.axis_size("sp_1")
    mine = z * nx + x
    rows = wr_ref.shape[0]
    loads = []
    for g in range(FOUR):
        for k, ref in enumerate((wr_ref, wk_ref, wv_ref, wq_ref)):
            loads.append((ref.at[:, g * PAIR : (g + 1) * PAIR], stage_ref.at[g, :, k * PAIR : (k + 1) * PAIR]))
    loads.append((x_ref, both_ref.at[c]))
    loads.append((extra_ref.at[0], ext_ref.at[f]))
    loads = [
        pltpu.make_async_copy(start, end, load_sem.at[number]) for number, (start, end) in enumerate(loads)
    ]
    for load in loads:
        load.start()
    for load in late:
        load.start()
    low = iota((rows, PAIR), 1) < HD
    keys, values = wak_ref[...].astype(F32), wav_ref[...].astype(F32)
    shared = [
        jnp.where(low, keys, pltpu.roll(values, HD, 1)).astype(BF),
        jnp.where(low, pltpu.roll(keys, HD, 1), values).astype(BF),
    ]
    for g in range(FOUR):
        stage_ref[g, :, 4 * PAIR :] = shared[g // 2]
    with jax.named_scope("f_load"):
        for load in loads:
            load.wait()
    my_rows = pl.ds(pl.multiple_of(f * rows, rows), rows)
    cols_ref[mine, my_rows, :] = stage_ref[f]
    with jax.named_scope("f_meet"):
        pl.semaphore_wait(pltpu.get_barrier_semaphore(), len(neighbours(place_of)))

    half_copy = pltpu.make_async_remote_copy(
        src_ref=both_ref.at[c], dst_ref=both_ref.at[c], send_sem=x_out, recv_sem=x_in,
        device_id={"tp": 1 - c}, device_id_type=MESH,
    )
    half_copy.start()

    def stage_copy(k):
        g = (f + k) % FOUR
        return pltpu.make_async_remote_copy(
            src_ref=stage_ref.at[g], dst_ref=cols_ref.at[mine, my_rows, :],
            send_sem=stage_out.at[k], recv_sem=stage_in.at[k], device_id={"fs": g}, device_id_type=MESH,
        )

    def stage_arrival(k):
        g = (f + FOUR - k) % FOUR
        return pltpu.make_async_remote_copy(
            src_ref=stage_ref.at[g], dst_ref=cols_ref.at[mine, pl.ds(pl.multiple_of(g * rows, rows), rows), :],
            send_sem=stage_out.at[k], recv_sem=stage_in.at[k], device_id={"fs": g}, device_id_type=MESH,
        )

    def ext_copy(k, source):
        return pltpu.make_async_remote_copy(
            src_ref=ext_ref.at[source], dst_ref=ext_ref.at[source],
            send_sem=ext_out.at[k], recv_sem=ext_in.at[k], device_id={"fs": (f + k) % FOUR}, device_id_type=MESH,
        )

    for k in range(1, FOUR):
        stage_copy(k).start()

    def z_block(k):
        if k == 0:
            return z
        step = (k - 1) // 2
        return (z + nz - 1 - step) % nz if k % 2 else (z + 1 + step) % nz

    def z_copy(k_from, side, step):
        where = cols_ref.at[z_block(k_from) * nx + x]
        return pltpu.make_async_remote_copy(
            src_ref=where, dst_ref=where, send_sem=z_out.at[side, step], recv_sem=z_in.at[side, step],
            device_id={"sp_0": (z + (1 if side == 0 else nz - 1)) % nz}, device_id_type=MESH,
        )

    def near_copy(k, side, column):
        where = cols_ref.at[z_block(k) * nx + column]
        return pltpu.make_async_remote_copy(
            src_ref=where, dst_ref=where, send_sem=near_out.at[k, side], recv_sem=near_in.at[k, side],
            device_id={"sp_1": (x + (1 if side == 0 else nx - 1)) % nx}, device_id_type=MESH,
        )

    def far_copy(k, column):
        where = cols_ref.at[z_block(k) * nx + column]
        return pltpu.make_async_remote_copy(
            src_ref=where, dst_ref=where, send_sem=far_out.at[k], recv_sem=far_in.at[k],
            device_id={"sp_1": (x + (1 if k % 2 == 0 else nx - 1)) % nx}, device_id_type=MESH,
        )

    left, right, across = (x + nx - 1) % nx, (x + 1) % nx, (x + 2) % nx

    def spread(k):
        near_copy(k, 0, x).start()
        near_copy(k, 1, x).start()

    def pass_on(k):
        near_copy(k, 0, left).wait_recv()
        near_copy(k, 1, right).wait_recv()
        far_copy(k, left if k % 2 == 0 else right).start()

    with jax.named_scope("f_stage_wait"):
        for k in range(1, FOUR):
            stage_arrival(k).wait_recv()
    z_copy(0, 0, 0).start()
    z_copy(0, 1, 0).start()
    spread(0)

    with jax.named_scope("f_norm"):
        half_copy.wait_recv()
        full = jnp.concatenate([both_ref[0], both_ref[1]], axis=1).astype(F32)
        scale = lax.rsqrt(jnp.mean(full * full, axis=-1, keepdims=True) + NORM_EPS)
        hid_ref[f] = (full * scale * gain_ref[...]).astype(BF)
    start, relay, arrive_near, arrive_far, finish_sends = ring_of_four(hid_ref, hid_out, hid_in)
    for k in range(1, FOUR):
        ext_copy(k, f).start()
    start()
    with jax.named_scope("f_rope"):
        rope_tables(mine, cos_ref, sin_ref)

    steps = nz // 2
    with jax.named_scope("f_ring"):
        for step in range(steps):
            k = 2 * step + 1
            z_copy(k, 0, step).wait_recv()
            if step < steps - 1:
                z_copy(k, 0, step + 1).start()
            spread(k)
            if step < steps - 1:
                z_copy(k + 1, 1, step).wait_recv()
                if step < steps - 2:
                    z_copy(k + 1, 1, step + 1).start()
                spread(k + 1)
            if step == 0:
                pass_on(0)
            else:
                pass_on(k - 2)
                pass_on(k - 1)
            if step == 1:
                relay()
    with jax.named_scope("f_pass_last"):
        pass_on(nz - 1)
    with jax.named_scope("f_hid_wait"):
        arrive_near()
        arrive_far()
        for k in range(1, FOUR):
            ext_copy(k, (f + FOUR - k) % FOUR).wait_recv()

    for load in late:
        load.wait()
    tokens = hid_ref.shape[1]
    hidden = hid_ref[...].reshape(FOUR * tokens, hid_ref.shape[2])
    with jax.named_scope("f_rates"):
        decay_low = dot(hidden, down_d_ref[...], NT).astype(BF)
        learn_low = dot(hidden, down_e_ref[...], NT).astype(BF)
        decay_act = jnp.tanh(decay_low.astype(F32)).astype(BF)
        heads = ext_ref.shape[1]
        first = c * heads * HD + f * PAIR
        chosen = pl.ds(pl.multiple_of(first, PAIR), PAIR)
        select = ones_where(iota((heads, PAIR), 0) == 2 * f + iota((heads, PAIR), 1) // HD).astype(F32)
        spikes = [
            lax.dot_general(
                ext_ref[p], select, TN, precision=lax.Precision.HIGHEST, preferred_element_type=F32
            )
            for p in range(FOUR)
        ]
        for d in range(2):
            pre = off_d_ref[d : d + 1, chosen] + dot(decay_act, up_d_ref[d, :, chosen])
            softplus = jnp.maximum(-pre, 0.0) + jnp.log1p(jnp.exp(-jnp.abs(pre)))
            rate = jnp.exp(-softplus - 0.5)
            learn = jax.nn.sigmoid(off_e_ref[d : d + 1, chosen] + dot(learn_low, up_e_ref[d, :, chosen]))
            for p in range(FOUR):
                part = slice(p * tokens, (p + 1) * tokens)
                logd_ref[d, p] = spikes[p] - rate[part]
                learn_ref[d, p] = learn[part]

    with jax.named_scope("f_far_wait"):
        for k in range(nz):
            far_copy(k, across).wait_recv()
    depth = cols_ref.shape[0] * cols_ref.shape[1]
    with jax.named_scope("f_proj"):
        for first_col, last_col in ((0, 256), (256, 512), (512, 640)):
            weight = cols_ref[:, :, first_col:last_col].reshape(depth, last_col - first_col)
            result = dot(hidden, weight).astype(BF)
            for p in range(FOUR):
                proj_ref[p, :, first_col:last_col] = result[p * tokens : (p + 1) * tokens]

    half_copy.wait_send()
    finish_sends()
    for k in range(1, FOUR):
        stage_copy(k).wait_send()
        ext_copy(k, f).wait_send()
    for step in range(steps):
        z_copy(0, 0, step).wait_send()
        if step < steps - 1:
            z_copy(0, 1, step).wait_send()
    for k in range(nz):
        near_copy(k, 0, x).wait_send()
        near_copy(k, 1, x).wait_send()
        far_copy(k, left).wait_send()


def stacked(x):
    low = iota(x.shape, 1) < HD
    return jnp.concatenate([jnp.where(low, x, 0.0), jnp.where(low, 0.0, x)], axis=0)


def unstacked(x):
    return x[:CH] + x[CH:]


def local_maps(refs, place_of, send_halo, send_maps):
    proj_ref, logd_ref, learn_ref, wout_ref, q_ref, o_ref, msg_ref, rows_ref, z_out, z_in, x_out, x_in = refs
    z, x = place_of[:2]
    nz, nx = lax.axis_size("sp_0"), lax.axis_size("sp_1")
    rows_ref[z, x] = wout_ref[...]

    def z_copy(k, source):
        return pltpu.make_async_remote_copy(
            src_ref=wout_ref, dst_ref=rows_ref.at[source, x], send_sem=z_out.at[k], recv_sem=z_in.at[k],
            device_id={"sp_0": (z + k) % nz}, device_id_type=MESH,
        )

    def x_copy(k, column):
        where = rows_ref.at[:, column]
        return pltpu.make_async_remote_copy(
            src_ref=where, dst_ref=where, send_sem=x_out.at[k], recv_sem=x_in.at[k],
            device_id={"sp_1": (x + k) % nx}, device_id_type=MESH,
        )

    for k in range(1, nz):
        z_copy(k, z).start()
    row = iota((2 * CH, 2 * CH), 0)
    col = iota((2 * CH, 2 * CH), 1)
    t, s = row % CH, col % CH
    eye = row == col
    same_head = ones_where(row // HD == col // HD)
    tri = [ones_where((iota((CH, CH), 0) >= iota((CH, CH), 1))), ones_where((iota((CH, CH), 0) <= iota((CH, CH), 1)))]
    strict = [t > s, t < s]
    within = [t >= s, t <= s]

    def one_pair(p, carry):
        @pl.when(p == 1)
        def _():
            send_halo()

        @pl.when(p == FOUR // 2)
        def _():
            for k in range(1, nz):
                z_copy(k, (z + nz - k) % nz).wait_recv()
            for k in range(1, nx):
                x_copy(k, x).start()

        recept = proj_ref[p, :, :PAIR].astype(F32)
        keys = proj_ref[p, :, PAIR : 2 * PAIR].astype(F32)
        values = proj_ref[p, :, 2 * PAIR : 3 * PAIR].astype(F32)
        squares = mm2(keys * keys, same_head)
        unit = keys * lax.rsqrt(squares + NORM_EPS)
        jobs = [(d, c) for d in range(2) for c in range(2)]
        stage = {}
        for d, c in jobs:
            rows = slice(c * CH, (c + 1) * CH)
            logd = logd_ref[d, p, rows, :]
            parts = jnp.concatenate(split3(logd), axis=0)
            total = dot(jnp.concatenate([tri[d]] * 3, axis=1), parts)
            middle = total[CH // 2 - 1 : CH // 2] if d == 0 else total[CH // 2 : CH // 2 + 1]
            last = total[CH - 1 : CH] if d == 0 else total[0:1]
            grow = jnp.exp(total - middle)
            shrink = jnp.exp(middle - total)
            read = recept[rows] * grow
            mark = unit[rows] * jnp.exp(total - logd - middle)
            erase = unit[rows] * learn_ref[d, p, rows, :] * shrink
            key = keys[rows] * shrink
            read_s, mark_s, erase_s, key_s = map(stacked, (read, mark, erase, key))
            scores = mm3(
                jnp.concatenate([mark_s, read_s], axis=0),
                jnp.concatenate([erase_s, key_s], axis=0),
                NT,
            )
            stage[d, c] = (read, mark_s, erase_s, key_s, scores, jnp.exp(middle), jnp.exp(last - middle), jnp.exp(last))
        inverse = {}
        grams = {}
        for d, c in jobs:
            gram = jnp.where(strict[d], stage[d, c][4][: 2 * CH, : 2 * CH], 0.0)
            grams[d, c] = gram
            inverse[d, c] = jnp.where(eye, 1.0, 0.0) - jnp.where(t // 2 == s // 2, gram, 0.0)
        block = 2
        while block < CH:
            joins = (t // (2 * block) == s // (2 * block)) & (t // block != s // block)
            for job in jobs:
                found = inverse[job]
                inverse[job] = found - mm3(found, mm3(jnp.where(joins, grams[job], 0.0), found))
            block *= 2
        maps, reads, outs = {}, {}, {}
        for d, c in jobs:
            rows = slice(c * CH, (c + 1) * CH)
            read, mark_s, erase_s, key_s, scores, to_start, to_end, whole = stage[d, c]
            val_s = stacked(values[rows]).astype(BF)
            cross = jnp.where(strict[d], scores[: 2 * CH, 2 * CH :], 0.0)
            read_e = jnp.where(within[d], scores[2 * CH :, : 2 * CH], 0.0)
            read_k = jnp.where(within[d], scores[2 * CH :, 2 * CH :], 0.0)
            solved = mm3(inverse[d, c], jnp.concatenate([mark_s, mm2(cross, val_s)], axis=1))
            solved = jnp.concatenate([solved[:, :PAIR] * to_start, solved[:, PAIR:]], axis=1)
            taken = mm3(read_e, solved)
            reads[d, c] = read * to_start - unstacked(taken[:, :PAIR])
            outs[d, c] = unstacked(mm2(read_k, val_s) - taken[:, PAIR:])
            ended = mm3(solved, erase_s * to_end, TN)
            k_hi, k_lo = split2(key_s * to_end)
            added = dot(jnp.concatenate([val_s, val_s], axis=0), jnp.concatenate([k_hi, k_lo], axis=0), TN)
            prod = jnp.where(eye, whole - 1.0, 0.0) - ended[:PAIR]
            maps[d, c] = (prod, added - ended[PAIR:])
        out_rows = [outs[0, 0] + outs[1, 0], outs[0, 1] + outs[1, 1]]
        for d in range(2):
            first, second = (0, 1) if d == 0 else (1, 0)
            (prod1, add1), (prod2, add2) = maps[d, first], maps[d, second]
            both = jnp.concatenate([prod1, add1], axis=0)
            through = mm3(reads[d, second], both, NT)
            q_ref[d, p, first * CH : (first + 1) * CH, :] = reads[d, first]
            q_ref[d, p, second * CH : (second + 1) * CH, :] = reads[d, second] + through[:, :PAIR]
            out_rows[second] = out_rows[second] + through[:, PAIR:]
            joined = mm3(both, prod2)
            prod = prod1 + prod2 + joined[:PAIR]
            add = add1 + joined[PAIR:] + add2
            for hh in range(2):
                for half in range(2):
                    message = jnp.concatenate(
                        [
                            folded(prod, hh, hh * HD, HD // 2),
                            folded(add, hh, hh * HD + half * (HD // 2), HD // 4),
                        ],
                        axis=0,
                    )
                    msg_ref[d * 16 + p * 4 + hh * 2 + half] = message.astype(msg_ref.dtype)
        for c in range(2):
            o_ref[p, c * CH : (c + 1) * CH, :] = out_rows[c]

        @pl.when(p > 0)
        def _():
            send_maps(p - 1)

        return carry

    with jax.named_scope("l_loop"):
        lax.fori_loop(0, FOUR, one_pair, 0)
    send_maps(FOUR - 1)

    def await_rows():
        for k in range(1, nx):
            x_copy(k, (x + nx - k) % nx).wait_recv()
        for k in range(1, nz):
            z_copy(k, z).wait_send()
        for k in range(1, nx):
            x_copy(k, x).wait_send()

    return await_rows


def folded(x, hh, first, count):
    upper, lower = x[first : first + count], x[first + count : first + 2 * count]
    if hh == 0:
        return upper + pltpu.roll(lower, HD, 1)
    return pltpu.roll(upper, HD, 1) + lower


def exchange(refs, place_of):
    (
        msg_ref, init_ref, reads_ref, local_ref, gain_ref, proj_ref, cos_ref, sin_ref, sink_ref, lin_ref, att_ref,
        recv_ref, sent_ref, enter_ref, halo_ref, comp_ref,
        out_sem, in_sem, back_out_sem, back_in_sem, halo_out_sem, halo_in_sem,
    ) = refs
    count = recv_ref.shape[0]
    place = place_of[0] * lax.axis_size("sp_1") + place_of[1]
    kv_first = 4 * PAIR

    def halo_copy(side):
        target = (place + count - 1 + 2 * side) % count
        return pltpu.make_async_remote_copy(
            src_ref=proj_ref.at[:, :, kv_first : kv_first + PAIR],
            dst_ref=halo_ref.at[1 - side],
            send_sem=halo_out_sem.at[side],
            recv_sem=halo_in_sem.at[1 - side],
            device_id=peer_id(target),
            device_id_type=MESH,
        )

    def map_copy(target):
        return pltpu.make_async_remote_copy(
            src_ref=msg_ref.at[target],
            dst_ref=recv_ref.at[place],
            send_sem=out_sem.at[target],
            recv_sem=in_sem.at[place],
            device_id=peer_id(target),
            device_id_type=MESH,
        )

    def map_arrival(source):
        return pltpu.make_async_remote_copy(
            src_ref=msg_ref.at[source],
            dst_ref=recv_ref.at[source],
            send_sem=out_sem.at[source],
            recv_sem=in_sem.at[source],
            device_id=peer_id(source),
            device_id_type=MESH,
        )

    def entry_copy(target):
        return pltpu.make_async_remote_copy(
            src_ref=sent_ref.at[target],
            dst_ref=enter_ref.at[place],
            send_sem=back_out_sem.at[target],
            recv_sem=back_in_sem.at[place],
            device_id=peer_id(target),
            device_id_type=MESH,
        )

    def entry_arrival(source):
        return pltpu.make_async_remote_copy(
            src_ref=sent_ref.at[source],
            dst_ref=enter_ref.at[source],
            send_sem=back_out_sem.at[source],
            recv_sem=back_in_sem.at[source],
            device_id=peer_id(source),
            device_id_type=MESH,
        )

    def send_halo():
        halo_copy(0).start()
        halo_copy(1).start()

    def send_maps(p):
        for d in range(2):
            for q in range(4):
                target = d * 16 + p * 4 + q

                @pl.when(target != place)
                def _():
                    map_copy(target).start()

    def run(after_attend, after_chain):
        tokens = local_ref.shape[1]
        with jax.named_scope("x_halo"):
            for side in range(2):
                halo_copy(side).wait()
        lane = iota((1, PAIR), 1)
        low = lane < HD
        front = lane % 32 < 16

        def turned(v, first, last):
            other = jnp.where(front, -pltpu.roll(v, PAIR - 16, 1), pltpu.roll(v, 16, 1))
            return v * cos_ref[first:last, :] + other * sin_ref[first:last, :]

        reach = 3 * tokens
        q_pos = place * tokens + iota((2 * tokens, reach), 0) % tokens
        k_pos = (place - 1) * tokens + iota((2 * tokens, reach), 1)
        allowed = (jnp.abs(q_pos - k_pos) <= WINDOW) & (k_pos >= 0) & (k_pos < count * tokens)
        upper = iota((2 * tokens, 1), 0) < tokens
        pair = lax.axis_index("fs")
        first_head = lax.axis_index("tp") * (2 * FOUR) + 2 * pair
        sink = jnp.where(upper, sink_ref[first_head], sink_ref[first_head + 1])

        def attend(p, carry):
            kv = jnp.concatenate(
                [halo_ref[0, p], proj_ref[p, :, kv_first : kv_first + PAIR], halo_ref[1, p]], axis=0
            ).astype(F32)
            roped = turned(kv, 0, reach)
            swapped = pltpu.roll(kv, HD, 1)
            key = jnp.where(low, roped, pltpu.roll(roped, HD, 1)).astype(BF)
            value = jnp.where(low, swapped, kv).astype(BF)
            query = turned(proj_ref[p, :, kv_first - PAIR : kv_first].astype(F32), tokens, 2 * tokens)
            query = jnp.concatenate([jnp.where(low, query, 0.0), jnp.where(low, 0.0, query)], axis=0)
            scores = dot(query.astype(BF), key, NT) * HD**-0.5
            scores = jnp.where(allowed, scores, -jnp.inf)
            top = jnp.maximum(jnp.max(scores, axis=-1, keepdims=True), sink)
            raised = jnp.exp(scores - top)
            total = jnp.exp(sink - top) + jnp.sum(raised, axis=-1, keepdims=True)
            mixed = dot((raised / total).astype(BF), value)
            att_ref[pair, p] = jnp.where(low, mixed[:tokens], mixed[tokens:]).astype(BF)
            return carry

        with jax.named_scope("x_attend"):
            lax.fori_loop(0, FOUR, attend, 0)

        after_attend()
        recv_ref[place] = msg_ref[place]

        def await_map(k, carry):
            map_arrival((place + k) % count).wait()
            return carry

        with jax.named_scope("x_await_map"):
            lax.fori_loop(1, count, await_map, 0)

        unit_idx = place // 2
        direction, half = unit_idx // 8, place % 2
        rows = HD // 2
        quarter = rows // 2
        start = pl.multiple_of(half * rows, rows)
        groups = 4
        length = count // groups

        def nth(step):
            return direction * (count - 1) + step * (1 - 2 * direction)

        def message(step):
            m = recv_ref[nth(step)].astype(F32)
            return jnp.concatenate([m[:rows, :HD], m[:rows, HD:], m[rows:, :HD], m[rows:, HD:]], axis=0)

        def extend(s, maps):
            longer = []
            for g in range(groups):
                step = message(g * length + s)
                comp_ref[g, s] = maps[g]
                longer.append(maps[g] + mm3(maps[g], step[:HD]) + step)
            return tuple(longer)

        nothing = jnp.zeros((3 * rows, HD), F32)
        with jax.named_scope("x_compose"):
            maps = lax.fori_loop(0, length, extend, (nothing,) * groups)
        state = init_ref[direction, first_head + unit_idx % 2, pl.ds(start, rows), :]

        def dispatch(g):
            def one(s, carry):
                target = nth(g * length + s)

                @pl.when(target != place)
                def _():
                    entry_copy(target).start()

                return carry

            lax.fori_loop(0, length, one, 0)

        with jax.named_scope("x_chain"):
            for g in range(groups):
                for s in range(length):
                    before = comp_ref[g, s]
                    entry = state + mm3(state, before[:HD]) + before[HD:] if s else state
                    sent_ref[nth(g * length + s)] = jnp.concatenate(
                        [entry[:quarter], entry[quarter:]], axis=1
                    ).astype(BF)
                state = state + mm3(state, maps[g][:HD]) + maps[g][HD:]
                if g:
                    dispatch(g - 1)
        enter_ref[place] = sent_ref[place]
        dispatch(groups - 1)
        after_chain()

        def await_entry(k, carry):
            entry_arrival((place + k) % count).wait()
            return carry

        with jax.named_scope("x_await_entry"):
            lax.fori_loop(1, count, await_entry, 0)
        with jax.named_scope("x_finish"):
            finish(reads_ref, local_ref, enter_ref, gain_ref, lin_ref.at[pair])

    return send_halo, send_maps, run


def finish(q_ref, o_ref, enter_ref, gain_ref, mix_ref):
    row = iota((PAIR, PAIR), 0)
    col = iota((PAIR, PAIR), 1)
    same_head = ones_where(row // HD == col // HD)
    low = iota((HD // 4, PAIR), 1) < HD
    start = (lax.axis_index("tp") * FOUR + lax.axis_index("fs")) * PAIR
    gain = gain_ref[:, pl.ds(pl.multiple_of(start, PAIR), PAIR)]
    for p in range(FOUR):
        out = o_ref[p]
        for d in range(2):
            pieces = []
            for hh in range(2):
                for half in range(2):
                    m = enter_ref[d * 16 + p * 4 + hh * 2 + half].astype(F32)
                    turned = pltpu.roll(m, HD, 1)
                    if hh == 0:
                        pieces += [jnp.where(low, m, 0.0), jnp.where(low, turned, 0.0)]
                    else:
                        pieces += [jnp.where(low, 0.0, turned), jnp.where(low, 0.0, m)]
            out = out + mm2(q_ref[d, p], jnp.concatenate(pieces, axis=0).astype(BF), NT)
        centred = out - mm2(out, same_head) * (1.0 / HD)
        spread = mm2(centred * centred, same_head) * (1.0 / HD)
        mix_ref[p] = (centred * lax.rsqrt(spread + GROUP_EPS) * gain).astype(BF)


def project_out(refs, place_of, weight):
    (
        out_ref, lin_ref, total_ref, other_ref, ready_ref, got_ref,
        lin_out, lin_in, half_out, half_in, back_out, back_in,
    ) = refs
    f, c = place_of[2:]
    tokens, columns = total_ref.shape[1:]
    start, relay, arrive_near, arrive_far, finish_sends = ring_of_four(lin_ref, lin_out, lin_in)
    start()
    with jax.named_scope("o_lin_wait"):
        relay()
        arrive_near()
        arrive_far()
    half = tokens // 2
    theirs = pl.ds(pl.multiple_of((1 - c) * half, half), half)
    ours = pl.ds(pl.multiple_of(c * half, half), half)

    def half_copy(p):
        return pltpu.make_async_remote_copy(
            src_ref=total_ref.at[p, theirs, :], dst_ref=other_ref.at[p],
            send_sem=half_out.at[p], recv_sem=half_in.at[p],
            device_id={"tp": 1 - c}, device_id_type=MESH,
        )

    with jax.named_scope("o_lin"):
        for p in range(FOUR):
            joined = jnp.concatenate([lin_ref[g, p] for g in range(FOUR)], axis=1)
            total_ref[p] += dot(joined, weight, NT)
            half_copy(p).start()

    def back_copy(target, source):
        return pltpu.make_async_remote_copy(
            src_ref=ready_ref.at[target], dst_ref=got_ref.at[source],
            send_sem=back_out.at[target], recv_sem=back_in.at[source],
            device_id={"fs": target}, device_id_type=MESH,
        )

    with jax.named_scope("o_half"):
        for p in range(FOUR):
            half_copy(p).wait_recv()
            ready_ref[p] = (total_ref[p, ours, :] + other_ref[p]).astype(BF)

            @pl.when(f != p)
            def _():
                back_copy(p, f).start()

    got_ref[f] = ready_ref[f]
    finish_sends()
    wide = FOUR * PAIR
    source, target = iota((wide, wide), 0), iota((wide, wide), 1)
    place = source % PAIR // 16 * (FOUR * 16) + source // PAIR * 16 + source % 16
    shuffle = ones_where(place == target)
    with jax.named_scope("o_back"):
        for k in range(1, FOUR):
            back_copy((f + k) % FOUR, (f + k) % FOUR).wait_recv()
    with jax.named_scope("o_shuffle"):
        for b in range(columns // PAIR):
            lanes = slice(b * PAIR, (b + 1) * PAIR)
            joined = jnp.concatenate([got_ref[g, :, lanes] for g in range(FOUR)], axis=1)
            out_ref[:, b * wide : (b + 1) * wide] = dot(joined, shuffle).astype(BF)
    with jax.named_scope("o_drain"):
        for p in range(FOUR):
            half_copy(p).wait_send()
        for k in range(1, FOUR):
            back_copy((f + k) % FOUR, f).wait_send()


def layer_kernel(
    x_ref, gain_ref, wr_ref, wk_ref, wv_ref, wq_ref, wak_ref, wav_ref, down_d_hbm, down_e_hbm,
    up_d_hbm, up_e_hbm, off_d_ref, off_e_ref, extra_ref, init_hbm, head_gain_ref, sink_ref,
    lin_out_ref, att_out_ref,
    out_ref,
    both_ref, hid_ref, stage_ref, cols_ref, ext_ref, down_d_ref, down_e_ref, up_d_ref, up_e_ref, init_ref,
    proj_ref, logd_ref, learn_ref, cos_ref, sin_ref, wout_ref,
    reads_ref, local_ref, msg_ref, rows_ref,
    recv_ref, sent_ref, enter_ref, halo_ref, comp_ref,
    lin_ref, att_ref, total_ref, other_ref, ready_ref, got_ref,
    load_sem, late_sem, x_out, x_in, hid_out, hid_in, stage_out, stage_in, ext_out, ext_in,
    z_out, z_in, near_out, near_in, far_out, far_in,
    wz_out, wz_in, wx_out, wx_in,
    out_sem, in_sem, back_out_sem, back_in_sem, halo_out_sem, halo_in_sem,
    lin_out, lin_in, att_out, att_in, half_out, half_in, back_out, back_in,
):
    place_of = tuple(lax.axis_index(a) for a in ("sp_0", "sp_1", "fs", "tp"))
    for peer in neighbours(place_of):
        pl.semaphore_signal(
            pltpu.get_barrier_semaphore(), inc=1, device_id=peer, device_id_type=MESH
        )
    pairs = (
        (down_d_hbm, down_d_ref), (down_e_hbm, down_e_ref), (up_d_hbm, up_d_ref), (up_e_hbm, up_e_ref),
        (init_hbm, init_ref),
    )
    late = [pltpu.make_async_copy(a, b, late_sem.at[k]) for k, (a, b) in enumerate(pairs)]
    width = lin_out_ref.shape[1]
    wout_ref[:, :width] = lin_out_ref[...]
    wout_ref[:, width:] = att_out_ref[...]
    front(
        (
            x_ref, gain_ref, wr_ref, wk_ref, wv_ref, wq_ref, wak_ref, wav_ref, down_d_ref, down_e_ref,
            up_d_ref, up_e_ref, off_d_ref, off_e_ref, extra_ref, proj_ref, logd_ref, learn_ref,
            both_ref, hid_ref, stage_ref, cols_ref, ext_ref, load_sem,
            x_out, x_in, hid_out, hid_in, stage_out, stage_in, ext_out, ext_in,
            z_out, z_in, near_out, near_in, far_out, far_in, cos_ref, sin_ref, late,
        ),
        place_of,
    )
    send_halo, send_maps, run = exchange(
        (
            msg_ref, init_ref, reads_ref, local_ref, head_gain_ref, proj_ref, cos_ref, sin_ref, sink_ref,
            lin_ref, att_ref, recv_ref, sent_ref, enter_ref, halo_ref, comp_ref,
            out_sem, in_sem, back_out_sem, back_in_sem, halo_out_sem, halo_in_sem,
        ),
        place_of,
    )
    await_rows = local_maps(
        (
            proj_ref, logd_ref, learn_ref, wout_ref, reads_ref, local_ref, msg_ref, rows_ref,
            wz_out, wz_in, wx_out, wx_in,
        ),
        place_of,
        send_halo,
        send_maps,
    )
    att_ring = ring_of_four(att_ref, att_out, att_in)
    width = wout_ref.shape[1] // 2
    columns = total_ref.shape[2]

    def weights(first):
        return rows_ref[:, :, :, first : first + width].reshape(columns, width)

    def after_chain():
        start, relay, arrive_near, arrive_far, finish_sends = att_ring
        with jax.named_scope("o_att_wait"):
            relay()
            await_rows()
            arrive_near()
            arrive_far()
        with jax.named_scope("o_att"):
            for p in range(FOUR):
                joined = jnp.concatenate([att_ref[g, p] for g in range(FOUR)], axis=1)
                total_ref[p] = dot(joined, weights(width), NT)

    run(att_ring[0], after_chain)
    att_ring[4]()
    project_out(
        (
            out_ref, lin_ref, total_ref, other_ref, ready_ref, got_ref,
            lin_out, lin_in, half_out, half_in, back_out, back_in,
        ),
        place_of,
        weights(0),
    )


def local(
    inputs, input_norm_gain, receptance_weight, linear_key_weight, linear_value_weight,
    window_query_weight, window_key_weight, window_value_weight, decay_down_weight, decay_up_weight,
    decay_offset, decay_log_extra, erasure_down_weight, erasure_up_weight, erasure_offset,
    initial_state, head_norm_gain, query_sink_logit, linear_output_weight, window_output_weight,
):
    tokens, model = inputs.shape[1], 2 * inputs.shape[2]
    places = lax.axis_size(SP)
    nz, nx = lax.axis_size("sp_0"), lax.axis_size("sp_1")
    rows = receptance_weight.shape[0]
    out_rows = linear_output_weight.shape[1]
    columns = places * out_rows
    vmem = pl.BlockSpec(memory_space=pltpu.VMEM)
    hbm = pl.BlockSpec(memory_space=pl.ANY)
    smem = pl.BlockSpec(memory_space=pltpu.SMEM)
    dma = pltpu.SemaphoreType.DMA
    down_d, down_e = decay_down_weight.T, erasure_down_weight.T

    def space(kind, *shape):
        return pltpu.VMEM(shape, kind)

    out = pl.pallas_call(
        layer_kernel,
        out_shape=jax.ShapeDtypeStruct((tokens // 2, FOUR * columns), BF),
        in_specs=[hbm, vmem, hbm, hbm, hbm, hbm, vmem, vmem, hbm, hbm, hbm, hbm, vmem, vmem, hbm, hbm, vmem, smem, vmem, vmem],
        out_specs=vmem,
        scratch_shapes=[
            space(BF, 2, tokens, model // 2),
            space(BF, FOUR, tokens, model),
            space(BF, FOUR, rows, 5 * PAIR),
            space(BF, places, FOUR * rows, 5 * PAIR),
            space(F32, FOUR, *decay_log_extra.shape[1:]),
            space(BF, *down_d.shape),
            space(BF, *down_e.shape),
            space(BF, *decay_up_weight.shape),
            space(BF, *erasure_up_weight.shape),
            space(F32, *initial_state.shape),
            space(BF, FOUR, tokens, 5 * PAIR),
            space(F32, 2, FOUR, tokens, PAIR),
            space(F32, 2, FOUR, tokens, PAIR),
            space(F32, tokens + 2 * WINDOW, PAIR),
            space(F32, tokens + 2 * WINDOW, PAIR),
            space(BF, out_rows, 2 * FOUR * PAIR),
            space(F32, 2, FOUR, tokens, PAIR),
            space(F32, FOUR, tokens, PAIR),
            space(BF, places, 48, PAIR),
            space(BF, nz, nx, out_rows, 2 * FOUR * PAIR),
            space(BF, places, 48, PAIR),
            space(BF, places, 16, PAIR),
            space(BF, places, 16, PAIR),
            space(BF, 2, FOUR, tokens, PAIR),
            space(F32, 4, places // 4, 3 * HD // 2, HD),
            space(BF, FOUR, FOUR, tokens, PAIR),
            space(BF, FOUR, FOUR, tokens, PAIR),
            space(F32, FOUR, tokens, columns),
            space(F32, FOUR, tokens // 2, columns),
            space(BF, FOUR, tokens // 2, columns),
            space(BF, FOUR, tokens // 2, columns),
            dma((18,)), dma((5,)),
            dma, dma, dma((6,)), dma((6,)), dma((FOUR,)), dma((FOUR,)), dma((FOUR,)), dma((FOUR,)),
            dma((2, nz // 2)), dma((2, nz // 2)), dma((nz, 2)), dma((nz, 2)), dma((nz,)), dma((nz,)),
            dma((nz,)), dma((nz,)), dma((nx,)), dma((nx,)),
            dma((places,)), dma((places,)), dma((places,)), dma((places,)), dma((2,)), dma((2,)),
            dma((6,)), dma((6,)), dma((6,)), dma((6,)), dma((FOUR,)), dma((FOUR,)), dma((FOUR,)), dma((FOUR,)),
        ],
        compiler_params=pltpu.CompilerParams(
            collective_id=0, has_side_effects=True, vmem_limit_bytes=63 * 2**20
        ),
        name="layer",
    )(
        inputs[0], input_norm_gain[None], receptance_weight, linear_key_weight, linear_value_weight,
        window_query_weight, window_key_weight, window_value_weight, down_d, down_e,
        decay_up_weight, erasure_up_weight, decay_offset, erasure_offset, decay_log_extra,
        initial_state, head_norm_gain[None], query_sink_logit, linear_output_weight.T,
        window_output_weight.T,
    )
    return out[None]


def solution(mesh):
    finer = Mesh(
        mesh.devices.reshape(8, 4, mesh.shape["fs"], mesh.shape["tp"]), ("sp_0", "sp_1", "fs", "tp")
    )
    placed = (
        P("fs", SP, "tp"),
        P(),
        P(SP_FS, "tp"),
        P(SP_FS, "tp"),
        P(SP_FS, "tp"),
        P(SP_FS, "tp"),
        P(SP_FS, "tp"),
        P(SP_FS, "tp"),
        P(),
        P(),
        P(),
        P("fs", "tp", SP),
        P(),
        P(),
        P(),
        P(),
        P(),
        P(),
        P("tp", SP_FS),
        P("tp", SP_FS),
    )
    return jax.shard_map(
        local, mesh=finer, in_specs=placed, out_specs=P("fs", SP_TP, None), check_vma=False
    )
```

```python
import math
import functools
import jax
import jax.numpy as jnp
from jax import lax
from jax.experimental import pallas as pl
from jax.experimental.pallas import tpu as pltpu

from jax.sharding import Mesh
from jax.sharding import PartitionSpec as P

HD = 64
CH = 64
PAIR = 128
WINDOW = 128
GRID_W = 64
ATT_BLOCK = 128
SP = ("sp_0", "sp_1")
FOUR = 4
ROUND = 2
SP_FS = ("sp_0", "sp_1", "fs")
SP_TP = ("sp_0", "sp_1", "tp")
NORM_EPS = 1e-06
GROUP_EPS = 0.00064
ROPE_BASE = 10000.0
F32 = jnp.float32
BF = jnp.bfloat16
MESSAGE = jnp.bfloat16
MESH = pl.DeviceIdType.MESH
NN = (((1,), (0,)), ((), ()))
NT = (((1,), (1,)), ((), ()))
TN = (((0,), (0,)), ((), ()))


def dot(a, b, dims=NN):
    return lax.dot_general(a, b, dims, preferred_element_type=F32)


def split2(a):
    high = a.astype(BF)
    return high, (a - high.astype(F32)).astype(BF)


def split3(a):
    high, rest = a.astype(BF), None
    rest = a - high.astype(F32)
    mid = rest.astype(BF)
    return high, mid, (rest - mid.astype(F32)).astype(BF)


def mm3(a, b, dims=NN):
    (ka,), (kb,) = dims[0]
    a_hi, a_lo = split2(a)
    b_hi, b_lo = split2(b)
    free = 1 - kb
    if b.shape[free] == PAIR:
        upper = jnp.concatenate([b_hi, b_lo], axis=free)
        lower = jnp.concatenate([b_hi, jnp.zeros_like(b_lo)], axis=free)
        wide = dot(
            jnp.concatenate([a_hi, a_lo], axis=ka), jnp.concatenate([upper, lower], axis=kb), dims
        )
        return wide[:, :PAIR] + wide[:, PAIR:]
    main = dot(
        jnp.concatenate([a_hi, a_lo], axis=ka), jnp.concatenate([b_hi, b_hi], axis=kb), dims
    )
    return main + dot(a_hi, b_lo, dims)


def mm2(a, b_exact, dims=NN):
    (ka,), (kb,) = dims[0]
    a_hi, a_lo = split2(a)
    return dot(
        jnp.concatenate([a_hi, a_lo], axis=ka), jnp.concatenate([b_exact, b_exact], axis=kb), dims
    )


def iota(shape, dim):
    return lax.broadcasted_iota(jnp.int32, shape, dim)


def ones_where(cond):
    return jnp.where(cond, 1.0, 0.0).astype(BF)


def settle(where, sem):
    pltpu.make_async_copy(where, where, sem).wait()


def ring_of_four(buf, out_sem, in_sem, give_ref=None, core=None):
    me = lax.axis_index("fs")
    right, left, far = (me + 1) % FOUR, (me + 3) % FOUR, (me + 2) % FOUR
    half = buf.shape[1] // 2
    near_buf = buf if give_ref is None else give_ref[1]

    def piece(block, part, target, number):
        where = buf.at[block, part * half : (part + 1) * half]
        return pltpu.make_async_remote_copy(
            src_ref=where, dst_ref=where, send_sem=out_sem.at[0], recv_sem=in_sem.at[number],
            device_id={"fs": target}, device_id_type=MESH,
        )

    def launch(part, target, number):
        if give_ref is None:
            piece(me, part, target, number).start()
            return
        rows = slice(part * half, (part + 1) * half)
        pltpu.make_async_remote_copy(
            src_ref=give_ref[0].at[rows], dst_ref=near_buf.at[me, rows],
            send_sem=out_sem.at[0], recv_sem=in_sem.at[number],
            device_id={"fs": target, "tp": core}, device_id_type=MESH,
        ).start()

    def start():
        launch(0, right, 0)
        launch(1, left, 1)
        launch(1, right, 2)
        launch(0, left, 2)

    def relay():
        piece(left, 0, right, 0).wait_recv()
        piece(left, 0, right, 3).start()
        piece(right, 1, left, 1).wait_recv()
        piece(right, 1, left, 3).start()

    def arrive_near():
        settle(buf.at[0], in_sem.at[2])

    def arrive_far():
        settle(buf.at[0], in_sem.at[3])

    def finish_sends():
        settle(buf.at[0:3], out_sem.at[0])

    return start, relay, arrive_near, arrive_far, finish_sends


def peer_id(index):
    inner = lax.axis_size("sp_1")
    return {"sp_0": index // inner, "sp_1": index % inner}


def neighbours(place_of):
    z, x, f, c = place_of
    nz, nx = lax.axis_size("sp_0"), lax.axis_size("sp_1")
    peers = [{"fs": (f + k) % FOUR} for k in range(1, FOUR)] + [{"tp": 1 - c}]
    peers += [{"sp_0": (z + k) % nz} for k in (1, nz - 1)]
    return peers + [{"sp_1": (x + k) % nx} for k in (1, nx - 1)]


def rope_tables(place, cos_ref, sin_ref):
    reach = cos_ref.shape[0]
    block = reach // 3
    spot = iota((reach, PAIR), 0)
    lane = iota((reach, PAIR), 1)
    grid_row = ((place - 1) * (block // GRID_W) + spot // GRID_W).astype(F32)
    grid_col = (spot % GRID_W).astype(F32)
    power = (lane % 16).astype(F32) * (1.0 / 16)
    angle = jnp.where(lane % HD < HD // 2, grid_row, grid_col) * jnp.exp(power * -math.log(ROPE_BASE))
    cos_ref[...] = jnp.cos(angle)
    sin_ref[...] = jnp.sin(angle)


def share(ref, give_ref, ring_sems, give_sems, place_of):
    f, c = place_of[2:]
    own = ring_of_four(ref.at[c], *ring_sems[0])
    other = ring_of_four(ref.at[1 - c], *ring_sems[1], (give_ref, ref.at[c]), 1 - c)

    def give(core):
        return pltpu.make_async_remote_copy(
            src_ref=give_ref, dst_ref=ref.at[core, f], send_sem=give_sems[0], recv_sem=give_sems[1],
            device_id={"tp": 1 - c}, device_id_type=MESH,
        )

    def start():
        own[0]()
        other[0]()
        give(c).start()

    def collect():
        own[1]()
        other[1]()
        give(1 - c).wait_recv()
        for ring in (own, other):
            ring[2]()
            ring[3]()

    def drain():
        give(c).wait_send()
        own[4]()
        other[4]()

    return start, collect, drain


def front(refs, place_of):
    (
        x_ref, gain_ref, wr_ref, wk_ref, wv_ref, wq_ref, wak_ref, wav_ref, down_d_ref, down_e_ref,
        up_d_ref, up_e_ref, off_d_ref, off_e_ref, extra_ref, proj_ref, logd_ref, learn_ref,
        both_ref, hid_ref, stage_ref, cols_ref, ext_ref, load_sem,
        x_out, x_in, hid_out, hid_in, stage_out, stage_in, ext_out, ext_in,
        ring_out, z_in, near_in, far_in, cos_ref, sin_ref, late, start_rows,
    ) = refs
    z, x, f, c = place_of
    nz, nx = lax.axis_size("sp_0"), lax.axis_size("sp_1")
    mine = z * nx + x
    rows = wr_ref.shape[0]
    loads = []
    for g in range(FOUR):
        for k, ref in enumerate((wr_ref, wk_ref, wv_ref, wq_ref)):
            loads.append((ref.at[:, g * PAIR : (g + 1) * PAIR], stage_ref.at[g, :, k * PAIR : (k + 1) * PAIR], 0))
    loads.append((x_ref, both_ref.at[c], 1))
    loads.append((extra_ref.at[0], ext_ref.at[f], 2))
    loads = [pltpu.make_async_copy(start, end, load_sem.at[number]) for start, end, number in loads]
    for load in loads:
        load.start()
    for load in late:
        load.start()
    low = iota((rows, PAIR), 1) < HD
    keys, values = wak_ref[...].astype(F32), wav_ref[...].astype(F32)
    shared = [
        jnp.where(low, keys, pltpu.roll(values, HD, 1)).astype(BF),
        jnp.where(low, pltpu.roll(keys, HD, 1), values).astype(BF),
    ]
    for g in range(FOUR):
        stage_ref[g, :, 4 * PAIR :] = shared[g // 2]
    with jax.named_scope("f_load"):
        settle(stage_ref.at[:, :, : 4 * PAIR], load_sem.at[0])
        for load in loads[-2:]:
            load.wait()
    my_rows = pl.ds(pl.multiple_of(f * rows, rows), rows)
    cols_ref[mine, my_rows, :] = stage_ref[f]
    with jax.named_scope("f_meet"):
        pl.semaphore_wait(pltpu.get_barrier_semaphore(), len(neighbours(place_of)))

    half_copy = pltpu.make_async_remote_copy(
        src_ref=both_ref.at[c], dst_ref=both_ref.at[c], send_sem=x_out, recv_sem=x_in,
        device_id={"tp": 1 - c}, device_id_type=MESH,
    )
    half_copy.start()

    def stage_copy(k):
        g = (f + k) % FOUR
        return pltpu.make_async_remote_copy(
            src_ref=stage_ref.at[g], dst_ref=cols_ref.at[mine, my_rows, :],
            send_sem=stage_out, recv_sem=stage_in, device_id={"fs": g}, device_id_type=MESH,
        )

    def ext_copy(k, source):
        return pltpu.make_async_remote_copy(
            src_ref=ext_ref.at[source], dst_ref=ext_ref.at[source],
            send_sem=ext_out, recv_sem=ext_in, device_id={"fs": (f + k) % FOUR}, device_id_type=MESH,
        )

    for k in range(1, FOUR):
        stage_copy(k).start()

    def z_block(k):
        if k == 0:
            return z
        step = (k - 1) // 2
        return (z + nz - 1 - step) % nz if k % 2 else (z + 1 + step) % nz

    def z_copy(k_from, side, step):
        where = cols_ref.at[z_block(k_from) * nx + x]
        return pltpu.make_async_remote_copy(
            src_ref=where, dst_ref=where, send_sem=ring_out, recv_sem=z_in.at[side, step],
            device_id={"sp_0": (z + (1 if side == 0 else nz - 1)) % nz}, device_id_type=MESH,
        )

    def near_copy(k, side, column):
        where = cols_ref.at[z_block(k) * nx + column]
        return pltpu.make_async_remote_copy(
            src_ref=where, dst_ref=where, send_sem=ring_out, recv_sem=near_in.at[k],
            device_id={"sp_1": (x + (1 if side == 0 else nx - 1)) % nx}, device_id_type=MESH,
        )

    def far_copy(k, column):
        where = cols_ref.at[z_block(k) * nx + column]
        return pltpu.make_async_remote_copy(
            src_ref=where, dst_ref=where, send_sem=ring_out, recv_sem=far_in,
            device_id={"sp_1": (x + (1 if k % 2 == 0 else nx - 1)) % nx}, device_id_type=MESH,
        )

    left, right, _ = (x + nx - 1) % nx, (x + 1) % nx, 0

    def spread(k):
        near_copy(k, 0, x).start()
        near_copy(k, 1, x).start()

    def pass_on(k):
        settle(cols_ref.at[0:2], near_in.at[k])
        far_copy(k, left if k % 2 == 0 else right).start()

    with jax.named_scope("f_stage_wait"):
        settle(stage_ref.at[1:FOUR], stage_in)
    z_copy(0, 0, 0).start()
    z_copy(0, 1, 0).start()
    spread(0)

    with jax.named_scope("f_norm"):
        half_copy.wait_recv()
        full = jnp.concatenate([both_ref[0], both_ref[1]], axis=1).astype(F32)
        scale = lax.rsqrt(jnp.mean(full * full, axis=-1, keepdims=True) + NORM_EPS)
        hid_ref[f] = (full * scale * gain_ref[...]).astype(BF)
    start, relay, arrive_near, arrive_far, finish_sends = ring_of_four(hid_ref, hid_out, hid_in)
    for k in range(1, FOUR):
        ext_copy(k, f).start()
    start()
    with jax.named_scope("f_rope"):
        rope_tables(mine, cos_ref, sin_ref)

    steps = nz // 2
    with jax.named_scope("f_ring"):
        for step in range(steps):
            k = 2 * step + 1
            z_copy(k, 0, step).wait_recv()
            if step < steps - 1:
                z_copy(k, 0, step + 1).start()
            spread(k)
            if step < steps - 1:
                z_copy(k + 1, 1, step).wait_recv()
                if step < steps - 2:
                    z_copy(k + 1, 1, step + 1).start()
                spread(k + 1)
            if step == 0:
                pass_on(0)
            else:
                pass_on(k - 2)
                pass_on(k - 1)
            if step == 1:
                relay()
    with jax.named_scope("f_pass_last"):
        pass_on(nz - 1)
    start_rows()
    with jax.named_scope("f_hid_wait"):
        arrive_near()
        arrive_far()
        settle(ext_ref.at[1:FOUR], ext_in)

    for load in late:
        load.wait()
    tokens = hid_ref.shape[1]
    hidden = hid_ref[...].reshape(FOUR * tokens, hid_ref.shape[2])
    with jax.named_scope("f_rates"):
        decay_low = dot(hidden, down_d_ref[...], NT).astype(BF)
        learn_low = dot(hidden, down_e_ref[...], NT).astype(BF)
        decay_act = jnp.tanh(decay_low.astype(F32)).astype(BF)
        heads = ext_ref.shape[1]
        first = c * heads * HD + f * PAIR
        chosen = pl.ds(pl.multiple_of(first, PAIR), PAIR)
        select = ones_where(iota((heads, PAIR), 0) == 2 * f + iota((heads, PAIR), 1) // HD).astype(F32)
        spikes = [
            lax.dot_general(
                ext_ref[p], select, TN, precision=lax.Precision.HIGHEST, preferred_element_type=F32
            )
            for p in range(FOUR)
        ]
        for d in range(2):
            pre = off_d_ref[d : d + 1, chosen] + dot(decay_act, up_d_ref[d, :, chosen])
            softplus = jnp.maximum(-pre, 0.0) + jnp.log1p(jnp.exp(-jnp.abs(pre)))
            rate = jnp.exp(-softplus - 0.5)
            learn = jax.nn.sigmoid(off_e_ref[d : d + 1, chosen] + dot(learn_low, up_e_ref[d, :, chosen]))
            for p in range(FOUR):
                part = slice(p * tokens, (p + 1) * tokens)
                logd_ref[d, p] = spikes[p] - rate[part]
                learn_ref[d, p] = learn[part]

    with jax.named_scope("f_far_wait"):
        settle(cols_ref.at[0:nz], far_in)
    depth = cols_ref.shape[0] * cols_ref.shape[1]
    with jax.named_scope("f_proj"):
        for first_col, last_col in ((0, 256), (256, 512), (512, 640)):
            weight = cols_ref[:, :, first_col:last_col].reshape(depth, last_col - first_col)
            result = dot(hidden, weight).astype(BF)
            for p in range(FOUR):
                proj_ref[p, :, first_col:last_col] = result[p * tokens : (p + 1) * tokens]

    half_copy.wait_send()
    finish_sends()
    settle(stage_ref.at[1:FOUR], stage_out)
    settle(ext_ref.at[1:FOUR], ext_out)
    settle(cols_ref.at[0 : 4 * nz - 1], ring_out)


def stacked(x):
    low = iota(x.shape, 1) < HD
    return jnp.concatenate([jnp.where(low, x, 0.0), jnp.where(low, 0.0, x)], axis=0)


def unstacked(x):
    return x[:CH] + x[CH:]


def gather_rows(refs, place_of):
    wout_ref, rows_ref, z_out, z_in, x_out, x_in, c_out, c_in = refs
    z, x, _, c = place_of
    nz, nx = lax.axis_size("sp_0"), lax.axis_size("sp_1")
    half = nz // 2
    left, right, across = (x + nx - 1) % nx, (x + 1) % nx, (x + 2) % nx

    def z_copy(k, source):
        return pltpu.make_async_remote_copy(
            src_ref=wout_ref, dst_ref=rows_ref.at[c, source, x], send_sem=z_out, recv_sem=z_in,
            device_id={"sp_0": (z + k) % nz}, device_id_type=MESH,
        )

    def x_copy(number, column):
        part = slice(0, nz) if number < 2 else slice(0, half) if number == 2 else slice(half, nz)
        where = rows_ref.at[c, part, column]
        return pltpu.make_async_remote_copy(
            src_ref=where, dst_ref=where, send_sem=x_out, recv_sem=x_in.at[min(number, 2)],
            device_id={"sp_1": right if number % 2 == 0 else left}, device_id_type=MESH,
        )

    def c_copy(number, core, column):
        where = rows_ref.at[core, :, column]
        return pltpu.make_async_remote_copy(
            src_ref=where, dst_ref=where, send_sem=c_out, recv_sem=c_in,
            device_id={"tp": 1 - c}, device_id_type=MESH,
        )

    def first():
        rows_ref[c, z, x] = wout_ref[...]
        for k in range(1, nz):
            z_copy(k, z).start()

    def second():
        settle(rows_ref.at[c, 1:nz, x], z_in)
        x_copy(0, x).start()
        x_copy(1, x).start()
        c_copy(0, c, x).start()

    def third():
        x_copy(0, left).wait_recv()
        x_copy(2, left).start()
        x_copy(1, right).wait_recv()
        x_copy(3, right).start()
        c_copy(1, c, left).start()
        c_copy(2, c, right).start()

    def fourth():
        settle(rows_ref.at[c, :, across], x_in.at[2])
        c_copy(3, c, across).start()

    def last():
        settle(rows_ref.at[1 - c], c_in)
        settle(rows_ref.at[c], c_out)
        settle(rows_ref.at[c, 1:nz, x], z_out)
        settle(rows_ref.at[c, :, 1:nx], x_out)

    return first, second, third, fourth, last


def local_maps(refs, send_halo, send_maps, rows_steps):
    proj_ref, logd_ref, learn_ref, q_ref, o_ref, msg_ref = refs
    rows_steps[1]()
    row = iota((2 * CH, 2 * CH), 0)
    col = iota((2 * CH, 2 * CH), 1)
    t, s = row % CH, col % CH
    eye = row == col
    same_head = ones_where(row // HD == col // HD)
    tri = [ones_where((iota((CH, CH), 0) >= iota((CH, CH), 1))), ones_where((iota((CH, CH), 0) <= iota((CH, CH), 1)))]
    strict = [t > s, t < s]
    within = [t >= s, t <= s]

    def one_round(it, carry):
        @pl.when(it == 1)
        def _():
            for u in range(ROUND):
                send_maps(u)
            send_halo()

        seqs = [it * ROUND + u for u in range(ROUND)]
        recept, keys, values, unit = {}, {}, {}, {}
        for u, p in enumerate(seqs):
            recept[u] = proj_ref[p, :, :PAIR].astype(F32)
            keys[u] = proj_ref[p, :, PAIR : 2 * PAIR].astype(F32)
            values[u] = proj_ref[p, :, 2 * PAIR : 3 * PAIR].astype(F32)
            unit[u] = keys[u] * lax.rsqrt(mm2(keys[u] * keys[u], same_head) + NORM_EPS)
        jobs = [(u, d, c) for u in range(ROUND) for d in range(2) for c in range(2)]
        stage = {}
        for u, d, c in jobs:
            rows = slice(c * CH, (c + 1) * CH)
            logd = logd_ref[d, seqs[u], rows, :]
            parts = jnp.concatenate(split3(logd), axis=0)
            total = dot(jnp.concatenate([tri[d]] * 3, axis=1), parts)
            middle = total[CH // 2 - 1 : CH // 2] if d == 0 else total[CH // 2 : CH // 2 + 1]
            last = total[CH - 1 : CH] if d == 0 else total[0:1]
            grow = jnp.exp(total - middle)
            shrink = jnp.exp(middle - total)
            read = recept[u][rows] * grow
            mark = unit[u][rows] * jnp.exp(total - logd - middle)
            erase = unit[u][rows] * learn_ref[d, seqs[u], rows, :] * shrink
            key = keys[u][rows] * shrink
            read_s, mark_s, erase_s, key_s = map(stacked, (read, mark, erase, key))
            scores = mm3(
                jnp.concatenate([mark_s, read_s], axis=0),
                jnp.concatenate([erase_s, key_s], axis=0),
                NT,
            )
            stage[u, d, c] = (read, mark_s, erase_s, key_s, scores, jnp.exp(middle), jnp.exp(last - middle), jnp.exp(last))
        inverse = {}
        grams = {}
        for u, d, c in jobs:
            gram = jnp.where(strict[d], stage[u, d, c][4][: 2 * CH, : 2 * CH], 0.0)
            grams[u, d, c] = gram
            inverse[u, d, c] = jnp.where(eye, 1.0, 0.0) - jnp.where(t // 2 == s // 2, gram, 0.0)
        block = 2
        while block < CH:
            joins = (t // (2 * block) == s // (2 * block)) & (t // block != s // block)
            for job in jobs:
                found = inverse[job]
                inverse[job] = found - mm3(found, mm3(jnp.where(joins, grams[job], 0.0), found))
            block *= 2
        maps, reads, outs = {}, {}, {}
        for u, d, c in jobs:
            rows = slice(c * CH, (c + 1) * CH)
            read, mark_s, erase_s, key_s, scores, to_start, to_end, whole = stage[u, d, c]
            val_s = stacked(values[u][rows]).astype(BF)
            cross = jnp.where(strict[d], scores[: 2 * CH, 2 * CH :], 0.0)
            read_e = jnp.where(within[d], scores[2 * CH :, : 2 * CH], 0.0)
            read_k = jnp.where(within[d], scores[2 * CH :, 2 * CH :], 0.0)
            solved = mm3(inverse[u, d, c], jnp.concatenate([mark_s, mm2(cross, val_s)], axis=1))
            solved = jnp.concatenate([solved[:, :PAIR] * to_start, solved[:, PAIR:]], axis=1)
            taken = mm3(read_e, solved)
            reads[u, d, c] = read * to_start - unstacked(taken[:, :PAIR])
            outs[u, d, c] = unstacked(mm2(read_k, val_s) - taken[:, PAIR:])
            ended = mm3(solved, erase_s * to_end, TN)
            k_hi, k_lo = split2(key_s * to_end)
            added = dot(jnp.concatenate([val_s, val_s], axis=0), jnp.concatenate([k_hi, k_lo], axis=0), TN)
            prod = jnp.where(eye, whole - 1.0, 0.0) - ended[:PAIR]
            maps[u, d, c] = (prod, added - ended[PAIR:])
        for u, p in enumerate(seqs):
            out_rows = [outs[u, 0, 0] + outs[u, 1, 0], outs[u, 0, 1] + outs[u, 1, 1]]
            for d in range(2):
                first, second = (0, 1) if d == 0 else (1, 0)
                (prod1, add1), (prod2, add2) = maps[u, d, first], maps[u, d, second]
                both = jnp.concatenate([prod1, add1], axis=0)
                through = mm3(reads[u, d, second], both, NT)
                q_ref[d, p, first * CH : (first + 1) * CH, :] = reads[u, d, first]
                q_ref[d, p, second * CH : (second + 1) * CH, :] = reads[u, d, second] + through[:, :PAIR]
                out_rows[second] = out_rows[second] + through[:, PAIR:]
                joined = mm3(both, prod2)
                prod = prod1 + prod2 + joined[:PAIR]
                add = add1 + joined[PAIR:] + add2
                for hh in range(2):
                    for half in range(2):
                        message = jnp.concatenate(
                            [
                                folded(prod, hh, hh * HD, HD // 2),
                                folded(add, hh, hh * HD + half * (HD // 2), HD // 4),
                            ],
                            axis=0,
                        )
                        msg_ref[d * 16 + p * 4 + hh * 2 + half] = message.astype(msg_ref.dtype)
            for c in range(2):
                o_ref[p, c * CH : (c + 1) * CH, :] = out_rows[c]

        return carry

    with jax.named_scope("l_loop"):
        lax.fori_loop(0, FOUR // ROUND, one_round, 0)
    for u in range(ROUND):
        send_maps(FOUR - ROUND + u)
    rows_steps[2]()


def folded(x, hh, first, count):
    upper, lower = x[first : first + count], x[first + count : first + 2 * count]
    if hh == 0:
        return upper + pltpu.roll(lower, HD, 1)
    return pltpu.roll(upper, HD, 1) + lower


def exchange(refs, place_of):
    (
        msg_ref, init_ref, reads_ref, local_ref, gain_ref, proj_ref, cos_ref, sin_ref, sink_ref, lin_ref, att_ref, lin_give, att_give,
        recv_ref, sent_ref, enter_ref, halo_ref, comp_ref,
        out_sem, in_sem, back_out_sem, back_in_sem, halo_out_sem, halo_in_sem,
    ) = refs
    count = recv_ref.shape[0]
    place = place_of[0] * lax.axis_size("sp_1") + place_of[1]
    kv_first = 4 * PAIR

    def halo_copy(side):
        target = (place + count - 1 + 2 * side) % count
        return pltpu.make_async_remote_copy(
            src_ref=proj_ref.at[:, :, kv_first : kv_first + PAIR],
            dst_ref=halo_ref.at[1 - side],
            send_sem=halo_out_sem,
            recv_sem=halo_in_sem,
            device_id=peer_id(target),
            device_id_type=MESH,
        )

    def map_copy(target):
        return pltpu.make_async_remote_copy(
            src_ref=msg_ref.at[target],
            dst_ref=recv_ref.at[place],
            send_sem=out_sem,
            recv_sem=in_sem,
            device_id=peer_id(target),
            device_id_type=MESH,
        )

    def entry_copy(target):
        return pltpu.make_async_remote_copy(
            src_ref=sent_ref.at[target],
            dst_ref=enter_ref.at[place],
            send_sem=back_out_sem,
            recv_sem=back_in_sem,
            device_id=peer_id(target),
            device_id_type=MESH,
        )

    def send_halo():
        halo_copy(0).start()
        halo_copy(1).start()

    def send_maps(p):
        for d in range(2):
            for q in range(4):
                target = d * 16 + p * 4 + q

                @pl.when(target != place)
                def _():
                    map_copy(target).start()

    def run(after_attend, after_chain):
        tokens = local_ref.shape[1]
        with jax.named_scope("x_halo"):
            settle(halo_ref, halo_in_sem)
            settle(halo_ref, halo_out_sem)
        lane = iota((1, PAIR), 1)
        low = lane < HD
        front = lane % 32 < 16

        def turned(v, first, last):
            other = jnp.where(front, -pltpu.roll(v, PAIR - 16, 1), pltpu.roll(v, 16, 1))
            return v * cos_ref[first:last, :] + other * sin_ref[first:last, :]

        reach = 3 * tokens
        q_pos = place * tokens + iota((2 * tokens, reach), 0) % tokens
        k_pos = (place - 1) * tokens + iota((2 * tokens, reach), 1)
        allowed = (jnp.abs(q_pos - k_pos) <= WINDOW) & (k_pos >= 0) & (k_pos < count * tokens)
        upper = iota((2 * tokens, 1), 0) < tokens
        pair = lax.axis_index("fs")
        first_head = lax.axis_index("tp") * (2 * FOUR) + 2 * pair
        sink = jnp.where(upper, sink_ref[first_head], sink_ref[first_head + 1])

        def attend(p, carry):
            kv = jnp.concatenate(
                [halo_ref[0, p], proj_ref[p, :, kv_first : kv_first + PAIR], halo_ref[1, p]], axis=0
            ).astype(F32)
            roped = turned(kv, 0, reach)
            swapped = pltpu.roll(kv, HD, 1)
            key = jnp.where(low, roped, pltpu.roll(roped, HD, 1)).astype(BF)
            value = jnp.where(low, swapped, kv).astype(BF)
            query = turned(proj_ref[p, :, kv_first - PAIR : kv_first].astype(F32), tokens, 2 * tokens)
            query = jnp.concatenate([jnp.where(low, query, 0.0), jnp.where(low, 0.0, query)], axis=0)
            scores = dot(query.astype(BF), key, NT) * HD**-0.5
            scores = jnp.where(allowed, scores, -jnp.inf)
            top = jnp.maximum(jnp.max(scores, axis=-1, keepdims=True), sink)
            raised = jnp.exp(scores - top)
            total = jnp.exp(sink - top) + jnp.sum(raised, axis=-1, keepdims=True)
            mixed = dot((raised / total).astype(BF), value)
            keep(jnp.where(low, mixed[:tokens], mixed[tokens:]).astype(BF), place_of, p, att_ref, att_give)
            return carry

        with jax.named_scope("x_attend"):
            lax.fori_loop(0, FOUR, attend, 0)

        after_attend()
        recv_ref[place] = msg_ref[place]

        with jax.named_scope("x_await_map"):
            settle(recv_ref.at[1:count], in_sem)
            settle(msg_ref.at[1:count], out_sem)

        unit_idx = place // 2
        direction, half = unit_idx // 8, place % 2
        rows = HD // 2
        quarter = rows // 2
        start = pl.multiple_of(half * rows, rows)
        groups = 4
        length = count // groups

        def nth(step):
            return direction * (count - 1) + step * (1 - 2 * direction)

        def message(step):
            m = recv_ref[nth(step)].astype(F32)
            return jnp.concatenate([m[:rows, :HD], m[:rows, HD:], m[rows:, :HD], m[rows:, HD:]], axis=0)

        def extend(s, maps):
            longer = []
            for g in range(groups):
                step = message(g * length + s)
                comp_ref[g, s] = maps[g]
                longer.append(maps[g] + mm3(maps[g], step[:HD]) + step)
            return tuple(longer)

        nothing = jnp.zeros((3 * rows, HD), F32)
        with jax.named_scope("x_compose"):
            maps = lax.fori_loop(0, length, extend, (nothing,) * groups)
        state = init_ref[direction, first_head + unit_idx % 2, pl.ds(start, rows), :]

        def dispatch(g):
            def one(s, carry):
                target = nth(g * length + s)

                @pl.when(target != place)
                def _():
                    entry_copy(target).start()

                return carry

            lax.fori_loop(0, length, one, 0)

        with jax.named_scope("x_chain"):
            for g in range(groups):
                for s in range(length):
                    before = comp_ref[g, s]
                    entry = state + mm3(state, before[:HD]) + before[HD:] if s else state
                    sent_ref[nth(g * length + s)] = jnp.concatenate(
                        [entry[:quarter], entry[quarter:]], axis=1
                    ).astype(BF)
                state = state + mm3(state, maps[g][:HD]) + maps[g][HD:]
                if g:
                    dispatch(g - 1)
        enter_ref[place] = sent_ref[place]
        dispatch(groups - 1)
        after_chain()

        with jax.named_scope("x_await_entry"):
            settle(enter_ref.at[1:count], back_in_sem)
            settle(sent_ref.at[1:count], back_out_sem)
        with jax.named_scope("x_finish"):
            finish(reads_ref, local_ref, enter_ref, gain_ref, lin_ref, lin_give, place_of)

    return send_halo, send_maps, run


def keep(value, place_of, p, mine_ref, give_ref):
    f, c = place_of[2:]
    half = value.shape[0] // 2
    mine_ref[c, f, p] = jnp.where(c == 0, value[:half], value[half:])
    give_ref[p] = jnp.where(c == 0, value[half:], value[:half])


def finish(q_ref, o_ref, enter_ref, gain_ref, lin_ref, lin_give, place_of):
    row = iota((PAIR, PAIR), 0)
    col = iota((PAIR, PAIR), 1)
    same_head = ones_where(row // HD == col // HD)
    low = iota((HD // 4, PAIR), 1) < HD
    start = (lax.axis_index("tp") * FOUR + lax.axis_index("fs")) * PAIR
    gain = gain_ref[:, pl.ds(pl.multiple_of(start, PAIR), PAIR)]
    for p in range(FOUR):
        out = o_ref[p]
        for d in range(2):
            pieces = []
            for hh in range(2):
                for half in range(2):
                    m = enter_ref[d * 16 + p * 4 + hh * 2 + half].astype(F32)
                    turned = pltpu.roll(m, HD, 1)
                    if hh == 0:
                        pieces += [jnp.where(low, m, 0.0), jnp.where(low, turned, 0.0)]
                    else:
                        pieces += [jnp.where(low, 0.0, turned), jnp.where(low, 0.0, m)]
            out = out + mm2(q_ref[d, p], jnp.concatenate(pieces, axis=0).astype(BF), NT)
        centred = out - mm2(out, same_head) * (1.0 / HD)
        spread = mm2(centred * centred, same_head) * (1.0 / HD)
        mix = (centred * lax.rsqrt(spread + GROUP_EPS) * gain).astype(BF)
        keep(mix, place_of, p, lin_ref, lin_give)


def send_back(refs, place_of):
    out_ref, ready_ref, got_ref, back_out, back_in = refs
    f = place_of[2]
    columns = ready_ref.shape[2]

    def back_copy(target, source):
        return pltpu.make_async_remote_copy(
            src_ref=ready_ref.at[target], dst_ref=got_ref.at[source],
            send_sem=back_out, recv_sem=back_in,
            device_id={"fs": target}, device_id_type=MESH,
        )

    for k in range(1, FOUR):
        back_copy((f + k) % FOUR, f).start()
    got_ref[f] = ready_ref[f]
    wide = FOUR * PAIR
    source, target = iota((wide, wide), 0), iota((wide, wide), 1)
    place = source % PAIR // 16 * (FOUR * 16) + source // PAIR * 16 + source % 16
    shuffle = ones_where(place == target)
    with jax.named_scope("o_back"):
        settle(got_ref.at[1:FOUR], back_in)
    with jax.named_scope("o_shuffle"):
        for b in range(columns // PAIR):
            lanes = slice(b * PAIR, (b + 1) * PAIR)
            joined = jnp.concatenate([got_ref[g, :, lanes] for g in range(FOUR)], axis=1)
            out_ref[:, b * wide : (b + 1) * wide] = dot(joined, shuffle).astype(BF)
    with jax.named_scope("o_drain"):
        settle(ready_ref.at[1:FOUR], back_out)


def layer_kernel(
    x_ref, gain_ref, wr_ref, wk_ref, wv_ref, wq_ref, wak_ref, wav_ref, down_d_hbm, down_e_hbm,
    up_d_hbm, up_e_hbm, off_d_ref, off_e_ref, extra_ref, init_hbm, head_gain_ref, sink_ref,
    lin_out_ref, att_out_ref,
    out_ref,
    both_ref, hid_ref, stage_ref, cols_ref, ext_ref, down_d_ref, down_e_ref, up_d_ref, up_e_ref, init_ref,
    proj_ref, logd_ref, learn_ref, cos_ref, sin_ref, wout_ref,
    reads_ref, local_ref, msg_ref, rows_ref,
    recv_ref, sent_ref, enter_ref, halo_ref, comp_ref, total_ref,
    lin_ref, att_ref, lin_give, att_give, ready_ref, got_ref,
    load_sem, late_sem, x_out, x_in, hid_out, hid_in, stage_out, stage_in, ext_out, ext_in,
    ring_out, z_in, near_in, far_in,
    wz_out, wz_in, wx_out, wx_in, wc_out, wc_in,
    out_sem, in_sem, back_out_sem, back_in_sem, halo_out_sem, halo_in_sem,
    lin_out, lin_in, lin_out2, lin_in2, att_out, att_in, att_out2, att_in2, give_sem, back_out, back_in,
):
    place_of = tuple(lax.axis_index(a) for a in ("sp_0", "sp_1", "fs", "tp"))
    for peer in neighbours(place_of):
        pl.semaphore_signal(
            pltpu.get_barrier_semaphore(), inc=1, device_id=peer, device_id_type=MESH
        )
    pairs = (
        (down_d_hbm, down_d_ref), (down_e_hbm, down_e_ref), (up_d_hbm, up_d_ref), (up_e_hbm, up_e_ref),
        (init_hbm, init_ref),
    )
    late = [pltpu.make_async_copy(a, b, late_sem.at[k]) for k, (a, b) in enumerate(pairs)]
    width = lin_out_ref.shape[1]
    wout_ref[:, :width] = lin_out_ref[...]
    wout_ref[:, width:] = att_out_ref[...]
    rows_steps = gather_rows(
        (wout_ref, rows_ref, wz_out, wz_in, wx_out, wx_in, wc_out, wc_in), place_of
    )
    front(
        (
            x_ref, gain_ref, wr_ref, wk_ref, wv_ref, wq_ref, wak_ref, wav_ref, down_d_ref, down_e_ref,
            up_d_ref, up_e_ref, off_d_ref, off_e_ref, extra_ref, proj_ref, logd_ref, learn_ref,
            both_ref, hid_ref, stage_ref, cols_ref, ext_ref, load_sem,
            x_out, x_in, hid_out, hid_in, stage_out, stage_in, ext_out, ext_in,
            ring_out, z_in, near_in, far_in, cos_ref, sin_ref, late, rows_steps[0],
        ),
        place_of,
    )
    send_halo, send_maps, run = exchange(
        (
            msg_ref, init_ref, reads_ref, local_ref, head_gain_ref, proj_ref, cos_ref, sin_ref, sink_ref,
            lin_ref, att_ref, lin_give, att_give, recv_ref, sent_ref, enter_ref, halo_ref, comp_ref,
            out_sem, in_sem, back_out_sem, back_in_sem, halo_out_sem, halo_in_sem,
        ),
        place_of,
    )
    local_maps(
        (proj_ref, logd_ref, learn_ref, reads_ref, local_ref, msg_ref),
        send_halo,
        send_maps,
        rows_steps,
    )
    att_share = share(
        att_ref, att_give, ((att_out, att_in), (att_out2, att_in2)), (give_sem.at[0], give_sem.at[1]), place_of
    )
    lin_share = share(
        lin_ref, lin_give, ((lin_out, lin_in), (lin_out2, lin_in2)), (give_sem.at[2], give_sem.at[3]), place_of
    )
    columns = ready_ref.shape[2]
    joined_rows = FOUR * ready_ref.shape[1]

    def product(ref, first):
        result = None
        for core in range(2):
            left = jnp.concatenate([ref[core, g].reshape(joined_rows, PAIR) for g in range(FOUR)], axis=1)
            weight = rows_ref[core, :, :, :, first : first + width].reshape(columns, width)
            term = dot(left, weight, NT)
            result = term if result is None else result + term
        return result

    def after_chain():
        with jax.named_scope("o_att_wait"):
            att_share[1]()
            rows_steps[4]()
        with jax.named_scope("o_att"):
            total_ref[...] = product(att_ref, width)

    def after_attend():
        att_share[0]()
        rows_steps[3]()

    run(after_attend, after_chain)
    lin_share[0]()
    att_share[2]()
    with jax.named_scope("o_lin_wait"):
        lin_share[1]()
    with jax.named_scope("o_lin"):
        result = (total_ref[...] + product(lin_ref, 0)).astype(BF)
        ready_ref[...] = result.reshape(ready_ref.shape)
    send_back((out_ref, ready_ref, got_ref, back_out, back_in), place_of)
    lin_share[2]()


def local(
    inputs, input_norm_gain, receptance_weight, linear_key_weight, linear_value_weight,
    window_query_weight, window_key_weight, window_value_weight, decay_down_weight, decay_up_weight,
    decay_offset, decay_log_extra, erasure_down_weight, erasure_up_weight, erasure_offset,
    initial_state, head_norm_gain, query_sink_logit, linear_output_weight, window_output_weight,
):
    tokens, model = inputs.shape[1], 2 * inputs.shape[2]
    places = lax.axis_size(SP)
    nz, nx = lax.axis_size("sp_0"), lax.axis_size("sp_1")
    rows = receptance_weight.shape[0]
    out_rows = linear_output_weight.shape[1]
    columns = places * out_rows
    vmem = pl.BlockSpec(memory_space=pltpu.VMEM)
    hbm = pl.BlockSpec(memory_space=pl.ANY)
    smem = pl.BlockSpec(memory_space=pltpu.SMEM)
    dma = pltpu.SemaphoreType.DMA
    down_d, down_e = decay_down_weight.T, erasure_down_weight.T

    def space(kind, *shape):
        return pltpu.VMEM(shape, kind)

    out = pl.pallas_call(
        layer_kernel,
        out_shape=jax.ShapeDtypeStruct((tokens // 2, FOUR * columns), BF),
        in_specs=[hbm, vmem, hbm, hbm, hbm, hbm, vmem, vmem, hbm, hbm, hbm, hbm, vmem, vmem, hbm, hbm, vmem, smem, vmem, vmem],
        out_specs=vmem,
        scratch_shapes=[
            space(BF, 2, tokens, model // 2),
            space(BF, FOUR, tokens, model),
            space(BF, FOUR, rows, 5 * PAIR),
            space(BF, places, FOUR * rows, 5 * PAIR),
            space(F32, FOUR, *decay_log_extra.shape[1:]),
            space(BF, *down_d.shape),
            space(BF, *down_e.shape),
            space(BF, *decay_up_weight.shape),
            space(BF, *erasure_up_weight.shape),
            space(F32, *initial_state.shape),
            space(BF, FOUR, tokens, 5 * PAIR),
            space(F32, 2, FOUR, tokens, PAIR),
            space(F32, 2, FOUR, tokens, PAIR),
            space(F32, tokens + 2 * WINDOW, PAIR),
            space(F32, tokens + 2 * WINDOW, PAIR),
            space(BF, out_rows, 2 * FOUR * PAIR),
            space(F32, 2, FOUR, tokens, PAIR),
            space(F32, FOUR, tokens, PAIR),
            space(BF, places, 48, PAIR),
            space(BF, 2, nz, nx, out_rows, 2 * FOUR * PAIR),
            space(BF, places, 48, PAIR),
            space(BF, places, 16, PAIR),
            space(BF, places, 16, PAIR),
            space(BF, 2, FOUR, tokens, PAIR),
            space(F32, 4, places // 4, 3 * HD // 2, HD),
            space(F32, FOUR * tokens // 2, columns),
            space(BF, 2, FOUR, FOUR, tokens // 2, PAIR),
            space(BF, 2, FOUR, FOUR, tokens // 2, PAIR),
            space(BF, FOUR, tokens // 2, PAIR),
            space(BF, FOUR, tokens // 2, PAIR),
            space(BF, FOUR, tokens // 2, columns),
            space(BF, FOUR, tokens // 2, columns),
            dma((3,)), dma((5,)),
            dma, dma, dma((1,)), dma((4,)), dma, dma, dma, dma,
            dma, dma((2, nz // 2)), dma((nz,)), dma,
            dma, dma, dma, dma((3,)), dma, dma,
            dma, dma, dma, dma, dma, dma,
            *[dma((1,)), dma((4,))] * 4, dma((FOUR,)), dma, dma,
        ],
        compiler_params=pltpu.CompilerParams(
            collective_id=0, has_side_effects=True, vmem_limit_bytes=63 * 2**20
        ),
        name="layer",
    )(
        inputs[0], input_norm_gain[None], receptance_weight, linear_key_weight, linear_value_weight,
        window_query_weight, window_key_weight, window_value_weight, down_d, down_e,
        decay_up_weight, erasure_up_weight, decay_offset, erasure_offset, decay_log_extra,
        initial_state, head_norm_gain[None], query_sink_logit, linear_output_weight.T,
        window_output_weight.T,
    )
    return out[None]


def solution(mesh):
    finer = Mesh(
        mesh.devices.reshape(8, 4, mesh.shape["fs"], mesh.shape["tp"]), ("sp_0", "sp_1", "fs", "tp")
    )
    placed = (
        P("fs", SP, "tp"),
        P(),
        P(SP_FS, "tp"),
        P(SP_FS, "tp"),
        P(SP_FS, "tp"),
        P(SP_FS, "tp"),
        P(SP_FS, "tp"),
        P(SP_FS, "tp"),
        P(),
        P(),
        P(),
        P("fs", "tp", SP),
        P(),
        P(),
        P(),
        P(),
        P(),
        P(),
        P("tp", SP_FS),
        P("tp", SP_FS),
    )
    return jax.shard_map(
        local, mesh=finer, in_specs=placed, out_specs=P("fs", SP_TP, None), check_vma=False
    )
```

```python
import math
import functools
import jax
import jax.numpy as jnp
from jax import lax
from jax.experimental import pallas as pl
from jax.experimental.pallas import tpu as pltpu

from jax.sharding import Mesh
from jax.sharding import PartitionSpec as P

HD = 64
CH = 64
PAIR = 128
WINDOW = 128
GRID_W = 64
ATT_BLOCK = 128
SP = ("sp_0", "sp_1")
FOUR = 4
ROUND = 2
SP_FS = ("sp_0", "sp_1", "fs")
SP_TP = ("sp_0", "sp_1", "tp")
NORM_EPS = 1e-06
GROUP_EPS = 0.00064
ROPE_BASE = 10000.0
F32 = jnp.float32
BF = jnp.bfloat16
MESSAGE = jnp.bfloat16
MESH = pl.DeviceIdType.MESH
NN = (((1,), (0,)), ((), ()))
NT = (((1,), (1,)), ((), ()))
TN = (((0,), (0,)), ((), ()))


def dot(a, b, dims=NN):
    return lax.dot_general(a, b, dims, preferred_element_type=F32)


def split2(a):
    high = a.astype(BF)
    return high, (a - high.astype(F32)).astype(BF)


def split3(a):
    high, rest = a.astype(BF), None
    rest = a - high.astype(F32)
    mid = rest.astype(BF)
    return high, mid, (rest - mid.astype(F32)).astype(BF)


def mm3(a, b, dims=NN):
    (ka,), (kb,) = dims[0]
    a_hi, a_lo = split2(a)
    b_hi, b_lo = split2(b)
    free = 1 - kb
    if b.shape[free] == PAIR:
        upper = jnp.concatenate([b_hi, b_lo], axis=free)
        lower = jnp.concatenate([b_hi, jnp.zeros_like(b_lo)], axis=free)
        wide = dot(
            jnp.concatenate([a_hi, a_lo], axis=ka), jnp.concatenate([upper, lower], axis=kb), dims
        )
        return wide[:, :PAIR] + wide[:, PAIR:]
    main = dot(
        jnp.concatenate([a_hi, a_lo], axis=ka), jnp.concatenate([b_hi, b_hi], axis=kb), dims
    )
    return main + dot(a_hi, b_lo, dims)


def mm2(a, b_exact, dims=NN):
    (ka,), (kb,) = dims[0]
    a_hi, a_lo = split2(a)
    return dot(
        jnp.concatenate([a_hi, a_lo], axis=ka), jnp.concatenate([b_exact, b_exact], axis=kb), dims
    )


def iota(shape, dim):
    return lax.broadcasted_iota(jnp.int32, shape, dim)


def ones_where(cond):
    return jnp.where(cond, 1.0, 0.0).astype(BF)


def settle(where, sem):
    pltpu.make_async_copy(where, where, sem).wait()


def ring_of_four(buf, out_sem, in_sem, give_ref=None, core=None):
    me = lax.axis_index("fs")
    right, left, far = (me + 1) % FOUR, (me + 3) % FOUR, (me + 2) % FOUR
    half = buf.shape[1] // 2
    near_buf = buf if give_ref is None else give_ref[1]

    def piece(block, part, target, number):
        where = buf.at[block, part * half : (part + 1) * half]
        return pltpu.make_async_remote_copy(
            src_ref=where, dst_ref=where, send_sem=out_sem.at[0], recv_sem=in_sem.at[number],
            device_id={"fs": target}, device_id_type=MESH,
        )

    def launch(part, target, number):
        if give_ref is None:
            piece(me, part, target, number).start()
            return
        rows = slice(part * half, (part + 1) * half)
        pltpu.make_async_remote_copy(
            src_ref=give_ref[0].at[rows], dst_ref=near_buf.at[me, rows],
            send_sem=out_sem.at[0], recv_sem=in_sem.at[number],
            device_id={"fs": target, "tp": core}, device_id_type=MESH,
        ).start()

    def start():
        launch(0, right, 0)
        launch(1, left, 1)
        launch(1, right, 2)
        launch(0, left, 2)

    def relay():
        piece(left, 0, right, 0).wait_recv()
        piece(left, 0, right, 3).start()
        piece(right, 1, left, 1).wait_recv()
        piece(right, 1, left, 3).start()

    def arrive_near():
        settle(buf.at[0], in_sem.at[2])

    def arrive_far():
        settle(buf.at[0], in_sem.at[3])

    def finish_sends():
        settle(buf.at[0:3], out_sem.at[0])

    return start, relay, arrive_near, arrive_far, finish_sends


def peer_id(index):
    inner = lax.axis_size("sp_1")
    return {"sp_0": index // inner, "sp_1": index % inner}


def neighbours(place_of):
    z, x, f, c = place_of
    nz, nx = lax.axis_size("sp_0"), lax.axis_size("sp_1")
    peers = [{"fs": (f + k) % FOUR} for k in range(1, FOUR)] + [{"tp": 1 - c}]
    peers += [{"sp_0": (z + k) % nz} for k in (1, nz - 1)]
    return peers + [{"sp_1": (x + k) % nx} for k in range(1, nx)]


def rope_tables(place, cos_ref, sin_ref):
    reach = cos_ref.shape[0]
    block = reach // 3
    spot = iota((reach, PAIR), 0)
    lane = iota((reach, PAIR), 1)
    grid_row = ((place - 1) * (block // GRID_W) + spot // GRID_W).astype(F32)
    grid_col = (spot % GRID_W).astype(F32)
    power = (lane % 16).astype(F32) * (1.0 / 16)
    angle = jnp.where(lane % HD < HD // 2, grid_row, grid_col) * jnp.exp(power * -math.log(ROPE_BASE))
    cos_ref[...] = jnp.cos(angle)
    sin_ref[...] = jnp.sin(angle)


def share(ref, give_ref, ring_sems, give_sems, place_of):
    f, c = place_of[2:]
    own = ring_of_four(ref.at[c], *ring_sems[0])
    other = ring_of_four(ref.at[1 - c], *ring_sems[1], (give_ref, ref.at[c]), 1 - c)

    def give(core):
        return pltpu.make_async_remote_copy(
            src_ref=give_ref, dst_ref=ref.at[core, f], send_sem=give_sems[0], recv_sem=give_sems[1],
            device_id={"tp": 1 - c}, device_id_type=MESH,
        )

    def start():
        own[0]()
        other[0]()
        give(c).start()

    def collect():
        own[1]()
        other[1]()
        give(1 - c).wait_recv()
        for ring in (own, other):
            ring[2]()
            ring[3]()

    def drain():
        give(c).wait_send()
        own[4]()
        other[4]()

    return start, collect, drain


def front(refs, place_of):
    (
        x_ref, gain_ref, wr_ref, wk_ref, wv_ref, wq_ref, wak_ref, wav_ref, down_d_ref, down_e_ref,
        up_d_ref, up_e_ref, off_d_ref, off_e_ref, extra_ref, proj_ref, logd_ref, learn_ref,
        both_ref, hid_ref, stage_ref, cols_ref, ext_ref, load_sem,
        x_out, x_in, hid_out, hid_in, stage_out, stage_in, ext_out, ext_in,
        ring_out, z_in, near_in, far_in, rest_x_out, rest_x_in, rest_z_out, rest_z_in, cos_ref, sin_ref, late,
    ) = refs
    z, x, f, c = place_of
    nz, nx = lax.axis_size("sp_0"), lax.axis_size("sp_1")
    mine = z * nx + x
    rows = wr_ref.shape[0]
    loads = []
    for g in range(FOUR):
        for k, ref in enumerate((wr_ref, wk_ref, wv_ref, wq_ref)):
            loads.append((ref.at[:, g * PAIR : (g + 1) * PAIR], stage_ref.at[g, :, k * PAIR : (k + 1) * PAIR], 0))
    loads.append((x_ref, both_ref.at[c], 1))
    loads.append((extra_ref.at[0], ext_ref.at[f], 2))
    loads = [pltpu.make_async_copy(start, end, load_sem.at[number]) for start, end, number in loads]
    for load in loads:
        load.start()
    for load in late:
        load.start()
    low = iota((rows, PAIR), 1) < HD
    keys, values = wak_ref[...].astype(F32), wav_ref[...].astype(F32)
    shared = [
        jnp.where(low, keys, pltpu.roll(values, HD, 1)).astype(BF),
        jnp.where(low, pltpu.roll(keys, HD, 1), values).astype(BF),
    ]
    for g in range(FOUR):
        stage_ref[g, :, 4 * PAIR :] = shared[g // 2]
    with jax.named_scope("f_load"):
        settle(stage_ref.at[:, :, : 4 * PAIR], load_sem.at[0])
        for load in loads[-2:]:
            load.wait()
    my_rows = pl.ds(pl.multiple_of(f * rows, rows), rows)
    cols_ref[mine, my_rows, :] = stage_ref[f]
    with jax.named_scope("f_meet"):
        pl.semaphore_wait(pltpu.get_barrier_semaphore(), len(neighbours(place_of)))

    half_copy = pltpu.make_async_remote_copy(
        src_ref=both_ref.at[c], dst_ref=both_ref.at[c], send_sem=x_out, recv_sem=x_in,
        device_id={"tp": 1 - c}, device_id_type=MESH,
    )
    half_copy.start()

    def stage_copy(k):
        g = (f + k) % FOUR
        return pltpu.make_async_remote_copy(
            src_ref=stage_ref.at[g], dst_ref=cols_ref.at[mine, my_rows, :],
            send_sem=stage_out, recv_sem=stage_in, device_id={"fs": g}, device_id_type=MESH,
        )

    def ext_copy(k, source):
        return pltpu.make_async_remote_copy(
            src_ref=ext_ref.at[source], dst_ref=ext_ref.at[source],
            send_sem=ext_out, recv_sem=ext_in, device_id={"fs": (f + k) % FOUR}, device_id_type=MESH,
        )

    for k in range(1, FOUR):
        stage_copy(k).start()

    def z_block(k):
        if k == 0:
            return z
        step = (k - 1) // 2
        return (z + nz - 1 - step) % nz if k % 2 else (z + 1 + step) % nz

    main = 3 * PAIR

    def rest_x_copy(k):
        where = cols_ref.at[mine, :, main:]
        return pltpu.make_async_remote_copy(
            src_ref=where, dst_ref=where, send_sem=rest_x_out, recv_sem=rest_x_in,
            device_id={"sp_1": (x + k) % nx}, device_id_type=MESH,
        )

    def rest_z_copy(block, side, step):
        where = cols_ref.at[pl.ds(block * nx, nx), :, main:]
        return pltpu.make_async_remote_copy(
            src_ref=where, dst_ref=where, send_sem=rest_z_out, recv_sem=rest_z_in.at[side, step],
            device_id={"sp_0": (z + (1 if side == 0 else nz - 1)) % nz}, device_id_type=MESH,
        )

    def rest_begin():
        settle(cols_ref.at[0 : nx - 1, :, main:], rest_x_in)
        rest_z_copy(z, 0, 0).start()
        rest_z_copy(z, 1, 0).start()

    def rest_pass(step):
        for side, last in ((0, nz // 2 - 1), (1, nz // 2 - 2)):
            if step <= last:
                block = z_block(2 * step + 1 + side)
                rest_z_copy(block, side, step).wait_recv()
                if step < last:
                    rest_z_copy(block, side, step + 1).start()

    def z_copy(k_from, side, step):
        where = cols_ref.at[z_block(k_from) * nx + x, :, :main]
        return pltpu.make_async_remote_copy(
            src_ref=where, dst_ref=where, send_sem=ring_out, recv_sem=z_in.at[side, step],
            device_id={"sp_0": (z + (1 if side == 0 else nz - 1)) % nz}, device_id_type=MESH,
        )

    def near_copy(k, side, column):
        where = cols_ref.at[z_block(k) * nx + column, :, :main]
        return pltpu.make_async_remote_copy(
            src_ref=where, dst_ref=where, send_sem=ring_out, recv_sem=near_in.at[k],
            device_id={"sp_1": (x + (1 if side == 0 else nx - 1)) % nx}, device_id_type=MESH,
        )

    def far_copy(k, column):
        where = cols_ref.at[z_block(k) * nx + column, :, :main]
        return pltpu.make_async_remote_copy(
            src_ref=where, dst_ref=where, send_sem=ring_out, recv_sem=far_in,
            device_id={"sp_1": (x + (1 if k % 2 == 0 else nx - 1)) % nx}, device_id_type=MESH,
        )

    left, right, _ = (x + nx - 1) % nx, (x + 1) % nx, 0

    def spread(k):
        near_copy(k, 0, x).start()
        near_copy(k, 1, x).start()

    def pass_on(k):
        settle(cols_ref.at[0:2, :, :main], near_in.at[k])
        far_copy(k, left if k % 2 == 0 else right).start()

    with jax.named_scope("f_stage_wait"):
        settle(stage_ref.at[1:FOUR], stage_in)
    z_copy(0, 0, 0).start()
    z_copy(0, 1, 0).start()
    spread(0)
    for k in range(1, nx):
        rest_x_copy(k).start()

    with jax.named_scope("f_norm"):
        half_copy.wait_recv()
        full = jnp.concatenate([both_ref[0], both_ref[1]], axis=1).astype(F32)
        scale = lax.rsqrt(jnp.mean(full * full, axis=-1, keepdims=True) + NORM_EPS)
        hid_ref[f] = (full * scale * gain_ref[...]).astype(BF)
    start, relay, arrive_near, arrive_far, finish_sends = ring_of_four(hid_ref, hid_out, hid_in)
    for k in range(1, FOUR):
        ext_copy(k, f).start()
    start()
    with jax.named_scope("f_rope"):
        rope_tables(mine, cos_ref, sin_ref)

    steps = nz // 2
    with jax.named_scope("f_ring"):
        for step in range(steps):
            k = 2 * step + 1
            z_copy(k, 0, step).wait_recv()
            if step < steps - 1:
                z_copy(k, 0, step + 1).start()
            spread(k)
            if step < steps - 1:
                z_copy(k + 1, 1, step).wait_recv()
                if step < steps - 2:
                    z_copy(k + 1, 1, step + 1).start()
                spread(k + 1)
            if step == 0:
                pass_on(0)
            else:
                pass_on(k - 2)
                pass_on(k - 1)
            if step == 0:
                rest_begin()
            elif step > 1:
                rest_pass(step - 2)
            if step == 1:
                relay()
    with jax.named_scope("f_pass_last"):
        pass_on(nz - 1)
    with jax.named_scope("f_hid_wait"):
        arrive_near()
        arrive_far()
        settle(ext_ref.at[1:FOUR], ext_in)

    for load in late:
        load.wait()
    tokens = hid_ref.shape[1]
    hidden = hid_ref[...].reshape(FOUR * tokens, hid_ref.shape[2])
    with jax.named_scope("f_rates"):
        decay_low = dot(hidden, down_d_ref[...], NT).astype(BF)
        learn_low = dot(hidden, down_e_ref[...], NT).astype(BF)
        decay_act = jnp.tanh(decay_low.astype(F32)).astype(BF)
        heads = ext_ref.shape[1]
        first = c * heads * HD + f * PAIR
        chosen = pl.ds(pl.multiple_of(first, PAIR), PAIR)
        select = ones_where(iota((heads, PAIR), 0) == 2 * f + iota((heads, PAIR), 1) // HD).astype(F32)
        spikes = [
            lax.dot_general(
                ext_ref[p], select, TN, precision=lax.Precision.HIGHEST, preferred_element_type=F32
            )
            for p in range(FOUR)
        ]
        for d in range(2):
            pre = off_d_ref[d : d + 1, chosen] + dot(decay_act, up_d_ref[d, :, chosen])
            softplus = jnp.maximum(-pre, 0.0) + jnp.log1p(jnp.exp(-jnp.abs(pre)))
            rate = jnp.exp(-softplus - 0.5)
            learn = jax.nn.sigmoid(off_e_ref[d : d + 1, chosen] + dot(learn_low, up_e_ref[d, :, chosen]))
            for p in range(FOUR):
                part = slice(p * tokens, (p + 1) * tokens)
                logd_ref[d, p] = spikes[p] - rate[part]
                learn_ref[d, p] = learn[part]

    with jax.named_scope("f_far_wait"):
        settle(cols_ref.at[0:nz, :, :main], far_in)
    depth = cols_ref.shape[0] * cols_ref.shape[1]
    with jax.named_scope("f_proj"):
        for first_col, last_col in ((0, 256), (256, 384)):
            weight = cols_ref[:, :, first_col:last_col].reshape(depth, last_col - first_col)
            result = dot(hidden, weight).astype(BF)
            for p in range(FOUR):
                proj_ref[p, :, first_col:last_col] = result[p * tokens : (p + 1) * tokens]

    rest_pass(nz // 2 - 2)
    half_copy.wait_send()
    finish_sends()
    settle(stage_ref.at[1:FOUR], stage_out)
    settle(ext_ref.at[1:FOUR], ext_out)
    settle(cols_ref.at[0 : 4 * nz - 1, :, :main], ring_out)

    def project_rest():
        rest_pass(nz // 2 - 1)
        weight = cols_ref[:, :, main:].reshape(depth, cols_ref.shape[2] - main)
        result = dot(hid_ref[...].reshape(FOUR * tokens, hid_ref.shape[2]), weight).astype(BF)
        for p in range(FOUR):
            proj_ref[p, :, main:] = result[p * tokens : (p + 1) * tokens]
        settle(cols_ref.at[0 : nx - 1, :, main:], rest_x_out)
        settle(cols_ref.at[0 : nx * (nz - 1), :, main:], rest_z_out)

    return project_rest


def stacked(x):
    low = iota(x.shape, 1) < HD
    return jnp.concatenate([jnp.where(low, x, 0.0), jnp.where(low, 0.0, x)], axis=0)


def unstacked(x):
    return x[:CH] + x[CH:]


def gather_rows(refs, place_of):
    wout_ref, rows_ref, z_out, z_in, x_out, x_in, c_out, c_in = refs
    z, x, _, c = place_of
    nz, nx = lax.axis_size("sp_0"), lax.axis_size("sp_1")
    half = nz // 2
    left, right, across = (x + nx - 1) % nx, (x + 1) % nx, (x + 2) % nx

    def z_copy(k, source):
        return pltpu.make_async_remote_copy(
            src_ref=wout_ref, dst_ref=rows_ref.at[c, source, x], send_sem=z_out, recv_sem=z_in,
            device_id={"sp_0": (z + k) % nz}, device_id_type=MESH,
        )

    def x_copy(number, column):
        part = slice(0, nz) if number < 2 else slice(0, half) if number == 2 else slice(half, nz)
        where = rows_ref.at[c, part, column]
        return pltpu.make_async_remote_copy(
            src_ref=where, dst_ref=where, send_sem=x_out, recv_sem=x_in.at[min(number, 2)],
            device_id={"sp_1": right if number % 2 == 0 else left}, device_id_type=MESH,
        )

    def c_copy(number, core, column):
        where = rows_ref.at[core, :, column]
        return pltpu.make_async_remote_copy(
            src_ref=where, dst_ref=where, send_sem=c_out, recv_sem=c_in,
            device_id={"tp": 1 - c}, device_id_type=MESH,
        )

    def first():
        rows_ref[c, z, x] = wout_ref[...]
        for k in range(1, nz):
            z_copy(k, z).start()

    def second():
        settle(rows_ref.at[c, 1:nz, x], z_in)
        x_copy(0, x).start()
        x_copy(1, x).start()
        c_copy(0, c, x).start()

    def third():
        x_copy(0, left).wait_recv()
        x_copy(2, left).start()
        x_copy(1, right).wait_recv()
        x_copy(3, right).start()
        c_copy(1, c, left).start()
        c_copy(2, c, right).start()

    def fourth():
        settle(rows_ref.at[c, :, across], x_in.at[2])
        c_copy(3, c, across).start()

    def last():
        settle(rows_ref.at[1 - c], c_in)
        settle(rows_ref.at[c], c_out)
        settle(rows_ref.at[c, 1:nz, x], z_out)
        settle(rows_ref.at[c, :, 1:nx], x_out)

    return first, second, third, fourth, last


def local_maps(refs, project_rest, send_halo, send_maps, rows_steps):
    proj_ref, logd_ref, learn_ref, q_ref, o_ref, msg_ref = refs
    rows_steps[0]()
    row = iota((2 * CH, 2 * CH), 0)
    col = iota((2 * CH, 2 * CH), 1)
    t, s = row % CH, col % CH
    eye = row == col
    same_head = ones_where(row // HD == col // HD)
    tri = [ones_where((iota((CH, CH), 0) >= iota((CH, CH), 1))), ones_where((iota((CH, CH), 0) <= iota((CH, CH), 1)))]
    strict = [t > s, t < s]
    within = [t >= s, t <= s]

    def one_round(it, carry):
        @pl.when(it == 1)
        def _():
            project_rest()
            for u in range(ROUND):
                send_maps(u)
            send_halo()

        seqs = [it * ROUND + u for u in range(ROUND)]
        recept, keys, values, unit = {}, {}, {}, {}
        for u, p in enumerate(seqs):
            recept[u] = proj_ref[p, :, :PAIR].astype(F32)
            keys[u] = proj_ref[p, :, PAIR : 2 * PAIR].astype(F32)
            values[u] = proj_ref[p, :, 2 * PAIR : 3 * PAIR].astype(F32)
            unit[u] = keys[u] * lax.rsqrt(mm2(keys[u] * keys[u], same_head) + NORM_EPS)
        jobs = [(u, d, c) for u in range(ROUND) for d in range(2) for c in range(2)]
        stage = {}
        for u, d, c in jobs:
            rows = slice(c * CH, (c + 1) * CH)
            logd = logd_ref[d, seqs[u], rows, :]
            parts = jnp.concatenate(split3(logd), axis=0)
            total = dot(jnp.concatenate([tri[d]] * 3, axis=1), parts)
            middle = total[CH // 2 - 1 : CH // 2] if d == 0 else total[CH // 2 : CH // 2 + 1]
            last = total[CH - 1 : CH] if d == 0 else total[0:1]
            grow = jnp.exp(total - middle)
            shrink = jnp.exp(middle - total)
            read = recept[u][rows] * grow
            mark = unit[u][rows] * jnp.exp(total - logd - middle)
            erase = unit[u][rows] * learn_ref[d, seqs[u], rows, :] * shrink
            key = keys[u][rows] * shrink
            read_s, mark_s, erase_s, key_s = map(stacked, (read, mark, erase, key))
            scores = mm3(
                jnp.concatenate([mark_s, read_s], axis=0),
                jnp.concatenate([erase_s, key_s], axis=0),
                NT,
            )
            stage[u, d, c] = (read, mark_s, erase_s, key_s, scores, jnp.exp(middle), jnp.exp(last - middle), jnp.exp(last))
        inverse = {}
        grams = {}
        for u, d, c in jobs:
            gram = jnp.where(strict[d], stage[u, d, c][4][: 2 * CH, : 2 * CH], 0.0)
            grams[u, d, c] = gram
            inverse[u, d, c] = jnp.where(eye, 1.0, 0.0) - jnp.where(t // 2 == s // 2, gram, 0.0)
        block = 2
        while block < CH:
            joins = (t // (2 * block) == s // (2 * block)) & (t // block != s // block)
            for job in jobs:
                found = inverse[job]
                inverse[job] = found - mm3(found, mm3(jnp.where(joins, grams[job], 0.0), found))
            block *= 2
        maps, reads, outs = {}, {}, {}
        for u, d, c in jobs:
            rows = slice(c * CH, (c + 1) * CH)
            read, mark_s, erase_s, key_s, scores, to_start, to_end, whole = stage[u, d, c]
            val_s = stacked(values[u][rows]).astype(BF)
            cross = jnp.where(strict[d], scores[: 2 * CH, 2 * CH :], 0.0)
            read_e = jnp.where(within[d], scores[2 * CH :, : 2 * CH], 0.0)
            read_k = jnp.where(within[d], scores[2 * CH :, 2 * CH :], 0.0)
            solved = mm3(inverse[u, d, c], jnp.concatenate([mark_s, mm2(cross, val_s)], axis=1))
            solved = jnp.concatenate([solved[:, :PAIR] * to_start, solved[:, PAIR:]], axis=1)
            taken = mm3(read_e, solved)
            reads[u, d, c] = read * to_start - unstacked(taken[:, :PAIR])
            outs[u, d, c] = unstacked(mm2(read_k, val_s) - taken[:, PAIR:])
            ended = mm3(solved, erase_s * to_end, TN)
            k_hi, k_lo = split2(key_s * to_end)
            added = dot(jnp.concatenate([val_s, val_s], axis=0), jnp.concatenate([k_hi, k_lo], axis=0), TN)
            prod = jnp.where(eye, whole - 1.0, 0.0) - ended[:PAIR]
            maps[u, d, c] = (prod, added - ended[PAIR:])
        for u, p in enumerate(seqs):
            out_rows = [outs[u, 0, 0] + outs[u, 1, 0], outs[u, 0, 1] + outs[u, 1, 1]]
            for d in range(2):
                first, second = (0, 1) if d == 0 else (1, 0)
                (prod1, add1), (prod2, add2) = maps[u, d, first], maps[u, d, second]
                both = jnp.concatenate([prod1, add1], axis=0)
                through = mm3(reads[u, d, second], both, NT)
                q_ref[d, p, first * CH : (first + 1) * CH, :] = reads[u, d, first]
                q_ref[d, p, second * CH : (second + 1) * CH, :] = reads[u, d, second] + through[:, :PAIR]
                out_rows[second] = out_rows[second] + through[:, PAIR:]
                joined = mm3(both, prod2)
                prod = prod1 + prod2 + joined[:PAIR]
                add = add1 + joined[PAIR:] + add2
                for hh in range(2):
                    for half in range(2):
                        message = jnp.concatenate(
                            [
                                folded(prod, hh, hh * HD, HD // 2),
                                folded(add, hh, hh * HD + half * (HD // 2), HD // 4),
                            ],
                            axis=0,
                        )
                        msg_ref[d * 16 + p * 4 + hh * 2 + half] = message.astype(msg_ref.dtype)
            for c in range(2):
                o_ref[p, c * CH : (c + 1) * CH, :] = out_rows[c]

        return carry

    with jax.named_scope("l_loop"):
        lax.fori_loop(0, FOUR // ROUND, one_round, 0)
    for u in range(ROUND):
        send_maps(FOUR - ROUND + u)
    rows_steps[1]()


def folded(x, hh, first, count):
    upper, lower = x[first : first + count], x[first + count : first + 2 * count]
    if hh == 0:
        return upper + pltpu.roll(lower, HD, 1)
    return pltpu.roll(upper, HD, 1) + lower


def exchange(refs, place_of):
    (
        msg_ref, init_ref, reads_ref, local_ref, gain_ref, proj_ref, cos_ref, sin_ref, sink_ref, lin_ref, att_ref, lin_give, att_give,
        recv_ref, sent_ref, enter_ref, halo_ref, comp_ref,
        out_sem, in_sem, back_out_sem, back_in_sem, halo_out_sem, halo_in_sem,
    ) = refs
    count = recv_ref.shape[0]
    place = place_of[0] * lax.axis_size("sp_1") + place_of[1]
    kv_first = 4 * PAIR

    def halo_copy(side):
        target = (place + count - 1 + 2 * side) % count
        return pltpu.make_async_remote_copy(
            src_ref=proj_ref.at[:, :, kv_first : kv_first + PAIR],
            dst_ref=halo_ref.at[1 - side],
            send_sem=halo_out_sem,
            recv_sem=halo_in_sem,
            device_id=peer_id(target),
            device_id_type=MESH,
        )

    def map_copy(target):
        return pltpu.make_async_remote_copy(
            src_ref=msg_ref.at[target],
            dst_ref=recv_ref.at[place],
            send_sem=out_sem,
            recv_sem=in_sem,
            device_id=peer_id(target),
            device_id_type=MESH,
        )

    def entry_copy(target):
        return pltpu.make_async_remote_copy(
            src_ref=sent_ref.at[target],
            dst_ref=enter_ref.at[place],
            send_sem=back_out_sem,
            recv_sem=back_in_sem,
            device_id=peer_id(target),
            device_id_type=MESH,
        )

    def send_halo():
        halo_copy(0).start()
        halo_copy(1).start()

    def send_maps(p):
        for d in range(2):
            for q in range(4):
                target = d * 16 + p * 4 + q

                @pl.when(target != place)
                def _():
                    map_copy(target).start()

    def run(after_attend, after_chain):
        tokens = local_ref.shape[1]
        with jax.named_scope("x_halo"):
            settle(halo_ref, halo_in_sem)
            settle(halo_ref, halo_out_sem)
        lane = iota((1, PAIR), 1)
        low = lane < HD
        front = lane % 32 < 16

        def turned(v, first, last):
            other = jnp.where(front, -pltpu.roll(v, PAIR - 16, 1), pltpu.roll(v, 16, 1))
            return v * cos_ref[first:last, :] + other * sin_ref[first:last, :]

        reach = 3 * tokens
        q_pos = place * tokens + iota((2 * tokens, reach), 0) % tokens
        k_pos = (place - 1) * tokens + iota((2 * tokens, reach), 1)
        allowed = (jnp.abs(q_pos - k_pos) <= WINDOW) & (k_pos >= 0) & (k_pos < count * tokens)
        upper = iota((2 * tokens, 1), 0) < tokens
        pair = lax.axis_index("fs")
        first_head = lax.axis_index("tp") * (2 * FOUR) + 2 * pair
        sink = jnp.where(upper, sink_ref[first_head], sink_ref[first_head + 1])

        def attend(p, carry):
            kv = jnp.concatenate(
                [halo_ref[0, p], proj_ref[p, :, kv_first : kv_first + PAIR], halo_ref[1, p]], axis=0
            ).astype(F32)
            roped = turned(kv, 0, reach)
            swapped = pltpu.roll(kv, HD, 1)
            key = jnp.where(low, roped, pltpu.roll(roped, HD, 1)).astype(BF)
            value = jnp.where(low, swapped, kv).astype(BF)
            query = turned(proj_ref[p, :, kv_first - PAIR : kv_first].astype(F32), tokens, 2 * tokens)
            query = jnp.concatenate([jnp.where(low, query, 0.0), jnp.where(low, 0.0, query)], axis=0)
            scores = dot(query.astype(BF), key, NT) * HD**-0.5
            scores = jnp.where(allowed, scores, -jnp.inf)
            top = jnp.maximum(jnp.max(scores, axis=-1, keepdims=True), sink)
            raised = jnp.exp(scores - top)
            total = jnp.exp(sink - top) + jnp.sum(raised, axis=-1, keepdims=True)
            mixed = dot((raised / total).astype(BF), value)
            keep(jnp.where(low, mixed[:tokens], mixed[tokens:]).astype(BF), place_of, p, att_ref, att_give)
            return carry

        with jax.named_scope("x_attend"):
            lax.fori_loop(0, FOUR, attend, 0)

        after_attend()
        recv_ref[place] = msg_ref[place]

        with jax.named_scope("x_await_map"):
            settle(recv_ref.at[1:count], in_sem)
            settle(msg_ref.at[1:count], out_sem)

        unit_idx = place // 2
        direction, half = unit_idx // 8, place % 2
        rows = HD // 2
        quarter = rows // 2
        start = pl.multiple_of(half * rows, rows)
        groups = 4
        length = count // groups

        def nth(step):
            return direction * (count - 1) + step * (1 - 2 * direction)

        def message(step):
            m = recv_ref[nth(step)].astype(F32)
            return jnp.concatenate([m[:rows, :HD], m[:rows, HD:], m[rows:, :HD], m[rows:, HD:]], axis=0)

        def extend(s, maps):
            longer = []
            for g in range(groups):
                step = message(g * length + s)
                comp_ref[g, s] = maps[g]
                longer.append(maps[g] + mm3(maps[g], step[:HD]) + step)
            return tuple(longer)

        nothing = jnp.zeros((3 * rows, HD), F32)
        with jax.named_scope("x_compose"):
            maps = lax.fori_loop(0, length, extend, (nothing,) * groups)
        state = init_ref[direction, first_head + unit_idx % 2, pl.ds(start, rows), :]

        def dispatch(g):
            def one(s, carry):
                target = nth(g * length + s)

                @pl.when(target != place)
                def _():
                    entry_copy(target).start()

                return carry

            lax.fori_loop(0, length, one, 0)

        with jax.named_scope("x_chain"):
            for g in range(groups):
                for s in range(length):
                    before = comp_ref[g, s]
                    entry = state + mm3(state, before[:HD]) + before[HD:] if s else state
                    sent_ref[nth(g * length + s)] = jnp.concatenate(
                        [entry[:quarter], entry[quarter:]], axis=1
                    ).astype(BF)
                state = state + mm3(state, maps[g][:HD]) + maps[g][HD:]
                if g:
                    dispatch(g - 1)
        enter_ref[place] = sent_ref[place]
        dispatch(groups - 1)
        after_chain()

        with jax.named_scope("x_await_entry"):
            settle(enter_ref.at[1:count], back_in_sem)
            settle(sent_ref.at[1:count], back_out_sem)
        with jax.named_scope("x_finish"):
            finish(reads_ref, local_ref, enter_ref, gain_ref, lin_ref, lin_give, place_of)

    return send_halo, send_maps, run


def keep(value, place_of, p, mine_ref, give_ref):
    f, c = place_of[2:]
    half = value.shape[0] // 2
    mine_ref[c, f, p] = jnp.where(c == 0, value[:half], value[half:])
    give_ref[p] = jnp.where(c == 0, value[half:], value[:half])


def finish(q_ref, o_ref, enter_ref, gain_ref, lin_ref, lin_give, place_of):
    row = iota((PAIR, PAIR), 0)
    col = iota((PAIR, PAIR), 1)
    same_head = ones_where(row // HD == col // HD)
    low = iota((HD // 4, PAIR), 1) < HD
    start = (lax.axis_index("tp") * FOUR + lax.axis_index("fs")) * PAIR
    gain = gain_ref[:, pl.ds(pl.multiple_of(start, PAIR), PAIR)]
    for p in range(FOUR):
        out = o_ref[p]
        for d in range(2):
            pieces = []
            for hh in range(2):
                for half in range(2):
                    m = enter_ref[d * 16 + p * 4 + hh * 2 + half].astype(F32)
                    turned = pltpu.roll(m, HD, 1)
                    if hh == 0:
                        pieces += [jnp.where(low, m, 0.0), jnp.where(low, turned, 0.0)]
                    else:
                        pieces += [jnp.where(low, 0.0, turned), jnp.where(low, 0.0, m)]
            out = out + mm2(q_ref[d, p], jnp.concatenate(pieces, axis=0).astype(BF), NT)
        centred = out - mm2(out, same_head) * (1.0 / HD)
        spread = mm2(centred * centred, same_head) * (1.0 / HD)
        mix = (centred * lax.rsqrt(spread + GROUP_EPS) * gain).astype(BF)
        keep(mix, place_of, p, lin_ref, lin_give)


def send_back(refs, place_of):
    out_ref, ready_ref, got_ref, back_out, back_in = refs
    f = place_of[2]
    columns = ready_ref.shape[2]

    def back_copy(target, source):
        return pltpu.make_async_remote_copy(
            src_ref=ready_ref.at[target], dst_ref=got_ref.at[source],
            send_sem=back_out, recv_sem=back_in,
            device_id={"fs": target}, device_id_type=MESH,
        )

    for k in range(1, FOUR):
        back_copy((f + k) % FOUR, f).start()
    got_ref[f] = ready_ref[f]
    wide = FOUR * PAIR
    source, target = iota((wide, wide), 0), iota((wide, wide), 1)
    place = source % PAIR // 16 * (FOUR * 16) + source // PAIR * 16 + source % 16
    shuffle = ones_where(place == target)
    with jax.named_scope("o_back"):
        settle(got_ref.at[1:FOUR], back_in)
    with jax.named_scope("o_shuffle"):
        for b in range(columns // PAIR):
            lanes = slice(b * PAIR, (b + 1) * PAIR)
            joined = jnp.concatenate([got_ref[g, :, lanes] for g in range(FOUR)], axis=1)
            out_ref[:, b * wide : (b + 1) * wide] = dot(joined, shuffle).astype(BF)
    with jax.named_scope("o_drain"):
        settle(ready_ref.at[1:FOUR], back_out)


def layer_kernel(
    x_ref, gain_ref, wr_ref, wk_ref, wv_ref, wq_ref, wak_ref, wav_ref, down_d_hbm, down_e_hbm,
    up_d_hbm, up_e_hbm, off_d_ref, off_e_ref, extra_ref, init_hbm, head_gain_ref, sink_ref,
    lin_out_ref, att_out_ref,
    out_ref,
    both_ref, hid_ref, stage_ref, cols_ref, ext_ref, down_d_ref, down_e_ref, up_d_ref, up_e_ref, init_ref,
    proj_ref, logd_ref, learn_ref, cos_ref, sin_ref, wout_ref,
    reads_ref, local_ref, msg_ref, rows_ref,
    recv_ref, sent_ref, enter_ref, halo_ref, comp_ref, total_ref,
    lin_ref, att_ref, lin_give, att_give, ready_ref, got_ref,
    load_sem, late_sem, x_out, x_in, hid_out, hid_in, stage_out, stage_in, ext_out, ext_in,
    ring_out, z_in, near_in, far_in, rest_x_out, rest_x_in, rest_z_out, rest_z_in,
    wz_out, wz_in, wx_out, wx_in, wc_out, wc_in,
    out_sem, in_sem, back_out_sem, back_in_sem, halo_out_sem, halo_in_sem,
    lin_out, lin_in, lin_out2, lin_in2, att_out, att_in, att_out2, att_in2, give_sem, back_out, back_in,
):
    place_of = tuple(lax.axis_index(a) for a in ("sp_0", "sp_1", "fs", "tp"))
    for peer in neighbours(place_of):
        pl.semaphore_signal(
            pltpu.get_barrier_semaphore(), inc=1, device_id=peer, device_id_type=MESH
        )
    pairs = (
        (down_d_hbm, down_d_ref), (down_e_hbm, down_e_ref), (up_d_hbm, up_d_ref), (up_e_hbm, up_e_ref),
        (init_hbm, init_ref),
    )
    late = [pltpu.make_async_copy(a, b, late_sem.at[k]) for k, (a, b) in enumerate(pairs)]
    width = lin_out_ref.shape[1]
    wout_ref[:, :width] = lin_out_ref[...]
    wout_ref[:, width:] = att_out_ref[...]
    rows_steps = gather_rows(
        (wout_ref, rows_ref, wz_out, wz_in, wx_out, wx_in, wc_out, wc_in), place_of
    )
    project_rest = front(
        (
            x_ref, gain_ref, wr_ref, wk_ref, wv_ref, wq_ref, wak_ref, wav_ref, down_d_ref, down_e_ref,
            up_d_ref, up_e_ref, off_d_ref, off_e_ref, extra_ref, proj_ref, logd_ref, learn_ref,
            both_ref, hid_ref, stage_ref, cols_ref, ext_ref, load_sem,
            x_out, x_in, hid_out, hid_in, stage_out, stage_in, ext_out, ext_in,
            ring_out, z_in, near_in, far_in, rest_x_out, rest_x_in, rest_z_out, rest_z_in, cos_ref, sin_ref, late,
        ),
        place_of,
    )
    send_halo, send_maps, run = exchange(
        (
            msg_ref, init_ref, reads_ref, local_ref, head_gain_ref, proj_ref, cos_ref, sin_ref, sink_ref,
            lin_ref, att_ref, lin_give, att_give, recv_ref, sent_ref, enter_ref, halo_ref, comp_ref,
            out_sem, in_sem, back_out_sem, back_in_sem, halo_out_sem, halo_in_sem,
        ),
        place_of,
    )
    local_maps(
        (proj_ref, logd_ref, learn_ref, reads_ref, local_ref, msg_ref),
        project_rest,
        send_halo,
        send_maps,
        rows_steps,
    )
    att_share = share(
        att_ref, att_give, ((att_out, att_in), (att_out2, att_in2)), (give_sem.at[0], give_sem.at[1]), place_of
    )
    lin_share = share(
        lin_ref, lin_give, ((lin_out, lin_in), (lin_out2, lin_in2)), (give_sem.at[2], give_sem.at[3]), place_of
    )
    columns = ready_ref.shape[2]
    joined_rows = FOUR * ready_ref.shape[1]

    def product(ref, first):
        result = None
        for core in range(2):
            left = jnp.concatenate([ref[core, g].reshape(joined_rows, PAIR) for g in range(FOUR)], axis=1)
            weight = rows_ref[core, :, :, :, first : first + width].reshape(columns, width)
            term = dot(left, weight, NT)
            result = term if result is None else result + term
        return result

    def after_attend():
        att_share[0]()

    run(after_attend, rows_steps[2])
    lin_share[0]()
    rows_steps[3]()
    with jax.named_scope("o_att_wait"):
        att_share[1]()
        rows_steps[4]()
    with jax.named_scope("o_att"):
        total_ref[...] = product(att_ref, width)
    att_share[2]()
    with jax.named_scope("o_lin_wait"):
        lin_share[1]()
    with jax.named_scope("o_lin"):
        result = (total_ref[...] + product(lin_ref, 0)).astype(BF)
        ready_ref[...] = result.reshape(ready_ref.shape)
    send_back((out_ref, ready_ref, got_ref, back_out, back_in), place_of)
    lin_share[2]()


def local(
    inputs, input_norm_gain, receptance_weight, linear_key_weight, linear_value_weight,
    window_query_weight, window_key_weight, window_value_weight, decay_down_weight, decay_up_weight,
    decay_offset, decay_log_extra, erasure_down_weight, erasure_up_weight, erasure_offset,
    initial_state, head_norm_gain, query_sink_logit, linear_output_weight, window_output_weight,
):
    tokens, model = inputs.shape[1], 2 * inputs.shape[2]
    places = lax.axis_size(SP)
    nz, nx = lax.axis_size("sp_0"), lax.axis_size("sp_1")
    rows = receptance_weight.shape[0]
    out_rows = linear_output_weight.shape[1]
    columns = places * out_rows
    vmem = pl.BlockSpec(memory_space=pltpu.VMEM)
    hbm = pl.BlockSpec(memory_space=pl.ANY)
    smem = pl.BlockSpec(memory_space=pltpu.SMEM)
    dma = pltpu.SemaphoreType.DMA
    down_d, down_e = decay_down_weight.T, erasure_down_weight.T

    def space(kind, *shape):
        return pltpu.VMEM(shape, kind)

    out = pl.pallas_call(
        layer_kernel,
        out_shape=jax.ShapeDtypeStruct((tokens // 2, FOUR * columns), BF),
        in_specs=[hbm, vmem, hbm, hbm, hbm, hbm, vmem, vmem, hbm, hbm, hbm, hbm, vmem, vmem, hbm, hbm, vmem, smem, vmem, vmem],
        out_specs=vmem,
        scratch_shapes=[
            space(BF, 2, tokens, model // 2),
            space(BF, FOUR, tokens, model),
            space(BF, FOUR, rows, 5 * PAIR),
            space(BF, places, FOUR * rows, 5 * PAIR),
            space(F32, FOUR, *decay_log_extra.shape[1:]),
            space(BF, *down_d.shape),
            space(BF, *down_e.shape),
            space(BF, *decay_up_weight.shape),
            space(BF, *erasure_up_weight.shape),
            space(F32, *initial_state.shape),
            space(BF, FOUR, tokens, 5 * PAIR),
            space(F32, 2, FOUR, tokens, PAIR),
            space(F32, 2, FOUR, tokens, PAIR),
            space(F32, tokens + 2 * WINDOW, PAIR),
            space(F32, tokens + 2 * WINDOW, PAIR),
            space(BF, out_rows, 2 * FOUR * PAIR),
            space(F32, 2, FOUR, tokens, PAIR),
            space(F32, FOUR, tokens, PAIR),
            space(BF, places, 48, PAIR),
            space(BF, 2, nz, nx, out_rows, 2 * FOUR * PAIR),
            space(BF, places, 48, PAIR),
            space(BF, places, 16, PAIR),
            space(BF, places, 16, PAIR),
            space(BF, 2, FOUR, tokens, PAIR),
            space(F32, 4, places // 4, 3 * HD // 2, HD),
            space(F32, FOUR * tokens // 2, columns),
            space(BF, 2, FOUR, FOUR, tokens // 2, PAIR),
            space(BF, 2, FOUR, FOUR, tokens // 2, PAIR),
            space(BF, FOUR, tokens // 2, PAIR),
            space(BF, FOUR, tokens // 2, PAIR),
            space(BF, FOUR, tokens // 2, columns),
            space(BF, FOUR, tokens // 2, columns),
            dma((3,)), dma((5,)),
            dma, dma, dma((1,)), dma((4,)), dma, dma, dma, dma,
            dma, dma((2, nz // 2)), dma((nz,)), dma, dma, dma, dma, dma((2, nz // 2)),
            dma, dma, dma, dma((3,)), dma, dma,
            dma, dma, dma, dma, dma, dma,
            *[dma((1,)), dma((4,))] * 4, dma((FOUR,)), dma, dma,
        ],
        compiler_params=pltpu.CompilerParams(
            collective_id=0, has_side_effects=True, vmem_limit_bytes=63 * 2**20
        ),
        name="layer",
    )(
        inputs[0], input_norm_gain[None], receptance_weight, linear_key_weight, linear_value_weight,
        window_query_weight, window_key_weight, window_value_weight, down_d, down_e,
        decay_up_weight, erasure_up_weight, decay_offset, erasure_offset, decay_log_extra,
        initial_state, head_norm_gain[None], query_sink_logit, linear_output_weight.T,
        window_output_weight.T,
    )
    return out[None]


def solution(mesh):
    finer = Mesh(
        mesh.devices.reshape(8, 4, mesh.shape["fs"], mesh.shape["tp"]), ("sp_0", "sp_1", "fs", "tp")
    )
    placed = (
        P("fs", SP, "tp"),
        P(),
        P(SP_FS, "tp"),
        P(SP_FS, "tp"),
        P(SP_FS, "tp"),
        P(SP_FS, "tp"),
        P(SP_FS, "tp"),
        P(SP_FS, "tp"),
        P(),
        P(),
        P(),
        P("fs", "tp", SP),
        P(),
        P(),
        P(),
        P(),
        P(),
        P(),
        P("tp", SP_FS),
        P("tp", SP_FS),
    )
    return jax.shard_map(
        local, mesh=finer, in_specs=placed, out_specs=P("fs", SP_TP, None), check_vma=False
    )
```

```python
import math
import functools
import jax
import jax.numpy as jnp
from jax import lax
from jax.experimental import pallas as pl
from jax.experimental.pallas import tpu as pltpu

from jax.sharding import Mesh
from jax.sharding import PartitionSpec as P

HD = 64
CH = 64
PAIR = 128
WINDOW = 128
GRID_W = 64
ATT_BLOCK = 128
SP = ("sp_0", "sp_1")
FOUR = 4
ROUND = 2
SP_FS = ("sp_0", "sp_1", "fs")
SP_TP = ("sp_0", "sp_1", "tp")
NORM_EPS = 1e-06
GROUP_EPS = 0.00064
ROPE_BASE = 10000.0
F32 = jnp.float32
BF = jnp.bfloat16
MESSAGE = jnp.bfloat16
MESH = pl.DeviceIdType.MESH
NN = (((1,), (0,)), ((), ()))
NT = (((1,), (1,)), ((), ()))
TN = (((0,), (0,)), ((), ()))


def dot(a, b, dims=NN):
    return lax.dot_general(a, b, dims, preferred_element_type=F32)


def split2(a):
    high = a.astype(BF)
    return high, (a - high.astype(F32)).astype(BF)


def split3(a):
    high, rest = a.astype(BF), None
    rest = a - high.astype(F32)
    mid = rest.astype(BF)
    return high, mid, (rest - mid.astype(F32)).astype(BF)


def mm3(a, b, dims=NN):
    (ka,), (kb,) = dims[0]
    a_hi, a_lo = split2(a)
    b_hi, b_lo = split2(b)
    free = 1 - kb
    if b.shape[free] == PAIR:
        upper = jnp.concatenate([b_hi, b_lo], axis=free)
        lower = jnp.concatenate([b_hi, jnp.zeros_like(b_lo)], axis=free)
        wide = dot(
            jnp.concatenate([a_hi, a_lo], axis=ka), jnp.concatenate([upper, lower], axis=kb), dims
        )
        return wide[:, :PAIR] + wide[:, PAIR:]
    main = dot(
        jnp.concatenate([a_hi, a_lo], axis=ka), jnp.concatenate([b_hi, b_hi], axis=kb), dims
    )
    return main + dot(a_hi, b_lo, dims)


def mm2(a, b_exact, dims=NN):
    (ka,), (kb,) = dims[0]
    a_hi, a_lo = split2(a)
    return dot(
        jnp.concatenate([a_hi, a_lo], axis=ka), jnp.concatenate([b_exact, b_exact], axis=kb), dims
    )


def iota(shape, dim):
    return lax.broadcasted_iota(jnp.int32, shape, dim)


def ones_where(cond):
    return jnp.where(cond, 1.0, 0.0).astype(BF)


def settle(where, sem):
    pltpu.make_async_copy(where, where, sem).wait()


def ring_of_four(buf, out_sem, in_sem, give_ref=None, core=None):
    me = lax.axis_index("fs")
    right, left, far = (me + 1) % FOUR, (me + 3) % FOUR, (me + 2) % FOUR
    half = buf.shape[1] // 2
    near_buf = buf if give_ref is None else give_ref[1]

    def piece(block, part, target, number):
        where = buf.at[block, part * half : (part + 1) * half]
        return pltpu.make_async_remote_copy(
            src_ref=where, dst_ref=where, send_sem=out_sem.at[0], recv_sem=in_sem.at[number],
            device_id={"fs": target}, device_id_type=MESH,
        )

    def launch(part, target, number):
        if give_ref is None:
            piece(me, part, target, number).start()
            return
        rows = slice(part * half, (part + 1) * half)
        pltpu.make_async_remote_copy(
            src_ref=give_ref[0].at[rows], dst_ref=near_buf.at[me, rows],
            send_sem=out_sem.at[0], recv_sem=in_sem.at[number],
            device_id={"fs": target, "tp": core}, device_id_type=MESH,
        ).start()

    def start():
        launch(0, right, 0)
        launch(1, left, 1)
        launch(1, right, 2)
        launch(0, left, 2)

    def relay():
        piece(left, 0, right, 0).wait_recv()
        piece(left, 0, right, 3).start()
        piece(right, 1, left, 1).wait_recv()
        piece(right, 1, left, 3).start()

    def arrive_near():
        settle(buf.at[0], in_sem.at[2])

    def arrive_far():
        settle(buf.at[0], in_sem.at[3])

    def finish_sends():
        settle(buf.at[0:3], out_sem.at[0])

    return start, relay, arrive_near, arrive_far, finish_sends


def peer_id(index):
    inner = lax.axis_size("sp_1")
    return {"sp_0": index // inner, "sp_1": index % inner}


def neighbours(place_of):
    z, x, f, c = place_of
    nz, nx = lax.axis_size("sp_0"), lax.axis_size("sp_1")
    peers = [{"fs": (f + k) % FOUR} for k in range(1, FOUR)] + [{"tp": 1 - c}]
    peers += [{"sp_0": (z + k) % nz} for k in (1, nz - 1)]
    return peers + [{"sp_1": (x + k) % nx} for k in range(1, nx)]


def rope_tables(place, cos_ref, sin_ref):
    reach = cos_ref.shape[0]
    block = reach // 3
    spot = iota((reach, PAIR), 0)
    lane = iota((reach, PAIR), 1)
    grid_row = ((place - 1) * (block // GRID_W) + spot // GRID_W).astype(F32)
    grid_col = (spot % GRID_W).astype(F32)
    power = (lane % 16).astype(F32) * (1.0 / 16)
    angle = jnp.where(lane % HD < HD // 2, grid_row, grid_col) * jnp.exp(power * -math.log(ROPE_BASE))
    cos_ref[...] = jnp.cos(angle)
    sin_ref[...] = jnp.sin(angle)


def share(ref, give_ref, ring_sems, give_sems, place_of):
    f, c = place_of[2:]
    own = ring_of_four(ref.at[c], *ring_sems[0])
    other = ring_of_four(ref.at[1 - c], *ring_sems[1], (give_ref, ref.at[c]), 1 - c)

    def give(core):
        return pltpu.make_async_remote_copy(
            src_ref=give_ref, dst_ref=ref.at[core, f], send_sem=give_sems[0], recv_sem=give_sems[1],
            device_id={"tp": 1 - c}, device_id_type=MESH,
        )

    def start():
        own[0]()
        other[0]()
        give(c).start()

    def collect():
        own[1]()
        other[1]()
        give(1 - c).wait_recv()
        for ring in (own, other):
            ring[2]()
            ring[3]()

    def drain():
        give(c).wait_send()
        own[4]()
        other[4]()

    return start, collect, drain


def front(refs, place_of):
    (
        x_ref, gain_ref, wr_ref, wk_ref, wv_ref, wq_ref, wak_ref, wav_ref, down_d_ref, down_e_ref,
        up_d_ref, up_e_ref, off_d_ref, off_e_ref, extra_ref, proj_ref, logd_ref, learn_ref,
        both_ref, hid_ref, stage_ref, cols_ref, ext_ref, load_sem,
        x_out, x_in, hid_out, hid_in, stage_out, stage_in, ext_out, ext_in,
        ring_out, z_in, near_in, far_in, rest_x_out, rest_x_in, rest_z_out, rest_z_in, cos_ref, sin_ref, late, early,
    ) = refs
    z, x, f, c = place_of
    nz, nx = lax.axis_size("sp_0"), lax.axis_size("sp_1")
    mine = z * nx + x
    rows = wr_ref.shape[0]
    loads = []
    for g in range(FOUR):
        for k, ref in enumerate((wr_ref, wk_ref, wv_ref, wq_ref)):
            loads.append((ref.at[:, g * PAIR : (g + 1) * PAIR], stage_ref.at[g, :, k * PAIR : (k + 1) * PAIR], 0))
    loads.append((x_ref, both_ref.at[c], 1))
    loads.append((extra_ref.at[0], ext_ref.at[f], 2))
    loads = [pltpu.make_async_copy(start, end, load_sem.at[number]) for start, end, number in loads]
    for load in early + loads + late:
        load.start()
    for load in early:
        load.wait()
    low = iota((rows, PAIR), 1) < HD
    keys, values = wak_ref[...].astype(F32), wav_ref[...].astype(F32)
    shared = [
        jnp.where(low, keys, pltpu.roll(values, HD, 1)).astype(BF),
        jnp.where(low, pltpu.roll(keys, HD, 1), values).astype(BF),
    ]
    for g in range(FOUR):
        stage_ref[g, :, 4 * PAIR :] = shared[g // 2]
    with jax.named_scope("f_load"):
        settle(stage_ref.at[:, :, : 4 * PAIR], load_sem.at[0])
        for load in loads[-2:]:
            load.wait()
    my_rows = pl.ds(pl.multiple_of(f * rows, rows), rows)
    cols_ref[mine, my_rows, :] = stage_ref[f]
    with jax.named_scope("f_meet"):
        pl.semaphore_wait(pltpu.get_barrier_semaphore(), len(neighbours(place_of)))

    half_copy = pltpu.make_async_remote_copy(
        src_ref=both_ref.at[c], dst_ref=both_ref.at[c], send_sem=x_out, recv_sem=x_in,
        device_id={"tp": 1 - c}, device_id_type=MESH,
    )
    half_copy.start()

    def stage_copy(k):
        g = (f + k) % FOUR
        return pltpu.make_async_remote_copy(
            src_ref=stage_ref.at[g], dst_ref=cols_ref.at[mine, my_rows, :],
            send_sem=stage_out, recv_sem=stage_in, device_id={"fs": g}, device_id_type=MESH,
        )

    def ext_copy(k, source):
        return pltpu.make_async_remote_copy(
            src_ref=ext_ref.at[source], dst_ref=ext_ref.at[source],
            send_sem=ext_out, recv_sem=ext_in, device_id={"fs": (f + k) % FOUR}, device_id_type=MESH,
        )

    for k in range(1, FOUR):
        stage_copy(k).start()

    def z_block(k):
        if k == 0:
            return z
        step = (k - 1) // 2
        return (z + nz - 1 - step) % nz if k % 2 else (z + 1 + step) % nz

    main = 3 * PAIR

    def rest_x_copy(k):
        where = cols_ref.at[mine, :, main:]
        return pltpu.make_async_remote_copy(
            src_ref=where, dst_ref=where, send_sem=rest_x_out, recv_sem=rest_x_in,
            device_id={"sp_1": (x + k) % nx}, device_id_type=MESH,
        )

    def rest_z_copy(block, side, step):
        where = cols_ref.at[pl.ds(block * nx, nx), :, main:]
        return pltpu.make_async_remote_copy(
            src_ref=where, dst_ref=where, send_sem=rest_z_out, recv_sem=rest_z_in.at[side, step],
            device_id={"sp_0": (z + (1 if side == 0 else nz - 1)) % nz}, device_id_type=MESH,
        )

    def rest_begin():
        settle(cols_ref.at[0 : nx - 1, :, main:], rest_x_in)
        rest_z_copy(z, 0, 0).start()
        rest_z_copy(z, 1, 0).start()

    def rest_pass(step):
        for side, last in ((0, nz // 2 - 1), (1, nz // 2 - 2)):
            if step <= last:
                block = z_block(2 * step + 1 + side)
                rest_z_copy(block, side, step).wait_recv()
                if step < last:
                    rest_z_copy(block, side, step + 1).start()

    def z_copy(k_from, side, step):
        where = cols_ref.at[z_block(k_from) * nx + x, :, :main]
        return pltpu.make_async_remote_copy(
            src_ref=where, dst_ref=where, send_sem=ring_out, recv_sem=z_in.at[side, step],
            device_id={"sp_0": (z + (1 if side == 0 else nz - 1)) % nz}, device_id_type=MESH,
        )

    def near_copy(k, side, column):
        where = cols_ref.at[z_block(k) * nx + column, :, :main]
        return pltpu.make_async_remote_copy(
            src_ref=where, dst_ref=where, send_sem=ring_out, recv_sem=near_in.at[k],
            device_id={"sp_1": (x + (1 if side == 0 else nx - 1)) % nx}, device_id_type=MESH,
        )

    def far_copy(k, column):
        where = cols_ref.at[z_block(k) * nx + column, :, :main]
        return pltpu.make_async_remote_copy(
            src_ref=where, dst_ref=where, send_sem=ring_out, recv_sem=far_in,
            device_id={"sp_1": (x + (1 if k % 2 == 0 else nx - 1)) % nx}, device_id_type=MESH,
        )

    left, right, _ = (x + nx - 1) % nx, (x + 1) % nx, 0

    def spread(k):
        near_copy(k, 0, x).start()
        near_copy(k, 1, x).start()

    def pass_on(k):
        settle(cols_ref.at[0:2, :, :main], near_in.at[k])
        far_copy(k, left if k % 2 == 0 else right).start()

    with jax.named_scope("f_stage_wait"):
        settle(stage_ref.at[1:FOUR], stage_in)
    z_copy(0, 0, 0).start()
    z_copy(0, 1, 0).start()
    spread(0)
    for k in range(1, nx):
        rest_x_copy(k).start()

    with jax.named_scope("f_norm"):
        half_copy.wait_recv()
        full = jnp.concatenate([both_ref[0], both_ref[1]], axis=1).astype(F32)
        scale = lax.rsqrt(jnp.mean(full * full, axis=-1, keepdims=True) + NORM_EPS)
        hid_ref[f] = (full * scale * gain_ref[...]).astype(BF)
    start, relay, arrive_near, arrive_far, finish_sends = ring_of_four(hid_ref, hid_out, hid_in)
    for k in range(1, FOUR):
        ext_copy(k, f).start()
    start()
    with jax.named_scope("f_rope"):
        rope_tables(mine, cos_ref, sin_ref)

    steps = nz // 2
    with jax.named_scope("f_ring"):
        for step in range(steps):
            k = 2 * step + 1
            z_copy(k, 0, step).wait_recv()
            if step < steps - 1:
                z_copy(k, 0, step + 1).start()
            spread(k)
            if step < steps - 1:
                z_copy(k + 1, 1, step).wait_recv()
                if step < steps - 2:
                    z_copy(k + 1, 1, step + 1).start()
                spread(k + 1)
            if step == 0:
                pass_on(0)
            else:
                pass_on(k - 2)
                pass_on(k - 1)
            if step == 0:
                rest_begin()
            elif step > 1:
                rest_pass(step - 2)
            if step == 1:
                relay()
    with jax.named_scope("f_pass_last"):
        pass_on(nz - 1)
    with jax.named_scope("f_hid_wait"):
        arrive_near()
        arrive_far()
        settle(ext_ref.at[1:FOUR], ext_in)

    for load in late:
        load.wait()
    tokens = hid_ref.shape[1]
    hidden = hid_ref[...].reshape(FOUR * tokens, hid_ref.shape[2])
    with jax.named_scope("f_rates"):
        decay_low = dot(hidden, down_d_ref[...], NT).astype(BF)
        learn_low = dot(hidden, down_e_ref[...], NT).astype(BF)
        decay_act = jnp.tanh(decay_low.astype(F32)).astype(BF)
        heads = ext_ref.shape[1]
        first = c * heads * HD + f * PAIR
        chosen = pl.ds(pl.multiple_of(first, PAIR), PAIR)
        select = ones_where(iota((heads, PAIR), 0) == 2 * f + iota((heads, PAIR), 1) // HD).astype(F32)
        spikes = [
            lax.dot_general(
                ext_ref[p], select, TN, precision=lax.Precision.HIGHEST, preferred_element_type=F32
            )
            for p in range(FOUR)
        ]
        for d in range(2):
            pre = off_d_ref[d : d + 1, chosen] + dot(decay_act, up_d_ref[d, :, chosen])
            softplus = jnp.maximum(-pre, 0.0) + jnp.log1p(jnp.exp(-jnp.abs(pre)))
            rate = jnp.exp(-softplus - 0.5)
            learn = jax.nn.sigmoid(off_e_ref[d : d + 1, chosen] + dot(learn_low, up_e_ref[d, :, chosen]))
            for p in range(FOUR):
                part = slice(p * tokens, (p + 1) * tokens)
                logd_ref[d, p] = spikes[p] - rate[part]
                learn_ref[d, p] = learn[part]

    with jax.named_scope("f_far_wait"):
        settle(cols_ref.at[0:nz, :, :main], far_in)
    depth = cols_ref.shape[0] * cols_ref.shape[1]
    with jax.named_scope("f_proj"):
        for first_col, last_col in ((0, 256), (256, 384)):
            weight = cols_ref[:, :, first_col:last_col].reshape(depth, last_col - first_col)
            result = dot(hidden, weight).astype(BF)
            for p in range(FOUR):
                proj_ref[p, :, first_col:last_col] = result[p * tokens : (p + 1) * tokens]

    rest_pass(nz // 2 - 2)
    half_copy.wait_send()
    finish_sends()
    settle(stage_ref.at[1:FOUR], stage_out)
    settle(ext_ref.at[1:FOUR], ext_out)
    settle(cols_ref.at[0 : 4 * nz - 1, :, :main], ring_out)

    def project_rest():
        rest_pass(nz // 2 - 1)
        weight = cols_ref[:, :, main:].reshape(depth, cols_ref.shape[2] - main)
        result = dot(hid_ref[...].reshape(FOUR * tokens, hid_ref.shape[2]), weight).astype(BF)
        for p in range(FOUR):
            proj_ref[p, :, main:] = result[p * tokens : (p + 1) * tokens]
        settle(cols_ref.at[0 : nx - 1, :, main:], rest_x_out)
        settle(cols_ref.at[0 : nx * (nz - 1), :, main:], rest_z_out)

    return project_rest


def stacked(x):
    low = iota(x.shape, 1) < HD
    return jnp.concatenate([jnp.where(low, x, 0.0), jnp.where(low, 0.0, x)], axis=0)


def unstacked(x):
    return x[:CH] + x[CH:]


def gather_rows(refs, place_of):
    wout_ref, rows_ref, z_out, z_in, x_out, x_in, c_out, c_in = refs
    z, x, _, c = place_of
    nz, nx = lax.axis_size("sp_0"), lax.axis_size("sp_1")
    half = nz // 2
    left, right, across = (x + nx - 1) % nx, (x + 1) % nx, (x + 2) % nx

    def z_copy(k, source):
        return pltpu.make_async_remote_copy(
            src_ref=wout_ref, dst_ref=rows_ref.at[c, source, x], send_sem=z_out, recv_sem=z_in,
            device_id={"sp_0": (z + k) % nz}, device_id_type=MESH,
        )

    def x_copy(number, column):
        part = slice(0, nz) if number < 2 else slice(0, half) if number == 2 else slice(half, nz)
        where = rows_ref.at[c, part, column]
        return pltpu.make_async_remote_copy(
            src_ref=where, dst_ref=where, send_sem=x_out, recv_sem=x_in.at[min(number, 2)],
            device_id={"sp_1": right if number % 2 == 0 else left}, device_id_type=MESH,
        )

    def c_copy(number, core, column):
        where = rows_ref.at[core, :, column]
        return pltpu.make_async_remote_copy(
            src_ref=where, dst_ref=where, send_sem=c_out, recv_sem=c_in,
            device_id={"tp": 1 - c}, device_id_type=MESH,
        )

    def first():
        rows_ref[c, z, x] = wout_ref[...]
        for k in range(1, nz):
            z_copy(k, z).start()

    def second():
        settle(rows_ref.at[c, 1:nz, x], z_in)
        x_copy(0, x).start()
        x_copy(1, x).start()
        c_copy(0, c, x).start()

    def third():
        x_copy(0, left).wait_recv()
        x_copy(2, left).start()
        x_copy(1, right).wait_recv()
        x_copy(3, right).start()
        c_copy(1, c, left).start()
        c_copy(2, c, right).start()

    def fourth():
        settle(rows_ref.at[c, :, across], x_in.at[2])
        c_copy(3, c, across).start()

    def last():
        settle(rows_ref.at[1 - c], c_in)
        settle(rows_ref.at[c], c_out)
        settle(rows_ref.at[c, 1:nz, x], z_out)
        settle(rows_ref.at[c, :, 1:nx], x_out)

    return first, second, third, fourth, last


def local_maps(refs, project_rest, send_halo, send_maps, rows_steps):
    proj_ref, logd_ref, learn_ref, q_ref, o_ref, msg_ref = refs
    rows_steps[0]()
    row = iota((2 * CH, 2 * CH), 0)
    col = iota((2 * CH, 2 * CH), 1)
    t, s = row % CH, col % CH
    eye = row == col
    same_head = ones_where(row // HD == col // HD)
    tri = [ones_where((iota((CH, CH), 0) >= iota((CH, CH), 1))), ones_where((iota((CH, CH), 0) <= iota((CH, CH), 1)))]
    strict = [t > s, t < s]
    within = [t >= s, t <= s]

    def one_round(it, carry):
        @pl.when(it == 1)
        def _():
            project_rest()
            for u in range(ROUND):
                send_maps(u)
            send_halo()

        seqs = [it * ROUND + u for u in range(ROUND)]
        recept, keys, values, unit = {}, {}, {}, {}
        for u, p in enumerate(seqs):
            recept[u] = proj_ref[p, :, :PAIR].astype(F32)
            keys[u] = proj_ref[p, :, PAIR : 2 * PAIR].astype(F32)
            values[u] = proj_ref[p, :, 2 * PAIR : 3 * PAIR].astype(F32)
            unit[u] = keys[u] * lax.rsqrt(mm2(keys[u] * keys[u], same_head) + NORM_EPS)
        jobs = [(u, d, c) for u in range(ROUND) for d in range(2) for c in range(2)]
        stage = {}
        for u, d, c in jobs:
            rows = slice(c * CH, (c + 1) * CH)
            logd = logd_ref[d, seqs[u], rows, :]
            parts = jnp.concatenate(split3(logd), axis=0)
            total = dot(jnp.concatenate([tri[d]] * 3, axis=1), parts)
            middle = total[CH // 2 - 1 : CH // 2] if d == 0 else total[CH // 2 : CH // 2 + 1]
            last = total[CH - 1 : CH] if d == 0 else total[0:1]
            grow = jnp.exp(total - middle)
            shrink = jnp.exp(middle - total)
            read = recept[u][rows] * grow
            mark = unit[u][rows] * jnp.exp(total - logd - middle)
            erase = unit[u][rows] * learn_ref[d, seqs[u], rows, :] * shrink
            key = keys[u][rows] * shrink
            read_s, mark_s, erase_s, key_s = map(stacked, (read, mark, erase, key))
            scores = mm3(
                jnp.concatenate([mark_s, read_s], axis=0),
                jnp.concatenate([erase_s, key_s], axis=0),
                NT,
            )
            stage[u, d, c] = (read, mark_s, erase_s, key_s, scores, jnp.exp(middle), jnp.exp(last - middle), jnp.exp(last))
        inverse = {}
        grams = {}
        for u, d, c in jobs:
            gram = jnp.where(strict[d], stage[u, d, c][4][: 2 * CH, : 2 * CH], 0.0)
            grams[u, d, c] = gram
            inverse[u, d, c] = jnp.where(eye, 1.0, 0.0) - jnp.where(t // 2 == s // 2, gram, 0.0)
        block = 2
        while block < CH:
            joins = (t // (2 * block) == s // (2 * block)) & (t // block != s // block)
            for job in jobs:
                found = inverse[job]
                inverse[job] = found - mm3(found, mm3(jnp.where(joins, grams[job], 0.0), found))
            block *= 2
        maps, reads, outs = {}, {}, {}
        for u, d, c in jobs:
            rows = slice(c * CH, (c + 1) * CH)
            read, mark_s, erase_s, key_s, scores, to_start, to_end, whole = stage[u, d, c]
            val_s = stacked(values[u][rows]).astype(BF)
            cross = jnp.where(strict[d], scores[: 2 * CH, 2 * CH :], 0.0)
            read_e = jnp.where(within[d], scores[2 * CH :, : 2 * CH], 0.0)
            read_k = jnp.where(within[d], scores[2 * CH :, 2 * CH :], 0.0)
            solved = mm3(inverse[u, d, c], jnp.concatenate([mark_s, mm2(cross, val_s)], axis=1))
            solved = jnp.concatenate([solved[:, :PAIR] * to_start, solved[:, PAIR:]], axis=1)
            taken = mm3(read_e, solved)
            reads[u, d, c] = read * to_start - unstacked(taken[:, :PAIR])
            outs[u, d, c] = unstacked(mm2(read_k, val_s) - taken[:, PAIR:])
            ended = mm3(solved, erase_s * to_end, TN)
            k_hi, k_lo = split2(key_s * to_end)
            added = dot(jnp.concatenate([val_s, val_s], axis=0), jnp.concatenate([k_hi, k_lo], axis=0), TN)
            prod = jnp.where(eye, whole - 1.0, 0.0) - ended[:PAIR]
            maps[u, d, c] = (prod, added - ended[PAIR:])
        for u, p in enumerate(seqs):
            out_rows = [outs[u, 0, 0] + outs[u, 1, 0], outs[u, 0, 1] + outs[u, 1, 1]]
            for d in range(2):
                first, second = (0, 1) if d == 0 else (1, 0)
                (prod1, add1), (prod2, add2) = maps[u, d, first], maps[u, d, second]
                both = jnp.concatenate([prod1, add1], axis=0)
                through = mm3(reads[u, d, second], both, NT)
                q_ref[d, p, first * CH : (first + 1) * CH, :] = reads[u, d, first]
                q_ref[d, p, second * CH : (second + 1) * CH, :] = reads[u, d, second] + through[:, :PAIR]
                out_rows[second] = out_rows[second] + through[:, PAIR:]
                joined = mm3(both, prod2)
                prod = prod1 + prod2 + joined[:PAIR]
                add = add1 + joined[PAIR:] + add2
                for hh in range(2):
                    for half in range(2):
                        message = jnp.concatenate(
                            [
                                folded(prod, hh, hh * HD, HD // 2),
                                folded(add, hh, hh * HD + half * (HD // 2), HD // 4),
                            ],
                            axis=0,
                        )
                        msg_ref[d * 16 + p * 4 + hh * 2 + half] = message.astype(msg_ref.dtype)
            for c in range(2):
                o_ref[p, c * CH : (c + 1) * CH, :] = out_rows[c]

        return carry

    with jax.named_scope("l_loop"):
        lax.fori_loop(0, FOUR // ROUND, one_round, 0)
    for u in range(ROUND):
        send_maps(FOUR - ROUND + u)
    rows_steps[1]()


def folded(x, hh, first, count):
    upper, lower = x[first : first + count], x[first + count : first + 2 * count]
    if hh == 0:
        return upper + pltpu.roll(lower, HD, 1)
    return pltpu.roll(upper, HD, 1) + lower


def exchange(refs, place_of):
    (
        msg_ref, init_ref, reads_ref, local_ref, gain_ref, proj_ref, cos_ref, sin_ref, sink_ref, lin_ref, att_ref, lin_give, att_give,
        recv_ref, sent_ref, enter_ref, halo_ref, comp_ref,
        out_sem, in_sem, back_out_sem, back_in_sem, halo_out_sem, halo_in_sem,
    ) = refs
    count = recv_ref.shape[0]
    place = place_of[0] * lax.axis_size("sp_1") + place_of[1]
    kv_first = 4 * PAIR

    def halo_copy(side):
        target = (place + count - 1 + 2 * side) % count
        return pltpu.make_async_remote_copy(
            src_ref=proj_ref.at[:, :, kv_first : kv_first + PAIR],
            dst_ref=halo_ref.at[1 - side],
            send_sem=halo_out_sem,
            recv_sem=halo_in_sem,
            device_id=peer_id(target),
            device_id_type=MESH,
        )

    def map_copy(target):
        return pltpu.make_async_remote_copy(
            src_ref=msg_ref.at[target],
            dst_ref=recv_ref.at[place],
            send_sem=out_sem,
            recv_sem=in_sem,
            device_id=peer_id(target),
            device_id_type=MESH,
        )

    def entry_copy(target):
        return pltpu.make_async_remote_copy(
            src_ref=sent_ref.at[target],
            dst_ref=enter_ref.at[place],
            send_sem=back_out_sem,
            recv_sem=back_in_sem,
            device_id=peer_id(target),
            device_id_type=MESH,
        )

    def send_halo():
        halo_copy(0).start()
        halo_copy(1).start()

    def send_maps(p):
        for d in range(2):
            for q in range(4):
                target = d * 16 + p * 4 + q

                @pl.when(target != place)
                def _():
                    map_copy(target).start()

    def run(after_attend, after_chain):
        tokens = local_ref.shape[1]
        with jax.named_scope("x_halo"):
            settle(halo_ref, halo_in_sem)
            settle(halo_ref, halo_out_sem)
        lane = iota((1, PAIR), 1)
        low = lane < HD
        front = lane % 32 < 16

        def turned(v, first, last):
            other = jnp.where(front, -pltpu.roll(v, PAIR - 16, 1), pltpu.roll(v, 16, 1))
            return v * cos_ref[first:last, :] + other * sin_ref[first:last, :]

        reach = 3 * tokens
        q_pos = place * tokens + iota((2 * tokens, reach), 0) % tokens
        k_pos = (place - 1) * tokens + iota((2 * tokens, reach), 1)
        allowed = (jnp.abs(q_pos - k_pos) <= WINDOW) & (k_pos >= 0) & (k_pos < count * tokens)
        upper = iota((2 * tokens, 1), 0) < tokens
        pair = lax.axis_index("fs")
        first_head = lax.axis_index("tp") * (2 * FOUR) + 2 * pair
        sink = jnp.where(upper, sink_ref[first_head], sink_ref[first_head + 1])

        def attend(p, carry):
            kv = jnp.concatenate(
                [halo_ref[0, p], proj_ref[p, :, kv_first : kv_first + PAIR], halo_ref[1, p]], axis=0
            ).astype(F32)
            roped = turned(kv, 0, reach)
            swapped = pltpu.roll(kv, HD, 1)
            key = jnp.where(low, roped, pltpu.roll(roped, HD, 1)).astype(BF)
            value = jnp.where(low, swapped, kv).astype(BF)
            query = turned(proj_ref[p, :, kv_first - PAIR : kv_first].astype(F32), tokens, 2 * tokens)
            query = jnp.concatenate([jnp.where(low, query, 0.0), jnp.where(low, 0.0, query)], axis=0)
            scores = dot(query.astype(BF), key, NT) * HD**-0.5
            scores = jnp.where(allowed, scores, -jnp.inf)
            top = jnp.maximum(jnp.max(scores, axis=-1, keepdims=True), sink)
            raised = jnp.exp(scores - top)
            total = jnp.exp(sink - top) + jnp.sum(raised, axis=-1, keepdims=True)
            mixed = dot((raised / total).astype(BF), value)
            keep(jnp.where(low, mixed[:tokens], mixed[tokens:]).astype(BF), place_of, p, att_ref, att_give)
            return carry

        with jax.named_scope("x_attend"):
            lax.fori_loop(0, FOUR, attend, 0)

        after_attend()
        recv_ref[place] = msg_ref[place]

        with jax.named_scope("x_await_map"):
            settle(recv_ref.at[1:count], in_sem)
            settle(msg_ref.at[1:count], out_sem)

        unit_idx = place // 2
        direction, half = unit_idx // 8, place % 2
        rows = HD // 2
        quarter = rows // 2
        start = pl.multiple_of(half * rows, rows)
        groups = 4
        length = count // groups

        def nth(step):
            return direction * (count - 1) + step * (1 - 2 * direction)

        def message(step):
            m = recv_ref[nth(step)].astype(F32)
            return jnp.concatenate([m[:rows, :HD], m[:rows, HD:], m[rows:, :HD], m[rows:, HD:]], axis=0)

        def extend(s, maps):
            longer = []
            for g in range(groups):
                step = message(g * length + s)
                comp_ref[g, s] = maps[g]
                longer.append(maps[g] + mm2(maps[g], step[:HD].astype(BF)) + step)
            return tuple(longer)

        nothing = jnp.zeros((3 * rows, HD), F32)
        with jax.named_scope("x_compose"):
            maps = lax.fori_loop(0, length, extend, (nothing,) * groups)
        state = init_ref[direction, first_head + unit_idx % 2, pl.ds(start, rows), :]

        def dispatch(g):
            def one(s, carry):
                target = nth(g * length + s)

                @pl.when(target != place)
                def _():
                    entry_copy(target).start()

                return carry

            lax.fori_loop(0, length, one, 0)

        with jax.named_scope("x_chain"):
            for g in range(groups):
                for s in range(length):
                    before = comp_ref[g, s]
                    entry = state + mm3(state, before[:HD]) + before[HD:] if s else state
                    sent_ref[nth(g * length + s)] = jnp.concatenate(
                        [entry[:quarter], entry[quarter:]], axis=1
                    ).astype(BF)
                state = state + mm3(state, maps[g][:HD]) + maps[g][HD:]
                if g:
                    dispatch(g - 1)
        enter_ref[place] = sent_ref[place]
        dispatch(groups - 1)
        after_chain()

        with jax.named_scope("x_await_entry"):
            settle(enter_ref.at[1:count], back_in_sem)
            settle(sent_ref.at[1:count], back_out_sem)
        with jax.named_scope("x_finish"):
            finish(reads_ref, local_ref, enter_ref, gain_ref, lin_ref, lin_give, place_of)

    return send_halo, send_maps, run


def keep(value, place_of, p, mine_ref, give_ref):
    f, c = place_of[2:]
    half = value.shape[0] // 2
    mine_ref[c, f, p] = jnp.where(c == 0, value[:half], value[half:])
    give_ref[p] = jnp.where(c == 0, value[half:], value[:half])


def finish(q_ref, o_ref, enter_ref, gain_ref, lin_ref, lin_give, place_of):
    row = iota((PAIR, PAIR), 0)
    col = iota((PAIR, PAIR), 1)
    same_head = ones_where(row // HD == col // HD)
    low = iota((HD // 4, PAIR), 1) < HD
    start = (lax.axis_index("tp") * FOUR + lax.axis_index("fs")) * PAIR
    gain = gain_ref[:, pl.ds(pl.multiple_of(start, PAIR), PAIR)]
    for p in range(FOUR):
        out = o_ref[p]
        for d in range(2):
            pieces = []
            for hh in range(2):
                for half in range(2):
                    m = enter_ref[d * 16 + p * 4 + hh * 2 + half].astype(F32)
                    turned = pltpu.roll(m, HD, 1)
                    if hh == 0:
                        pieces += [jnp.where(low, m, 0.0), jnp.where(low, turned, 0.0)]
                    else:
                        pieces += [jnp.where(low, 0.0, turned), jnp.where(low, 0.0, m)]
            out = out + mm2(q_ref[d, p], jnp.concatenate(pieces, axis=0).astype(BF), NT)
        centred = out - mm2(out, same_head) * (1.0 / HD)
        spread = mm2(centred * centred, same_head) * (1.0 / HD)
        mix = (centred * lax.rsqrt(spread + GROUP_EPS) * gain).astype(BF)
        keep(mix, place_of, p, lin_ref, lin_give)


def send_back(refs, place_of):
    out_ref, ready_ref, got_ref, back_out, back_in = refs
    f = place_of[2]
    columns = ready_ref.shape[2]

    def back_copy(target, source):
        return pltpu.make_async_remote_copy(
            src_ref=ready_ref.at[target], dst_ref=got_ref.at[source],
            send_sem=back_out, recv_sem=back_in,
            device_id={"fs": target}, device_id_type=MESH,
        )

    for k in range(1, FOUR):
        back_copy((f + k) % FOUR, f).start()
    got_ref[f] = ready_ref[f]
    wide = FOUR * PAIR
    source, target = iota((wide, wide), 0), iota((wide, wide), 1)
    place = source % PAIR // 16 * (FOUR * 16) + source // PAIR * 16 + source % 16
    shuffle = ones_where(place == target)
    with jax.named_scope("o_back"):
        settle(got_ref.at[1:FOUR], back_in)
    with jax.named_scope("o_shuffle"):
        for b in range(columns // PAIR):
            lanes = slice(b * PAIR, (b + 1) * PAIR)
            joined = jnp.concatenate([got_ref[g, :, lanes] for g in range(FOUR)], axis=1)
            out_ref[:, b * wide : (b + 1) * wide] = dot(joined, shuffle).astype(BF)
    with jax.named_scope("o_drain"):
        settle(ready_ref.at[1:FOUR], back_out)


def layer_kernel(
    x_ref, gain_hbm, wr_ref, wk_ref, wv_ref, wq_ref, wak_hbm, wav_hbm, down_d_hbm, down_e_hbm,
    up_d_hbm, up_e_hbm, off_d_hbm, off_e_hbm, extra_ref, init_hbm, head_gain_hbm, sink_hbm,
    lin_out_hbm, att_out_hbm,
    out_ref,
    gain_ref, wak_ref, wav_ref, off_d_ref, off_e_ref, head_gain_ref, sink_ref,
    both_ref, hid_ref, stage_ref, cols_ref, ext_ref, down_d_ref, down_e_ref, up_d_ref, up_e_ref, init_ref,
    proj_ref, logd_ref, learn_ref, cos_ref, sin_ref, wout_ref,
    reads_ref, local_ref, msg_ref, rows_ref,
    recv_ref, sent_ref, enter_ref, halo_ref, comp_ref, total_ref,
    lin_ref, att_ref, lin_give, att_give, ready_ref, got_ref,
    load_sem, late_sem, x_out, x_in, hid_out, hid_in, stage_out, stage_in, ext_out, ext_in,
    ring_out, z_in, near_in, far_in, rest_x_out, rest_x_in, rest_z_out, rest_z_in,
    wz_out, wz_in, wx_out, wx_in, wc_out, wc_in,
    out_sem, in_sem, back_out_sem, back_in_sem, halo_out_sem, halo_in_sem,
    lin_out, lin_in, lin_out2, lin_in2, att_out, att_in, att_out2, att_in2, give_sem, back_out, back_in,
):
    place_of = tuple(lax.axis_index(a) for a in ("sp_0", "sp_1", "fs", "tp"))
    width = lin_out_hbm.shape[1]
    for peer in neighbours(place_of):
        pl.semaphore_signal(
            pltpu.get_barrier_semaphore(), inc=1, device_id=peer, device_id_type=MESH
        )
    pairs = (
        (down_d_hbm, down_d_ref), (down_e_hbm, down_e_ref), (up_d_hbm, up_d_ref), (up_e_hbm, up_e_ref),
        (init_hbm, init_ref), (off_d_hbm, off_d_ref), (off_e_hbm, off_e_ref), (head_gain_hbm, head_gain_ref),
        (sink_hbm, sink_ref), (lin_out_hbm, wout_ref.at[:, :width]), (att_out_hbm, wout_ref.at[:, width:]),
    )
    late = [pltpu.make_async_copy(a, b, late_sem.at[k]) for k, (a, b) in enumerate(pairs)]
    early = [
        pltpu.make_async_copy(a, b, load_sem.at[3 + k])
        for k, (a, b) in enumerate(((gain_hbm, gain_ref), (wak_hbm, wak_ref), (wav_hbm, wav_ref)))
    ]
    rows_steps = gather_rows(
        (wout_ref, rows_ref, wz_out, wz_in, wx_out, wx_in, wc_out, wc_in), place_of
    )
    project_rest = front(
        (
            x_ref, gain_ref, wr_ref, wk_ref, wv_ref, wq_ref, wak_ref, wav_ref, down_d_ref, down_e_ref,
            up_d_ref, up_e_ref, off_d_ref, off_e_ref, extra_ref, proj_ref, logd_ref, learn_ref,
            both_ref, hid_ref, stage_ref, cols_ref, ext_ref, load_sem,
            x_out, x_in, hid_out, hid_in, stage_out, stage_in, ext_out, ext_in,
            ring_out, z_in, near_in, far_in, rest_x_out, rest_x_in, rest_z_out, rest_z_in, cos_ref, sin_ref, late, early,
        ),
        place_of,
    )
    send_halo, send_maps, run = exchange(
        (
            msg_ref, init_ref, reads_ref, local_ref, head_gain_ref, proj_ref, cos_ref, sin_ref, sink_ref,
            lin_ref, att_ref, lin_give, att_give, recv_ref, sent_ref, enter_ref, halo_ref, comp_ref,
            out_sem, in_sem, back_out_sem, back_in_sem, halo_out_sem, halo_in_sem,
        ),
        place_of,
    )
    local_maps(
        (proj_ref, logd_ref, learn_ref, reads_ref, local_ref, msg_ref),
        project_rest,
        send_halo,
        send_maps,
        rows_steps,
    )
    att_share = share(
        att_ref, att_give, ((att_out, att_in), (att_out2, att_in2)), (give_sem.at[0], give_sem.at[1]), place_of
    )
    lin_share = share(
        lin_ref, lin_give, ((lin_out, lin_in), (lin_out2, lin_in2)), (give_sem.at[2], give_sem.at[3]), place_of
    )
    columns = ready_ref.shape[2]
    joined_rows = FOUR * ready_ref.shape[1]

    def product(ref, first):
        result = None
        for core in range(2):
            left = jnp.concatenate([ref[core, g].reshape(joined_rows, PAIR) for g in range(FOUR)], axis=1)
            weight = rows_ref[core, :, :, :, first : first + width].reshape(columns, width)
            term = dot(left, weight, NT)
            result = term if result is None else result + term
        return result

    def after_attend():
        att_share[0]()

    run(after_attend, rows_steps[2])
    lin_share[0]()
    rows_steps[3]()
    with jax.named_scope("o_att_wait"):
        att_share[1]()
        rows_steps[4]()
    with jax.named_scope("o_att"):
        total_ref[...] = product(att_ref, width)
    att_share[2]()
    with jax.named_scope("o_lin_wait"):
        lin_share[1]()
    with jax.named_scope("o_lin"):
        result = (total_ref[...] + product(lin_ref, 0)).astype(BF)
        ready_ref[...] = result.reshape(ready_ref.shape)
    send_back((out_ref, ready_ref, got_ref, back_out, back_in), place_of)
    lin_share[2]()


def local(
    inputs, input_norm_gain, receptance_weight, linear_key_weight, linear_value_weight,
    window_query_weight, window_key_weight, window_value_weight, decay_down_weight, decay_up_weight,
    decay_offset, decay_log_extra, erasure_down_weight, erasure_up_weight, erasure_offset,
    initial_state, head_norm_gain, query_sink_logit, linear_output_weight, window_output_weight,
):
    tokens, model = inputs.shape[1], 2 * inputs.shape[2]
    places = lax.axis_size(SP)
    nz, nx = lax.axis_size("sp_0"), lax.axis_size("sp_1")
    rows = receptance_weight.shape[0]
    out_rows = linear_output_weight.shape[1]
    columns = places * out_rows
    vmem = pl.BlockSpec(memory_space=pltpu.VMEM)
    hbm = pl.BlockSpec(memory_space=pltpu.HBM)
    dma = pltpu.SemaphoreType.DMA
    down_d, down_e = decay_down_weight.T, erasure_down_weight.T

    def space(kind, *shape):
        return pltpu.VMEM(shape, kind)

    out = pl.pallas_call(
        layer_kernel,
        out_shape=jax.ShapeDtypeStruct((tokens // 2, FOUR * columns), BF),
        in_specs=[hbm] * 20,
        out_specs=vmem,
        scratch_shapes=[
            space(F32, 1, model),
            space(BF, *window_key_weight.shape),
            space(BF, *window_value_weight.shape),
            space(F32, *decay_offset.shape),
            space(F32, *erasure_offset.shape),
            space(F32, 1, *head_norm_gain.shape),
            pltpu.SMEM(query_sink_logit.shape, F32),
            space(BF, 2, tokens, model // 2),
            space(BF, FOUR, tokens, model),
            space(BF, FOUR, rows, 5 * PAIR),
            space(BF, places, FOUR * rows, 5 * PAIR),
            space(F32, FOUR, *decay_log_extra.shape[1:]),
            space(BF, *down_d.shape),
            space(BF, *down_e.shape),
            space(BF, *decay_up_weight.shape),
            space(BF, *erasure_up_weight.shape),
            space(F32, *initial_state.shape),
            space(BF, FOUR, tokens, 5 * PAIR),
            space(F32, 2, FOUR, tokens, PAIR),
            space(F32, 2, FOUR, tokens, PAIR),
            space(F32, tokens + 2 * WINDOW, PAIR),
            space(F32, tokens + 2 * WINDOW, PAIR),
            space(BF, out_rows, 2 * FOUR * PAIR),
            space(F32, 2, FOUR, tokens, PAIR),
            space(F32, FOUR, tokens, PAIR),
            space(BF, places, 48, PAIR),
            space(BF, 2, nz, nx, out_rows, 2 * FOUR * PAIR),
            space(BF, places, 48, PAIR),
            space(BF, places, 16, PAIR),
            space(BF, places, 16, PAIR),
            space(BF, 2, FOUR, tokens, PAIR),
            space(F32, 4, places // 4, 3 * HD // 2, HD),
            space(F32, FOUR * tokens // 2, columns),
            space(BF, 2, FOUR, FOUR, tokens // 2, PAIR),
            space(BF, 2, FOUR, FOUR, tokens // 2, PAIR),
            space(BF, FOUR, tokens // 2, PAIR),
            space(BF, FOUR, tokens // 2, PAIR),
            space(BF, FOUR, tokens // 2, columns),
            space(BF, FOUR, tokens // 2, columns),
            dma((6,)), dma((11,)),
            dma, dma, dma((1,)), dma((4,)), dma, dma, dma, dma,
            dma, dma((2, nz // 2)), dma((nz,)), dma, dma, dma, dma, dma((2, nz // 2)),
            dma, dma, dma, dma((3,)), dma, dma,
            dma, dma, dma, dma, dma, dma,
            *[dma((1,)), dma((4,))] * 4, dma((FOUR,)), dma, dma,
        ],
        compiler_params=pltpu.CompilerParams(
            collective_id=0, has_side_effects=True, vmem_limit_bytes=63 * 2**20
        ),
        name="layer",
    )(
        inputs[0], input_norm_gain[None], receptance_weight, linear_key_weight, linear_value_weight,
        window_query_weight, window_key_weight, window_value_weight, down_d, down_e,
        decay_up_weight, erasure_up_weight, decay_offset, erasure_offset, decay_log_extra,
        initial_state, head_norm_gain[None], query_sink_logit, linear_output_weight.T,
        window_output_weight.T,
    )
    return out[None]


def solution(mesh):
    finer = Mesh(
        mesh.devices.reshape(8, 4, mesh.shape["fs"], mesh.shape["tp"]), ("sp_0", "sp_1", "fs", "tp")
    )
    placed = (
        P("fs", SP, "tp"),
        P(),
        P(SP_FS, "tp"),
        P(SP_FS, "tp"),
        P(SP_FS, "tp"),
        P(SP_FS, "tp"),
        P(SP_FS, "tp"),
        P(SP_FS, "tp"),
        P(),
        P(),
        P(),
        P("fs", "tp", SP),
        P(),
        P(),
        P(),
        P(),
        P(),
        P(),
        P("tp", SP_FS),
        P("tp", SP_FS),
    )
    return jax.shard_map(
        local, mesh=finer, in_specs=placed, out_specs=P("fs", SP_TP, None), check_vma=False
    )
```

```python
import math
import functools
import jax
import jax.numpy as jnp
from jax import lax
from jax.experimental import pallas as pl
from jax.experimental.pallas import tpu as pltpu

from jax.sharding import Mesh
from jax.sharding import PartitionSpec as P

HD = 64
CH = 64
PAIR = 128
WINDOW = 128
GRID_W = 64
ATT_BLOCK = 128
SP = ("sp_0", "sp_1")
FOUR = 4
ROUND = 2
SP_FS = ("sp_0", "sp_1", "fs")
SP_TP = ("sp_0", "sp_1", "tp")
NORM_EPS = 1e-06
GROUP_EPS = 0.00064
ROPE_BASE = 10000.0
F32 = jnp.float32
BF = jnp.bfloat16
MESSAGE = jnp.bfloat16
MESH = pl.DeviceIdType.MESH
NN = (((1,), (0,)), ((), ()))
NT = (((1,), (1,)), ((), ()))
TN = (((0,), (0,)), ((), ()))


def dot(a, b, dims=NN):
    return lax.dot_general(a, b, dims, preferred_element_type=F32)


def split2(a):
    high = a.astype(BF)
    return high, (a - high.astype(F32)).astype(BF)


def split3(a):
    high, rest = a.astype(BF), None
    rest = a - high.astype(F32)
    mid = rest.astype(BF)
    return high, mid, (rest - mid.astype(F32)).astype(BF)


def mm3(a, b, dims=NN):
    (ka,), (kb,) = dims[0]
    a_hi, a_lo = split2(a)
    b_hi, b_lo = split2(b)
    free = 1 - kb
    if b.shape[free] == PAIR:
        upper = jnp.concatenate([b_hi, b_lo], axis=free)
        lower = jnp.concatenate([b_hi, jnp.zeros_like(b_lo)], axis=free)
        wide = dot(
            jnp.concatenate([a_hi, a_lo], axis=ka), jnp.concatenate([upper, lower], axis=kb), dims
        )
        return wide[:, :PAIR] + wide[:, PAIR:]
    main = dot(
        jnp.concatenate([a_hi, a_lo], axis=ka), jnp.concatenate([b_hi, b_hi], axis=kb), dims
    )
    return main + dot(a_hi, b_lo, dims)


def mm2(a, b_exact, dims=NN):
    (ka,), (kb,) = dims[0]
    a_hi, a_lo = split2(a)
    return dot(
        jnp.concatenate([a_hi, a_lo], axis=ka), jnp.concatenate([b_exact, b_exact], axis=kb), dims
    )


def iota(shape, dim):
    return lax.broadcasted_iota(jnp.int32, shape, dim)


def ones_where(cond):
    return jnp.where(cond, 1.0, 0.0).astype(BF)


def settle(where, sem):
    pltpu.make_async_copy(where, where, sem).wait()


def ring_of_four(buf, out_sem, in_sem, give_ref=None, core=None):
    me = lax.axis_index("fs")
    right, left, far = (me + 1) % FOUR, (me + 3) % FOUR, (me + 2) % FOUR
    half = buf.shape[1] // 2
    near_buf = buf if give_ref is None else give_ref[1]

    def piece(block, part, target, number):
        where = buf.at[block, part * half : (part + 1) * half]
        return pltpu.make_async_remote_copy(
            src_ref=where, dst_ref=where, send_sem=out_sem.at[0], recv_sem=in_sem.at[number],
            device_id={"fs": target}, device_id_type=MESH,
        )

    def launch(part, target, number):
        if give_ref is None:
            piece(me, part, target, number).start()
            return
        rows = slice(part * half, (part + 1) * half)
        pltpu.make_async_remote_copy(
            src_ref=give_ref[0].at[rows], dst_ref=near_buf.at[me, rows],
            send_sem=out_sem.at[0], recv_sem=in_sem.at[number],
            device_id={"fs": target, "tp": core}, device_id_type=MESH,
        ).start()

    def start():
        launch(0, right, 0)
        launch(1, left, 1)
        launch(1, right, 2)
        launch(0, left, 2)

    def relay():
        piece(left, 0, right, 0).wait_recv()
        piece(left, 0, right, 3).start()
        piece(right, 1, left, 1).wait_recv()
        piece(right, 1, left, 3).start()

    def arrive_near():
        settle(buf.at[0], in_sem.at[2])

    def arrive_far():
        settle(buf.at[0], in_sem.at[3])

    def finish_sends():
        settle(buf.at[0:3], out_sem.at[0])

    return start, relay, arrive_near, arrive_far, finish_sends


def peer_id(index):
    inner = lax.axis_size("sp_1")
    return {"sp_0": index // inner, "sp_1": index % inner}


def neighbours(place_of):
    z, x, f, c = place_of
    nz, nx = lax.axis_size("sp_0"), lax.axis_size("sp_1")
    peers = [{"fs": (f + k) % FOUR} for k in range(1, FOUR)] + [{"tp": 1 - c}]
    peers += [{"sp_0": (z + k) % nz} for k in (1, nz - 1)]
    return peers + [{"sp_1": (x + k) % nx} for k in range(1, nx)]


def rope_tables(place, cos_ref, sin_ref):
    reach = cos_ref.shape[0]
    block = reach // 3
    spot = iota((reach, PAIR), 0)
    lane = iota((reach, PAIR), 1)
    grid_row = ((place - 1) * (block // GRID_W) + spot // GRID_W).astype(F32)
    grid_col = (spot % GRID_W).astype(F32)
    power = (lane % 16).astype(F32) * (1.0 / 16)
    angle = jnp.where(lane % HD < HD // 2, grid_row, grid_col) * jnp.exp(power * -math.log(ROPE_BASE))
    cos_ref[...] = jnp.cos(angle)
    sin_ref[...] = jnp.sin(angle)


def share(ref, give_ref, ring_sems, give_sems, place_of):
    f, c = place_of[2:]
    own = ring_of_four(ref.at[c], *ring_sems[0])
    other = ring_of_four(ref.at[1 - c], *ring_sems[1], (give_ref, ref.at[c]), 1 - c)

    def give(core):
        return pltpu.make_async_remote_copy(
            src_ref=give_ref, dst_ref=ref.at[core, f], send_sem=give_sems[0], recv_sem=give_sems[1],
            device_id={"tp": 1 - c}, device_id_type=MESH,
        )

    def start():
        own[0]()
        other[0]()
        give(c).start()

    def collect():
        own[1]()
        other[1]()
        give(1 - c).wait_recv()
        for ring in (own, other):
            ring[2]()
            ring[3]()

    def drain():
        give(c).wait_send()
        own[4]()
        other[4]()

    return start, collect, drain


def front(refs, place_of):
    (
        x_ref, gain_ref, wr_ref, wk_ref, wv_ref, wq_ref, wak_ref, wav_ref, down_d_ref, down_e_ref,
        up_d_ref, up_e_ref, off_d_ref, off_e_ref, extra_ref, proj_ref, logd_ref, learn_ref,
        both_ref, hid_ref, stage_ref, cols_ref, ext_ref, load_sem,
        x_out, x_in, hid_out, hid_in, stage_out, stage_in, ext_out, ext_in,
        ring_out, z_in, near_in, far_in, rest_x_out, rest_x_in, rest_z_out, rest_z_in, cos_ref, sin_ref, late, early,
    ) = refs
    z, x, f, c = place_of
    nz, nx = lax.axis_size("sp_0"), lax.axis_size("sp_1")
    mine = z * nx + x
    rows = wr_ref.shape[0]
    loads = []
    for g in range(FOUR):
        for k, ref in enumerate((wr_ref, wk_ref, wv_ref, wq_ref)):
            loads.append((ref.at[:, g * PAIR : (g + 1) * PAIR], stage_ref.at[g, :, k * PAIR : (k + 1) * PAIR], 0))
    loads.append((x_ref, both_ref.at[c], 1))
    loads.append((extra_ref.at[0], ext_ref.at[f], 2))
    loads = [pltpu.make_async_copy(start, end, load_sem.at[number]) for start, end, number in loads]
    for load in early + loads + late:
        load.start()
    for load in early:
        load.wait()
    low = iota((rows, PAIR), 1) < HD
    keys, values = wak_ref[...].astype(F32), wav_ref[...].astype(F32)
    shared = [
        jnp.where(low, keys, pltpu.roll(values, HD, 1)).astype(BF),
        jnp.where(low, pltpu.roll(keys, HD, 1), values).astype(BF),
    ]
    for g in range(FOUR):
        stage_ref[g, :, 4 * PAIR :] = shared[g // 2]
    with jax.named_scope("f_load"):
        settle(stage_ref.at[:, :, : 4 * PAIR], load_sem.at[0])
        for load in loads[-2:]:
            load.wait()
    my_rows = pl.ds(pl.multiple_of(f * rows, rows), rows)
    cols_ref[mine, my_rows, :] = stage_ref[f]
    with jax.named_scope("f_meet"):
        pl.semaphore_wait(pltpu.get_barrier_semaphore(), len(neighbours(place_of)))

    half_copy = pltpu.make_async_remote_copy(
        src_ref=both_ref.at[c], dst_ref=both_ref.at[c], send_sem=x_out, recv_sem=x_in,
        device_id={"tp": 1 - c}, device_id_type=MESH,
    )
    half_copy.start()

    def stage_copy(k):
        g = (f + k) % FOUR
        return pltpu.make_async_remote_copy(
            src_ref=stage_ref.at[g], dst_ref=cols_ref.at[mine, my_rows, :],
            send_sem=stage_out, recv_sem=stage_in, device_id={"fs": g}, device_id_type=MESH,
        )

    def ext_copy(k, source):
        return pltpu.make_async_remote_copy(
            src_ref=ext_ref.at[source], dst_ref=ext_ref.at[source],
            send_sem=ext_out, recv_sem=ext_in, device_id={"fs": (f + k) % FOUR}, device_id_type=MESH,
        )

    for k in range(1, FOUR):
        stage_copy(k).start()

    def z_block(k):
        if k == 0:
            return z
        step = (k - 1) // 2
        return (z + nz - 1 - step) % nz if k % 2 else (z + 1 + step) % nz

    main = 3 * PAIR

    def rest_x_copy(k):
        where = cols_ref.at[mine, :, main:]
        return pltpu.make_async_remote_copy(
            src_ref=where, dst_ref=where, send_sem=rest_x_out, recv_sem=rest_x_in,
            device_id={"sp_1": (x + k) % nx}, device_id_type=MESH,
        )

    def rest_z_copy(block, side, step):
        where = cols_ref.at[pl.ds(block * nx, nx), :, main:]
        return pltpu.make_async_remote_copy(
            src_ref=where, dst_ref=where, send_sem=rest_z_out, recv_sem=rest_z_in.at[side, step],
            device_id={"sp_0": (z + (1 if side == 0 else nz - 1)) % nz}, device_id_type=MESH,
        )

    def rest_begin():
        settle(cols_ref.at[0 : nx - 1, :, main:], rest_x_in)
        rest_z_copy(z, 0, 0).start()
        rest_z_copy(z, 1, 0).start()

    def rest_pass(step):
        for side, last in ((0, nz // 2 - 1), (1, nz // 2 - 2)):
            if step <= last:
                block = z_block(2 * step + 1 + side)
                rest_z_copy(block, side, step).wait_recv()
                if step < last:
                    rest_z_copy(block, side, step + 1).start()

    def z_copy(k_from, side, step):
        where = cols_ref.at[z_block(k_from) * nx + x, :, :main]
        return pltpu.make_async_remote_copy(
            src_ref=where, dst_ref=where, send_sem=ring_out, recv_sem=z_in.at[side, step],
            device_id={"sp_0": (z + (1 if side == 0 else nz - 1)) % nz}, device_id_type=MESH,
        )

    def near_copy(k, side, column):
        where = cols_ref.at[z_block(k) * nx + column, :, :main]
        return pltpu.make_async_remote_copy(
            src_ref=where, dst_ref=where, send_sem=ring_out, recv_sem=near_in.at[k],
            device_id={"sp_1": (x + (1 if side == 0 else nx - 1)) % nx}, device_id_type=MESH,
        )

    def far_copy(k, column):
        where = cols_ref.at[z_block(k) * nx + column, :, :main]
        return pltpu.make_async_remote_copy(
            src_ref=where, dst_ref=where, send_sem=ring_out, recv_sem=far_in,
            device_id={"sp_1": (x + (1 if k % 2 == 0 else nx - 1)) % nx}, device_id_type=MESH,
        )

    left, right, _ = (x + nx - 1) % nx, (x + 1) % nx, 0

    def spread(k):
        near_copy(k, 0, x).start()
        near_copy(k, 1, x).start()

    def pass_on(k):
        settle(cols_ref.at[0:2, :, :main], near_in.at[k])
        far_copy(k, left if k % 2 == 0 else right).start()

    with jax.named_scope("f_stage_wait"):
        settle(stage_ref.at[1:FOUR], stage_in)
    z_copy(0, 0, 0).start()
    z_copy(0, 1, 0).start()
    spread(0)
    for k in range(1, nx):
        rest_x_copy(k).start()

    with jax.named_scope("f_norm"):
        half_copy.wait_recv()
        full = jnp.concatenate([both_ref[0], both_ref[1]], axis=1).astype(F32)
        scale = lax.rsqrt(jnp.mean(full * full, axis=-1, keepdims=True) + NORM_EPS)
        hid_ref[f] = (full * scale * gain_ref[...]).astype(BF)
    start, relay, arrive_near, arrive_far, finish_sends = ring_of_four(hid_ref, hid_out, hid_in)
    for k in range(1, FOUR):
        ext_copy(k, f).start()
    start()
    with jax.named_scope("f_rope"):
        rope_tables(mine, cos_ref, sin_ref)

    steps = nz // 2
    with jax.named_scope("f_ring"):
        for step in range(steps):
            k = 2 * step + 1
            z_copy(k, 0, step).wait_recv()
            if step < steps - 1:
                z_copy(k, 0, step + 1).start()
            spread(k)
            if step < steps - 1:
                z_copy(k + 1, 1, step).wait_recv()
                if step < steps - 2:
                    z_copy(k + 1, 1, step + 1).start()
                spread(k + 1)
            if step == 0:
                pass_on(0)
            else:
                pass_on(k - 2)
                pass_on(k - 1)
            if step == 0:
                rest_begin()
            elif step > 1:
                rest_pass(step - 2)
            if step == 1:
                relay()
    with jax.named_scope("f_pass_last"):
        pass_on(nz - 1)
    for load in late:
        load.wait()
    settle(ext_ref.at[1:FOUR], ext_in)
    tokens = hid_ref.shape[1]
    heads = ext_ref.shape[1]
    chosen = pl.ds(pl.multiple_of(c * heads * HD + f * PAIR, PAIR), PAIR)
    select = ones_where(iota((heads, PAIR), 0) == 2 * f + iota((heads, PAIR), 1) // HD).astype(F32)

    def rates(p):
        rows_in = hid_ref[p]
        decay_low = dot(rows_in, down_d_ref[...], NT).astype(BF)
        learn_low = dot(rows_in, down_e_ref[...], NT).astype(BF)
        decay_act = jnp.tanh(decay_low.astype(F32)).astype(BF)
        spikes = lax.dot_general(
            ext_ref[p], select, TN, precision=lax.Precision.HIGHEST, preferred_element_type=F32
        )
        for d in range(2):
            pre = off_d_ref[d : d + 1, chosen] + dot(decay_act, up_d_ref[d, :, chosen])
            softplus = jnp.maximum(-pre, 0.0) + jnp.log1p(jnp.exp(-jnp.abs(pre)))
            logd_ref[d, p] = spikes - jnp.exp(-softplus - 0.5)
            learn_ref[d, p] = jax.nn.sigmoid(
                off_e_ref[d : d + 1, chosen] + dot(learn_low, up_e_ref[d, :, chosen])
            )

    with jax.named_scope("f_rates"):
        rates(f)
        arrive_near()
        rates((f + 1) % FOUR)
        rates((f + 3) % FOUR)
    with jax.named_scope("f_hid_wait"):
        arrive_far()
    with jax.named_scope("f_rates_far"):
        rates((f + 2) % FOUR)
    hidden = hid_ref[...].reshape(FOUR * tokens, hid_ref.shape[2])

    with jax.named_scope("f_far_wait"):
        settle(cols_ref.at[0:nz, :, :main], far_in)
    depth = cols_ref.shape[0] * cols_ref.shape[1]
    with jax.named_scope("f_proj"):
        for first_col, last_col in ((0, 256), (256, 384)):
            weight = cols_ref[:, :, first_col:last_col].reshape(depth, last_col - first_col)
            result = dot(hidden, weight).astype(BF)
            for p in range(FOUR):
                proj_ref[p, :, first_col:last_col] = result[p * tokens : (p + 1) * tokens]

    rest_pass(nz // 2 - 2)
    half_copy.wait_send()
    finish_sends()
    settle(stage_ref.at[1:FOUR], stage_out)
    settle(ext_ref.at[1:FOUR], ext_out)
    settle(cols_ref.at[0 : 4 * nz - 1, :, :main], ring_out)

    def project_rest():
        rest_pass(nz // 2 - 1)
        weight = cols_ref[:, :, main:].reshape(depth, cols_ref.shape[2] - main)
        result = dot(hid_ref[...].reshape(FOUR * tokens, hid_ref.shape[2]), weight).astype(BF)
        for p in range(FOUR):
            proj_ref[p, :, main:] = result[p * tokens : (p + 1) * tokens]
        settle(cols_ref.at[0 : nx - 1, :, main:], rest_x_out)
        settle(cols_ref.at[0 : nx * (nz - 1), :, main:], rest_z_out)

    return project_rest


def stacked(x):
    low = iota(x.shape, 1) < HD
    return jnp.concatenate([jnp.where(low, x, 0.0), jnp.where(low, 0.0, x)], axis=0)


def unstacked(x):
    return x[:CH] + x[CH:]


def gather_rows(refs, place_of):
    wout_ref, rows_ref, z_out, z_in, x_out, x_in, c_out, c_in = refs
    z, x, _, c = place_of
    nz, nx = lax.axis_size("sp_0"), lax.axis_size("sp_1")
    half = nz // 2
    left, right, across = (x + nx - 1) % nx, (x + 1) % nx, (x + 2) % nx

    def z_copy(k, source):
        return pltpu.make_async_remote_copy(
            src_ref=wout_ref, dst_ref=rows_ref.at[c, source, x], send_sem=z_out, recv_sem=z_in,
            device_id={"sp_0": (z + k) % nz}, device_id_type=MESH,
        )

    def x_copy(number, column):
        part = slice(0, nz) if number < 2 else slice(0, half) if number == 2 else slice(half, nz)
        where = rows_ref.at[c, part, column]
        return pltpu.make_async_remote_copy(
            src_ref=where, dst_ref=where, send_sem=x_out, recv_sem=x_in.at[min(number, 2)],
            device_id={"sp_1": right if number % 2 == 0 else left}, device_id_type=MESH,
        )

    def c_copy(number, core, column):
        where = rows_ref.at[core, :, column]
        return pltpu.make_async_remote_copy(
            src_ref=where, dst_ref=where, send_sem=c_out, recv_sem=c_in,
            device_id={"tp": 1 - c}, device_id_type=MESH,
        )

    def first():
        rows_ref[c, z, x] = wout_ref[...]
        for k in range(1, nz):
            z_copy(k, z).start()

    def second():
        settle(rows_ref.at[c, 1:nz, x], z_in)
        x_copy(0, x).start()
        x_copy(1, x).start()
        c_copy(0, c, x).start()

    def third():
        x_copy(0, left).wait_recv()
        x_copy(2, left).start()
        x_copy(1, right).wait_recv()
        x_copy(3, right).start()
        c_copy(1, c, left).start()
        c_copy(2, c, right).start()

    def fourth():
        settle(rows_ref.at[c, :, across], x_in.at[2])
        c_copy(3, c, across).start()

    def last():
        settle(rows_ref.at[1 - c], c_in)
        settle(rows_ref.at[c], c_out)
        settle(rows_ref.at[c, 1:nz, x], z_out)
        settle(rows_ref.at[c, :, 1:nx], x_out)

    return first, second, third, fourth, last


def local_maps(refs, project_rest, send_halo, send_maps, rows_steps):
    proj_ref, logd_ref, learn_ref, q_ref, o_ref, msg_ref = refs
    rows_steps[0]()
    row = iota((2 * CH, 2 * CH), 0)
    col = iota((2 * CH, 2 * CH), 1)
    t, s = row % CH, col % CH
    eye = row == col
    same_head = ones_where(row // HD == col // HD)
    tri = [ones_where((iota((CH, CH), 0) >= iota((CH, CH), 1))), ones_where((iota((CH, CH), 0) <= iota((CH, CH), 1)))]
    strict = [t > s, t < s]
    within = [t >= s, t <= s]

    def one_round(it, carry):
        @pl.when(it == 1)
        def _():
            project_rest()
            for u in range(ROUND):
                send_maps(u)
            send_halo()

        seqs = [it * ROUND + u for u in range(ROUND)]
        recept, keys, values, unit = {}, {}, {}, {}
        for u, p in enumerate(seqs):
            recept[u] = proj_ref[p, :, :PAIR].astype(F32)
            keys[u] = proj_ref[p, :, PAIR : 2 * PAIR].astype(F32)
            values[u] = proj_ref[p, :, 2 * PAIR : 3 * PAIR].astype(F32)
            unit[u] = keys[u] * lax.rsqrt(mm2(keys[u] * keys[u], same_head) + NORM_EPS)
        jobs = [(u, d, c) for u in range(ROUND) for d in range(2) for c in range(2)]
        stage = {}
        for u, d, c in jobs:
            rows = slice(c * CH, (c + 1) * CH)
            logd = logd_ref[d, seqs[u], rows, :]
            parts = jnp.concatenate(split3(logd), axis=0)
            total = dot(jnp.concatenate([tri[d]] * 3, axis=1), parts)
            middle = total[CH // 2 - 1 : CH // 2] if d == 0 else total[CH // 2 : CH // 2 + 1]
            last = total[CH - 1 : CH] if d == 0 else total[0:1]
            grow = jnp.exp(total - middle)
            shrink = jnp.exp(middle - total)
            read = recept[u][rows] * grow
            mark = unit[u][rows] * jnp.exp(total - logd - middle)
            erase = unit[u][rows] * learn_ref[d, seqs[u], rows, :] * shrink
            key = keys[u][rows] * shrink
            read_s, mark_s, erase_s, key_s = map(stacked, (read, mark, erase, key))
            scores = mm3(
                jnp.concatenate([mark_s, read_s], axis=0),
                jnp.concatenate([erase_s, key_s], axis=0),
                NT,
            )
            stage[u, d, c] = (read, mark_s, erase_s, key_s, scores, jnp.exp(middle), jnp.exp(last - middle), jnp.exp(last))
        inverse = {}
        grams = {}
        for u, d, c in jobs:
            gram = jnp.where(strict[d], stage[u, d, c][4][: 2 * CH, : 2 * CH], 0.0)
            grams[u, d, c] = gram
            inverse[u, d, c] = jnp.where(eye, 1.0, 0.0) - jnp.where(t // 2 == s // 2, gram, 0.0)
        block = 2
        while block < CH:
            joins = (t // (2 * block) == s // (2 * block)) & (t // block != s // block)
            for job in jobs:
                found = inverse[job]
                inverse[job] = found - mm3(found, mm3(jnp.where(joins, grams[job], 0.0), found))
            block *= 2
        maps, reads, outs = {}, {}, {}
        for u, d, c in jobs:
            rows = slice(c * CH, (c + 1) * CH)
            read, mark_s, erase_s, key_s, scores, to_start, to_end, whole = stage[u, d, c]
            val_s = stacked(values[u][rows]).astype(BF)
            cross = jnp.where(strict[d], scores[: 2 * CH, 2 * CH :], 0.0)
            read_e = jnp.where(within[d], scores[2 * CH :, : 2 * CH], 0.0)
            read_k = jnp.where(within[d], scores[2 * CH :, 2 * CH :], 0.0)
            solved = mm3(inverse[u, d, c], jnp.concatenate([mark_s, mm2(cross, val_s)], axis=1))
            solved = jnp.concatenate([solved[:, :PAIR] * to_start, solved[:, PAIR:]], axis=1)
            taken = mm3(read_e, solved)
            reads[u, d, c] = read * to_start - unstacked(taken[:, :PAIR])
            outs[u, d, c] = unstacked(mm2(read_k, val_s) - taken[:, PAIR:])
            ended = mm3(solved, erase_s * to_end, TN)
            k_hi, k_lo = split2(key_s * to_end)
            added = dot(jnp.concatenate([val_s, val_s], axis=0), jnp.concatenate([k_hi, k_lo], axis=0), TN)
            prod = jnp.where(eye, whole - 1.0, 0.0) - ended[:PAIR]
            maps[u, d, c] = (prod, added - ended[PAIR:])
        for u, p in enumerate(seqs):
            out_rows = [outs[u, 0, 0] + outs[u, 1, 0], outs[u, 0, 1] + outs[u, 1, 1]]
            for d in range(2):
                first, second = (0, 1) if d == 0 else (1, 0)
                (prod1, add1), (prod2, add2) = maps[u, d, first], maps[u, d, second]
                both = jnp.concatenate([prod1, add1], axis=0)
                through = mm3(reads[u, d, second], both, NT)
                q_ref[d, p, first * CH : (first + 1) * CH, :] = reads[u, d, first]
                q_ref[d, p, second * CH : (second + 1) * CH, :] = reads[u, d, second] + through[:, :PAIR]
                out_rows[second] = out_rows[second] + through[:, PAIR:]
                joined = mm3(both, prod2)
                prod = prod1 + prod2 + joined[:PAIR]
                add = add1 + joined[PAIR:] + add2
                for hh in range(2):
                    for half in range(2):
                        message = jnp.concatenate(
                            [
                                folded(prod, hh, hh * HD, HD // 2),
                                folded(add, hh, hh * HD + half * (HD // 2), HD // 4),
                            ],
                            axis=0,
                        )
                        msg_ref[d * 16 + p * 4 + hh * 2 + half] = message.astype(msg_ref.dtype)
            for c in range(2):
                o_ref[p, c * CH : (c + 1) * CH, :] = out_rows[c]

        return carry

    with jax.named_scope("l_loop"):
        lax.fori_loop(0, FOUR // ROUND, one_round, 0)
    for u in range(ROUND):
        send_maps(FOUR - ROUND + u)
    rows_steps[1]()


def folded(x, hh, first, count):
    upper, lower = x[first : first + count], x[first + count : first + 2 * count]
    if hh == 0:
        return upper + pltpu.roll(lower, HD, 1)
    return pltpu.roll(upper, HD, 1) + lower


def exchange(refs, place_of):
    (
        msg_ref, init_ref, reads_ref, local_ref, gain_ref, proj_ref, cos_ref, sin_ref, sink_ref, lin_ref, att_ref, lin_give, att_give,
        recv_ref, sent_ref, enter_ref, halo_ref, comp_ref,
        out_sem, in_sem, back_out_sem, back_in_sem, halo_out_sem, halo_in_sem,
    ) = refs
    count = recv_ref.shape[0]
    place = place_of[0] * lax.axis_size("sp_1") + place_of[1]
    kv_first = 4 * PAIR

    def halo_copy(side):
        target = (place + count - 1 + 2 * side) % count
        return pltpu.make_async_remote_copy(
            src_ref=proj_ref.at[:, :, kv_first : kv_first + PAIR],
            dst_ref=halo_ref.at[1 - side],
            send_sem=halo_out_sem,
            recv_sem=halo_in_sem,
            device_id=peer_id(target),
            device_id_type=MESH,
        )

    def map_copy(target):
        return pltpu.make_async_remote_copy(
            src_ref=msg_ref.at[target],
            dst_ref=recv_ref.at[place],
            send_sem=out_sem,
            recv_sem=in_sem,
            device_id=peer_id(target),
            device_id_type=MESH,
        )

    def entry_copy(target):
        return pltpu.make_async_remote_copy(
            src_ref=sent_ref.at[target],
            dst_ref=enter_ref.at[place],
            send_sem=back_out_sem,
            recv_sem=back_in_sem,
            device_id=peer_id(target),
            device_id_type=MESH,
        )

    def send_halo():
        halo_copy(0).start()
        halo_copy(1).start()

    def send_maps(p):
        for d in range(2):
            for q in range(4):
                target = d * 16 + p * 4 + q

                @pl.when(target != place)
                def _():
                    map_copy(target).start()

    def run(after_attend, after_chain):
        tokens = local_ref.shape[1]
        with jax.named_scope("x_halo"):
            settle(halo_ref, halo_in_sem)
            settle(halo_ref, halo_out_sem)
        lane = iota((1, PAIR), 1)
        low = lane < HD
        front = lane % 32 < 16

        def turned(v, first, last):
            other = jnp.where(front, -pltpu.roll(v, PAIR - 16, 1), pltpu.roll(v, 16, 1))
            return v * cos_ref[first:last, :] + other * sin_ref[first:last, :]

        reach = 3 * tokens
        q_pos = place * tokens + iota((2 * tokens, reach), 0) % tokens
        k_pos = (place - 1) * tokens + iota((2 * tokens, reach), 1)
        allowed = (jnp.abs(q_pos - k_pos) <= WINDOW) & (k_pos >= 0) & (k_pos < count * tokens)
        upper = iota((2 * tokens, 1), 0) < tokens
        pair = lax.axis_index("fs")
        first_head = lax.axis_index("tp") * (2 * FOUR) + 2 * pair
        sink = jnp.where(upper, sink_ref[first_head], sink_ref[first_head + 1])

        def attend(p, carry):
            kv = jnp.concatenate(
                [halo_ref[0, p], proj_ref[p, :, kv_first : kv_first + PAIR], halo_ref[1, p]], axis=0
            ).astype(F32)
            roped = turned(kv, 0, reach)
            swapped = pltpu.roll(kv, HD, 1)
            key = jnp.where(low, roped, pltpu.roll(roped, HD, 1)).astype(BF)
            value = jnp.where(low, swapped, kv).astype(BF)
            query = turned(proj_ref[p, :, kv_first - PAIR : kv_first].astype(F32), tokens, 2 * tokens)
            query = jnp.concatenate([jnp.where(low, query, 0.0), jnp.where(low, 0.0, query)], axis=0)
            scores = dot(query.astype(BF), key, NT) * HD**-0.5
            scores = jnp.where(allowed, scores, -jnp.inf)
            top = jnp.maximum(jnp.max(scores, axis=-1, keepdims=True), sink)
            raised = jnp.exp(scores - top)
            total = jnp.exp(sink - top) + jnp.sum(raised, axis=-1, keepdims=True)
            mixed = dot((raised / total).astype(BF), value)
            keep(jnp.where(low, mixed[:tokens], mixed[tokens:]).astype(BF), place_of, p, att_ref, att_give)
            return carry

        with jax.named_scope("x_attend"):
            lax.fori_loop(0, FOUR, attend, 0)

        after_attend()
        recv_ref[place] = msg_ref[place]

        with jax.named_scope("x_await_map"):
            settle(recv_ref.at[1:count], in_sem)
            settle(msg_ref.at[1:count], out_sem)

        unit_idx = place // 2
        direction, half = unit_idx // 8, place % 2
        rows = HD // 2
        quarter = rows // 2
        start = pl.multiple_of(half * rows, rows)
        groups = 4
        length = count // groups

        def nth(step):
            return direction * (count - 1) + step * (1 - 2 * direction)

        def message(step):
            m = recv_ref[nth(step)].astype(F32)
            return jnp.concatenate([m[:rows, :HD], m[:rows, HD:], m[rows:, :HD], m[rows:, HD:]], axis=0)

        def extend(s, maps):
            longer = []
            for g in range(groups):
                step = message(g * length + s)
                comp_ref[g, s] = maps[g]
                longer.append(maps[g] + mm2(maps[g], step[:HD].astype(BF)) + step)
            return tuple(longer)

        nothing = jnp.zeros((3 * rows, HD), F32)
        with jax.named_scope("x_compose"):
            maps = lax.fori_loop(0, length, extend, (nothing,) * groups)
        state = init_ref[direction, first_head + unit_idx % 2, pl.ds(start, rows), :]

        def dispatch(g):
            def one(s, carry):
                target = nth(g * length + s)

                @pl.when(target != place)
                def _():
                    entry_copy(target).start()

                return carry

            lax.fori_loop(0, length, one, 0)

        with jax.named_scope("x_chain"):
            for g in range(groups):
                for s in range(length):
                    before = comp_ref[g, s]
                    entry = state + mm3(state, before[:HD]) + before[HD:] if s else state
                    sent_ref[nth(g * length + s)] = jnp.concatenate(
                        [entry[:quarter], entry[quarter:]], axis=1
                    ).astype(BF)
                state = state + mm3(state, maps[g][:HD]) + maps[g][HD:]
                if g:
                    dispatch(g - 1)
        enter_ref[place] = sent_ref[place]
        dispatch(groups - 1)
        after_chain()

        with jax.named_scope("x_await_entry"):
            settle(enter_ref.at[1:count], back_in_sem)
            settle(sent_ref.at[1:count], back_out_sem)
        with jax.named_scope("x_finish"):
            finish(reads_ref, local_ref, enter_ref, gain_ref, lin_ref, lin_give, place_of)

    return send_halo, send_maps, run


def keep(value, place_of, p, mine_ref, give_ref):
    f, c = place_of[2:]
    half = value.shape[0] // 2
    mine_ref[c, f, p] = jnp.where(c == 0, value[:half], value[half:])
    give_ref[p] = jnp.where(c == 0, value[half:], value[:half])


def finish(q_ref, o_ref, enter_ref, gain_ref, lin_ref, lin_give, place_of):
    row = iota((PAIR, PAIR), 0)
    col = iota((PAIR, PAIR), 1)
    same_head = ones_where(row // HD == col // HD)
    low = iota((HD // 4, PAIR), 1) < HD
    start = (lax.axis_index("tp") * FOUR + lax.axis_index("fs")) * PAIR
    gain = gain_ref[:, pl.ds(pl.multiple_of(start, PAIR), PAIR)]
    for p in range(FOUR):
        out = o_ref[p]
        for d in range(2):
            pieces = []
            for hh in range(2):
                for half in range(2):
                    m = enter_ref[d * 16 + p * 4 + hh * 2 + half].astype(F32)
                    turned = pltpu.roll(m, HD, 1)
                    if hh == 0:
                        pieces += [jnp.where(low, m, 0.0), jnp.where(low, turned, 0.0)]
                    else:
                        pieces += [jnp.where(low, 0.0, turned), jnp.where(low, 0.0, m)]
            out = out + mm2(q_ref[d, p], jnp.concatenate(pieces, axis=0).astype(BF), NT)
        centred = out - mm2(out, same_head) * (1.0 / HD)
        spread = mm2(centred * centred, same_head) * (1.0 / HD)
        mix = (centred * lax.rsqrt(spread + GROUP_EPS) * gain).astype(BF)
        keep(mix, place_of, p, lin_ref, lin_give)


def send_back(refs, place_of):
    out_ref, ready_ref, got_ref, back_out, back_in = refs
    f = place_of[2]
    columns = ready_ref.shape[2]

    def back_copy(target, source):
        return pltpu.make_async_remote_copy(
            src_ref=ready_ref.at[target], dst_ref=got_ref.at[source],
            send_sem=back_out, recv_sem=back_in,
            device_id={"fs": target}, device_id_type=MESH,
        )

    for k in range(1, FOUR):
        back_copy((f + k) % FOUR, f).start()
    got_ref[f] = ready_ref[f]
    wide = FOUR * PAIR
    source, target = iota((wide, wide), 0), iota((wide, wide), 1)
    place = source % PAIR // 16 * (FOUR * 16) + source // PAIR * 16 + source % 16
    shuffle = ones_where(place == target)
    with jax.named_scope("o_back"):
        settle(got_ref.at[1:FOUR], back_in)
    with jax.named_scope("o_shuffle"):
        for b in range(columns // PAIR):
            lanes = slice(b * PAIR, (b + 1) * PAIR)
            joined = jnp.concatenate([got_ref[g, :, lanes] for g in range(FOUR)], axis=1)
            out_ref[:, b * wide : (b + 1) * wide] = dot(joined, shuffle).astype(BF)
    with jax.named_scope("o_drain"):
        settle(ready_ref.at[1:FOUR], back_out)


def layer_kernel(
    x_ref, gain_hbm, wr_ref, wk_ref, wv_ref, wq_ref, wak_hbm, wav_hbm, down_d_hbm, down_e_hbm,
    up_d_hbm, up_e_hbm, off_d_hbm, off_e_hbm, extra_ref, init_hbm, head_gain_hbm, sink_hbm,
    lin_out_hbm, att_out_hbm,
    out_ref,
    gain_ref, wak_ref, wav_ref, off_d_ref, off_e_ref, head_gain_ref, sink_ref,
    both_ref, hid_ref, stage_ref, cols_ref, ext_ref, down_d_ref, down_e_ref, up_d_ref, up_e_ref, init_ref,
    proj_ref, logd_ref, learn_ref, cos_ref, sin_ref, wout_ref,
    reads_ref, local_ref, msg_ref, rows_ref,
    recv_ref, sent_ref, enter_ref, halo_ref, comp_ref, total_ref,
    lin_ref, att_ref, lin_give, att_give, ready_ref, got_ref,
    load_sem, late_sem, x_out, x_in, hid_out, hid_in, stage_out, stage_in, ext_out, ext_in,
    ring_out, z_in, near_in, far_in, rest_x_out, rest_x_in, rest_z_out, rest_z_in,
    wz_out, wz_in, wx_out, wx_in, wc_out, wc_in,
    out_sem, in_sem, back_out_sem, back_in_sem, halo_out_sem, halo_in_sem,
    lin_out, lin_in, lin_out2, lin_in2, att_out, att_in, att_out2, att_in2, give_sem, back_out, back_in,
):
    place_of = tuple(lax.axis_index(a) for a in ("sp_0", "sp_1", "fs", "tp"))
    width = lin_out_hbm.shape[1]
    for peer in neighbours(place_of):
        pl.semaphore_signal(
            pltpu.get_barrier_semaphore(), inc=1, device_id=peer, device_id_type=MESH
        )
    pairs = (
        (down_d_hbm, down_d_ref), (down_e_hbm, down_e_ref), (up_d_hbm, up_d_ref), (up_e_hbm, up_e_ref),
        (init_hbm, init_ref), (off_d_hbm, off_d_ref), (off_e_hbm, off_e_ref), (head_gain_hbm, head_gain_ref),
        (sink_hbm, sink_ref), (lin_out_hbm, wout_ref.at[:, :width]), (att_out_hbm, wout_ref.at[:, width:]),
    )
    late = [pltpu.make_async_copy(a, b, late_sem.at[k]) for k, (a, b) in enumerate(pairs)]
    early = [
        pltpu.make_async_copy(a, b, load_sem.at[3 + k])
        for k, (a, b) in enumerate(((gain_hbm, gain_ref), (wak_hbm, wak_ref), (wav_hbm, wav_ref)))
    ]
    rows_steps = gather_rows(
        (wout_ref, rows_ref, wz_out, wz_in, wx_out, wx_in, wc_out, wc_in), place_of
    )
    project_rest = front(
        (
            x_ref, gain_ref, wr_ref, wk_ref, wv_ref, wq_ref, wak_ref, wav_ref, down_d_ref, down_e_ref,
            up_d_ref, up_e_ref, off_d_ref, off_e_ref, extra_ref, proj_ref, logd_ref, learn_ref,
            both_ref, hid_ref, stage_ref, cols_ref, ext_ref, load_sem,
            x_out, x_in, hid_out, hid_in, stage_out, stage_in, ext_out, ext_in,
            ring_out, z_in, near_in, far_in, rest_x_out, rest_x_in, rest_z_out, rest_z_in, cos_ref, sin_ref, late, early,
        ),
        place_of,
    )
    send_halo, send_maps, run = exchange(
        (
            msg_ref, init_ref, reads_ref, local_ref, head_gain_ref, proj_ref, cos_ref, sin_ref, sink_ref,
            lin_ref, att_ref, lin_give, att_give, recv_ref, sent_ref, enter_ref, halo_ref, comp_ref,
            out_sem, in_sem, back_out_sem, back_in_sem, halo_out_sem, halo_in_sem,
        ),
        place_of,
    )
    local_maps(
        (proj_ref, logd_ref, learn_ref, reads_ref, local_ref, msg_ref),
        project_rest,
        send_halo,
        send_maps,
        rows_steps,
    )
    att_share = share(
        att_ref, att_give, ((att_out, att_in), (att_out2, att_in2)), (give_sem.at[0], give_sem.at[1]), place_of
    )
    lin_share = share(
        lin_ref, lin_give, ((lin_out, lin_in), (lin_out2, lin_in2)), (give_sem.at[2], give_sem.at[3]), place_of
    )
    columns = ready_ref.shape[2]
    joined_rows = FOUR * ready_ref.shape[1]

    def product(ref, first):
        result = None
        for core in range(2):
            left = jnp.concatenate([ref[core, g].reshape(joined_rows, PAIR) for g in range(FOUR)], axis=1)
            weight = rows_ref[core, :, :, :, first : first + width].reshape(columns, width)
            term = dot(left, weight, NT)
            result = term if result is None else result + term
        return result

    def after_attend():
        att_share[0]()

    run(after_attend, rows_steps[2])
    lin_share[0]()
    rows_steps[3]()
    with jax.named_scope("o_att_wait"):
        att_share[1]()
        rows_steps[4]()
    with jax.named_scope("o_att"):
        total_ref[...] = product(att_ref, width)
    att_share[2]()
    with jax.named_scope("o_lin_wait"):
        lin_share[1]()
    with jax.named_scope("o_lin"):
        result = (total_ref[...] + product(lin_ref, 0)).astype(BF)
        ready_ref[...] = result.reshape(ready_ref.shape)
    send_back((out_ref, ready_ref, got_ref, back_out, back_in), place_of)
    lin_share[2]()


def local(
    inputs, input_norm_gain, receptance_weight, linear_key_weight, linear_value_weight,
    window_query_weight, window_key_weight, window_value_weight, decay_down_weight, decay_up_weight,
    decay_offset, decay_log_extra, erasure_down_weight, erasure_up_weight, erasure_offset,
    initial_state, head_norm_gain, query_sink_logit, linear_output_weight, window_output_weight,
):
    tokens, model = inputs.shape[1], 2 * inputs.shape[2]
    places = lax.axis_size(SP)
    nz, nx = lax.axis_size("sp_0"), lax.axis_size("sp_1")
    rows = receptance_weight.shape[0]
    out_rows = linear_output_weight.shape[1]
    columns = places * out_rows
    vmem = pl.BlockSpec(memory_space=pltpu.VMEM)
    hbm = pl.BlockSpec(memory_space=pltpu.HBM)
    dma = pltpu.SemaphoreType.DMA
    down_d, down_e = decay_down_weight.T, erasure_down_weight.T

    def space(kind, *shape):
        return pltpu.VMEM(shape, kind)

    out = pl.pallas_call(
        layer_kernel,
        out_shape=jax.ShapeDtypeStruct((tokens // 2, FOUR * columns), BF),
        in_specs=[hbm] * 20,
        out_specs=vmem,
        scratch_shapes=[
            space(F32, 1, model),
            space(BF, *window_key_weight.shape),
            space(BF, *window_value_weight.shape),
            space(F32, *decay_offset.shape),
            space(F32, *erasure_offset.shape),
            space(F32, 1, *head_norm_gain.shape),
            pltpu.SMEM(query_sink_logit.shape, F32),
            space(BF, 2, tokens, model // 2),
            space(BF, FOUR, tokens, model),
            space(BF, FOUR, rows, 5 * PAIR),
            space(BF, places, FOUR * rows, 5 * PAIR),
            space(F32, FOUR, *decay_log_extra.shape[1:]),
            space(BF, *down_d.shape),
            space(BF, *down_e.shape),
            space(BF, *decay_up_weight.shape),
            space(BF, *erasure_up_weight.shape),
            space(F32, *initial_state.shape),
            space(BF, FOUR, tokens, 5 * PAIR),
            space(F32, 2, FOUR, tokens, PAIR),
            space(F32, 2, FOUR, tokens, PAIR),
            space(F32, tokens + 2 * WINDOW, PAIR),
            space(F32, tokens + 2 * WINDOW, PAIR),
            space(BF, out_rows, 2 * FOUR * PAIR),
            space(F32, 2, FOUR, tokens, PAIR),
            space(F32, FOUR, tokens, PAIR),
            space(BF, places, 48, PAIR),
            space(BF, 2, nz, nx, out_rows, 2 * FOUR * PAIR),
            space(BF, places, 48, PAIR),
            space(BF, places, 16, PAIR),
            space(BF, places, 16, PAIR),
            space(BF, 2, FOUR, tokens, PAIR),
            space(F32, 4, places // 4, 3 * HD // 2, HD),
            space(F32, FOUR * tokens // 2, columns),
            space(BF, 2, FOUR, FOUR, tokens // 2, PAIR),
            space(BF, 2, FOUR, FOUR, tokens // 2, PAIR),
            space(BF, FOUR, tokens // 2, PAIR),
            space(BF, FOUR, tokens // 2, PAIR),
            space(BF, FOUR, tokens // 2, columns),
            space(BF, FOUR, tokens // 2, columns),
            dma((6,)), dma((11,)),
            dma, dma, dma((1,)), dma((4,)), dma, dma, dma, dma,
            dma, dma((2, nz // 2)), dma((nz,)), dma, dma, dma, dma, dma((2, nz // 2)),
            dma, dma, dma, dma((3,)), dma, dma,
            dma, dma, dma, dma, dma, dma,
            *[dma((1,)), dma((4,))] * 4, dma((FOUR,)), dma, dma,
        ],
        compiler_params=pltpu.CompilerParams(
            collective_id=0, has_side_effects=True, vmem_limit_bytes=63 * 2**20
        ),
        name="layer",
    )(
        inputs[0], input_norm_gain[None], receptance_weight, linear_key_weight, linear_value_weight,
        window_query_weight, window_key_weight, window_value_weight, down_d, down_e,
        decay_up_weight, erasure_up_weight, decay_offset, erasure_offset, decay_log_extra,
        initial_state, head_norm_gain[None], query_sink_logit, linear_output_weight.T,
        window_output_weight.T,
    )
    return out[None]


def solution(mesh):
    finer = Mesh(
        mesh.devices.reshape(8, 4, mesh.shape["fs"], mesh.shape["tp"]), ("sp_0", "sp_1", "fs", "tp")
    )
    placed = (
        P("fs", SP, "tp"),
        P(),
        P(SP_FS, "tp"),
        P(SP_FS, "tp"),
        P(SP_FS, "tp"),
        P(SP_FS, "tp"),
        P(SP_FS, "tp"),
        P(SP_FS, "tp"),
        P(),
        P(),
        P(),
        P("fs", "tp", SP),
        P(),
        P(),
        P(),
        P(),
        P(),
        P(),
        P("tp", SP_FS),
        P("tp", SP_FS),
    )
    return jax.shard_map(
        local, mesh=finer, in_specs=placed, out_specs=P("fs", SP_TP, None), check_vma=False
    )
```
